256 devices in a mesh: fs: 32 (over z, y), rep: 4 (over x), tp: 2 (over core).
Axes of the slice: x: 4, y: 4, z: 8, core: 2. Of those that a mesh axis runs over, the one named last changes fastest.
Arguments:
- input_act: bfloat16 [98304, 2048], P(('fs', 'rep')), may hold values from -24 to 24
- query_cot: bfloat16 [98304, 1024], P(('fs', 'rep'), 'tp'), may hold values from -6 to 6
- out_cot: bfloat16 [98304, 2048], P(('fs', 'rep')), may hold values from -24 to 24
- attn_out: bfloat16 [98304, 1024], P(('fs', 'rep'), 'tp'), may hold values from -6 to 6
- query_w: float32 [2048, 1024], P('fs', 'tp'), may hold values from -0.125 to 0.125
- out_w: float32 [1024, 2048], P('tp', 'fs'), may hold values from -0.1875 to 0.1875
- query_factor: bfloat16 [2048, 512], P('fs'), may hold values from -0.125 to 0.125
- out_factor: bfloat16 [2048, 512], P('fs'), may hold values from -0.125 to 0.125
- first_q: float32 [512, 1024], P('fs', 'tp'), may hold values from -6 to 6
- second_q: float32 [512, 1024], P('fs', 'tp'), may hold values from 0.075 to 120
- first_o: float32 [512, 1024], P('fs', 'tp'), may hold values from -6 to 6
- second_o: float32 [512, 1024], P('fs', 'tp'), may hold values from 0.075 to 120
Outputs:
- new_query_w: float32 [2048, 1024], P('fs', 'tp')
- new_out_w: float32 [1024, 2048], P('tp', 'fs')
- query_step: float32 [2048, 1024], P('fs', 'tp')
- out_step: float32 [1024, 2048], P('tp', 'fs')
- new_first_q: float32 [512, 1024], P('fs', 'tp')
- new_second_q: float32 [512, 1024], P('fs', 'tp')
- new_first_o: float32 [512, 1024], P('fs', 'tp')
- new_second_o: float32 [512, 1024], P('fs', 'tp')
- query_copy: bfloat16 [2048, 1024], P(None, 'tp')
- out_copy: bfloat16 [1024, 2048], P('tp')
The draws below stay inside these ranges and needn't reach their ends.
All inputs are finite; a program needn't handle non-finite values.
Results may differ from the reference program's by a relative error of at most 0.0085.
Values may be sent and summed in bfloat16 or wider, within the bound.
A program may use at most 64 MiB of HBM per device.

```python
import math
import jax
import jax.numpy as jnp
from jax import lax

D = 2048
RANK = 512
HQ = 1024
TOKENS = 98304


def second_law(key, marker):
    local_key = jax.random.fold_in(key, marker)
    row_place = jnp.arange(RANK, dtype=jnp.float32)[:, None] / RANK
    spread = jax.random.uniform(local_key, (RANK, HQ), jnp.float32, math.log(0.3), math.log(3.0))
    return jnp.exp(spread + row_place * math.log(10.0))


def draw_second_q(key, part):
    return second_law(key, 11)


def draw_second_o(key, part):
    return second_law(key, 23)


def raised(values, stream_key, source, target, shards_of, factor):
    def block_of(position):
        return (jnp.arange(values.shape[position]) // (values.shape[position] // shards_of)).reshape((-1,) + (1,) * (values.ndim - 1 - position))

    near = jax.random.permutation(stream_key, shards_of)[block_of(target)]
    far = (block_of(target) + shards_of // 2) % shards_of
    return jnp.where((block_of(source) == near) | (block_of(source) == far), factor * values, values)


def level_of(own_key, shape, shards, least, high):
    factor_of, own = 1.0, jax.random.fold_in(own_key, 6)
    for position, parts in shards:
        steps = jnp.exp(jax.random.uniform(jax.random.fold_in(own, position), (parts,), jnp.float32, least / len(shards), high / len(shards)))
        factor_of = factor_of * jnp.repeat(steps, shape[position] // parts).reshape([-1 if axis == position else 1 for axis in range(len(shape))])
    return factor_of


def normal_values(own_key, extent, width, reach, cuts=(), kind=jnp.bfloat16):
    values = jax.random.normal(own_key, extent, jnp.float32) * width
    if len(cuts) > 0:
        values = level_of(own_key, extent, cuts, -0.22, 0.18) * values
    return jnp.clip(values, min=-reach, max=reach).astype(kind)


def gaussian_with(stream_key, dims, width, bound, shards, heavy, kind=jnp.bfloat16):
    values = width * jax.random.normal(stream_key, dims, jnp.float32)
    if shards:
        values = values * level_of(stream_key, dims, shards, -0.22, 0.18)
    return jnp.clip(raised(values, jax.random.fold_in(stream_key, 3), *heavy), -bound, bound).astype(kind)


def setup_inputs(seed: int = 0) -> dict:
    key_of = jax.random.split(jax.random.key(seed), 13)
    input_act = gaussian_with(key_of[0], (TOKENS, D), 1.0, 24.0, ((0, 128),), (0, 1, 128, 5.5))
    query_cot = normal_values(key_of[1], (TOKENS, HQ), 1.0, 6.0, ((0, 128), (1, 2)))
    out_cot = gaussian_with(key_of[2], (TOKENS, D), 1.0, 24.0, ((0, 128),), (0, 1, 128, 5.5))
    attn_out = normal_values(key_of[3], (TOKENS, HQ), 1.0, 6.0, ((0, 128), (1, 2)))
    query_w = normal_values(key_of[4], (D, HQ), D ** -0.5, 0.125, ((0, 32), (1, 2)), jnp.float32)
    out_w = normal_values(key_of[5], (HQ, D), HQ ** -0.5, 0.1875, ((0, 2), (1, 32)), jnp.float32)
    query_factor = normal_values(key_of[6], (D, RANK), D ** -0.5, 0.125, ((0, 32),))
    out_factor = normal_values(key_of[7], (D, RANK), D ** -0.5, 0.125, ((0, 32),))
    first_q = normal_values(key_of[8], (RANK, HQ), 1.0, 6.0, ((0, 32), (1, 2)), jnp.float32)
    second_q = draw_second_q(jax.random.fold_in(key_of[12], 71), 0)
    first_o = normal_values(key_of[10], (RANK, HQ), 1.0, 6.0, ((0, 32), (1, 2)), jnp.float32)
    second_o = draw_second_o(jax.random.fold_in(key_of[12], 71), 0)
    return dict(input_act=input_act, query_cot=query_cot, out_cot=out_cot, attn_out=attn_out, query_w=query_w, out_w=out_w, query_factor=query_factor, out_factor=out_factor, first_q=first_q, second_q=second_q, first_o=first_o, second_o=second_o)


def contract_rows(left_side, right_side):
    return lax.dot_general(left_side, right_side, (((0,), (0,)), ((), ())), preferred_element_type=jnp.float32)

def exact_dot(left_side, right_side):
    return jnp.dot(left_side, right_side, precision=lax.Precision.HIGHEST, preferred_element_type=jnp.float32)

def reference(input_act, query_cot, out_cot, attn_out, query_w, out_w, query_factor, out_factor, first_q, second_q, first_o, second_o):
    scale_tokens = 1.0 / math.sqrt(TOKENS)
    grad_q = contract_rows(input_act, query_cot) * scale_tokens
    grad_o = contract_rows(out_cot, attn_out) * scale_tokens
    factor_q = query_factor.astype(jnp.float32)
    factor_o = out_factor.astype(jnp.float32)
    proj_q = exact_dot(factor_q.T, grad_q)
    proj_o = exact_dot(factor_o.T, grad_o)
    new_first_q = 0.8 * first_q + 0.2 * proj_q
    new_second_q = 0.9 * second_q + 0.1 * proj_q * proj_q
    new_first_o = 0.8 * first_o + 0.2 * proj_o
    new_second_o = 0.9 * second_o + 0.1 * proj_o * proj_o
    dir_q = new_first_q / jnp.sqrt(new_second_q)
    dir_o = new_first_o / jnp.sqrt(new_second_o)
    mean_square = (jnp.sum(dir_q * dir_q) + jnp.sum(dir_o * dir_o)) / (2 * RANK * HQ)
    norm_scale = jnp.sqrt(mean_square + 1e-06)
    query_step = exact_dot(factor_q, dir_q) / norm_scale
    out_step = (exact_dot(factor_o, dir_o) / norm_scale).T
    new_query_w = query_w - 0.01 * query_step
    new_out_w = out_w - 0.01 * out_step
    query_copy = new_query_w.astype(jnp.bfloat16)
    out_copy = new_out_w.astype(jnp.bfloat16)
    return (new_query_w, new_out_w, query_step, out_step, new_first_q, new_second_q, new_first_o, new_second_o, query_copy, out_copy)
```

```python
import functools
import math

import jax
import jax.numpy as jnp
from jax import lax
from jax.experimental import pallas as pl
from jax.experimental.pallas import tpu as pltpu
from jax.sharding import Mesh
from jax.sharding import PartitionSpec as P

NZ, NY, NX = 8, 4, 4
NF = NZ * NY
D, RANK, HQ, TOKENS = 2048, 512, 1024, 98304
HALF = HQ // 2
TOK = TOKENS // (NF * NX)
ROWS = D // NF
MINE = RANK // NF
Z, Y, X, C = "fs_0", "fs_1", "rep", "tp"
FS = (Z, Y)
FS_REP = (Z, Y, X)
BF, F32 = jnp.bfloat16, jnp.float32
MESH = pl.DeviceIdType.MESH


def reach(n, flip):
    far = (n // 2, n - 1 - n // 2)
    return far[::-1] if flip else far


def ring_plan(axes, sizes, flip):
    first = reach(sizes[0], flip)
    events = []
    for i in range(-first[1], first[0] + 1):
        second = reach(sizes[1], (i + flip) % 2)
        for j in range(-second[1], second[0] + 1):
            on = []
            if j == 0:
                for s, far in ((1, first[0]), (-1, first[1])):
                    if i * s >= 0 and abs(i) < far:
                        on.append((axes[0], s, (i + s, 0)))
                on += [(axes[1], s, (i, s)) for s in (1, -1)]
            else:
                s = 1 if j > 0 else -1
                if abs(j) < second[0 if s > 0 else 1]:
                    on.append((axes[1], s, (i, j + s)))
            events.append((abs(i) + abs(j), (i, j), on))
    events.sort(key=lambda e: e[0])
    slots = {e[1]: n for n, e in enumerate(events[1:])}
    return dict(axes=axes, events=events, slots=slots)


class Gather:
    def __init__(self, plan, piece, where, send_sem, recv_sem, span):
        self.plan, self.piece, self.where = plan, piece, where
        self.send_sem, self.recv_sem, self.span = send_sem, recv_sem, span

    def ref(self, key):
        off = dict(zip(self.plan["axes"], key))
        z = lax.rem(self.where[Z] + (NZ - off[Z]), NZ)
        y = lax.rem(self.where[Y] + (NY - off[Y]), NY)
        return self.piece(z * NY + y)

    def copy(self, key, axis, sign, landed):
        n = NZ if axis == Z else NY
        ref = self.ref(key)
        return pltpu.make_async_remote_copy(
            src_ref=ref,
            dst_ref=ref,
            send_sem=self.send_sem,
            recv_sem=self.recv_sem.at[self.plan["slots"][landed]],
            device_id={axis: lax.rem(self.where[axis] + (n + sign), n)},
            device_id_type=MESH,
        )

    def pass_on(self, event):
        _, key, on = event
        for axis, sign, landed in on:
            self.copy(key, axis, sign, landed).start()

    def start(self):
        self.pass_on(self.plan["events"][0])

    def arrive(self, event):
        key = event[1]
        self.copy(key, self.plan["axes"][0], 1, key).wait_recv()
        self.pass_on(event)

    def hops(self, number):
        return [(self, e) for e in self.plan["events"] if e[0] == number]

    def finish(self):
        ref = self.span
        pltpu.make_async_remote_copy(
            src_ref=ref,
            dst_ref=ref,
            send_sem=self.send_sem,
            recv_sem=self.recv_sem.at[0],
            device_id={Z: lax.rem(self.where[Z] + 1, NZ)},
            device_id_type=MESH,
        ).wait_send()


ZY = ring_plan((Z, Y), (NZ, NY), 0)
YZ = ring_plan((Y, Z), (NY, NZ), 0)
PIECES = NF - 1
HOPS = ZY["events"][-1][0]


def arrivals(gathers, number):
    todo = [g.hops(number) for g in gathers]
    for k in range(max(len(t) for t in todo)):
        for t in todo:
            if k < len(t):
                t[k][0].arrive(t[k][1])


def turned(value):
    return jnp.concatenate([value, jnp.zeros_like(value)], axis=1).T[:ROWS]


def turned_back(value):
    return jnp.concatenate([value, jnp.zeros_like(value)], axis=0).T[:, :ROWS]


def kernel(*refs):
    (
        input_act, query_cot, out_cot, attn_out, query_w, out_w, query_factor, out_factor,
        first_q, second_q, first_o, second_o,
        new_qw, new_ow, q_step, o_step, nf_q, ns_q, nf_o, ns_o, q_copy, o_copy,
        gf, gw, gd, act, cot, own_f, qw, ow, moments, low_hi, low_lo, px, rx1, rx2, s1, ry, s2,
        rz, sp, sp_out, norm, norm_in, outq, outo, st_q, st_o, nw_q, nw_o, nm,
        load, f_send, f_recv, w_send, w_recv, d_send, d_recv, cot_send, cot_recv, fx_send, fx_recv,
        rx1_send, rx1_recv, rx2_send, rx2_recv, ry_send, ry_recv, rz_send, rz_recv,
        sp_send, sp_recv, nrm_sem, out_sem, copy_sem,
    ) = refs
    z, y, x, c = (lax.axis_index(a) for a in (Z, Y, X, C))
    f = z * NY + y
    where = {Z: z, Y: y}
    other = 1 - c
    owner = x // 2

    def load_own(number, if_q, if_o, dst):
        @pl.when(c == 0)
        def _():
            pltpu.make_async_copy(if_q, dst, load.at[number]).start()

        @pl.when(c == 1)
        def _():
            pltpu.make_async_copy(if_o, dst, load.at[number]).start()

        return pltpu.make_async_copy(if_q, dst, load.at[number])

    def load_plain(number, src, dst):
        cp = pltpu.make_async_copy(src, dst, load.at[number])
        cp.start()
        return cp

    fac = []
    for j in range(4):
        cols = pl.ds(128 * j, 128)
        fac.append(load_own(j, query_factor.at[:, cols], out_factor.at[:, cols], gf.at[c, j, f]))
    w_loads = [load_plain(4, query_w, qw), load_plain(5, out_w, ow)]
    act_load = load_own(6, input_act, out_cot, act)
    cot_loads = []
    for k in range(2):
        cols = pl.ds(256 * k, 256)
        cot_loads.append(
            load_own(7 + k, query_cot.at[:, cols], attn_out.at[:, cols], cot.at[2 * c + k])
        )
    late = [load_plain(9, query_factor, own_f.at[0]), load_plain(10, out_factor, own_f.at[1])]
    for k, m in enumerate((first_q, second_q, first_o, second_o)):
        late.append(load_plain(11 + k, m, moments.at[k]))

    barrier = pltpu.get_barrier_semaphore()
    peers = [{Z: lax.rem(z + d, NZ)} for d in range(1, NZ)]
    peers += [{Y: lax.rem(y + d, NY)} for d in range(1, NY)]
    for d in range(1, NX):
        for core in (c, other):
            peers.append({X: lax.rem(x + d, NX), C: core})
    peers.append({C: other})
    for peer in peers:
        pl.semaphore_signal(barrier, inc=1, device_id=peer, device_id_type=MESH)

    for w in w_loads:
        w.wait()
    w_q = qw[...]
    w_o = turned(ow[...])
    for k in range(2):
        gw[k, f, 0] = w_q[:, 256 * k : 256 * k + 256].astype(BF)
        gw[k, f, 1] = w_o[:, 256 * k : 256 * k + 256].astype(BF)
    for w in fac:
        w.wait()
    pl.semaphore_wait(barrier, len(peers))

    def factor_gather(j):
        return Gather(
            ZY if j % 2 == 0 else YZ,
            lambda p, j=j: gf.at[c, j, p],
            where,
            f_send.at[j],
            f_recv.at[j],
            gf.at[c, j, pl.ds(0, PIECES)],
        )

    def weight_gather(k):
        return Gather(
            ZY if k == 0 else YZ,
            lambda p, k=k: gw.at[k, p],
            where,
            w_send.at[k],
            w_recv.at[k],
            gw.at[k, pl.ds(0, PIECES)],
        )

    def dir_gather(k):
        return Gather(
            ZY if k == 0 else YZ,
            lambda p, k=k: gd.at[k, p],
            where,
            d_send.at[k],
            d_recv.at[k],
            gd.at[k, pl.ds(0, PIECES)],
        )

    fg = [factor_gather(j) for j in range(4)]
    wg = [weight_gather(k) for k in range(2)]
    dg = [dir_gather(k) for k in range(2)]

    def cot_copy(src, k):
        return pltpu.make_async_remote_copy(
            src_ref=src.at[:, pl.ds(256 * k, 256)],
            dst_ref=cot.at[2 * c + k],
            send_sem=cot_send.at[k],
            recv_sem=cot_recv.at[k],
            device_id={C: other},
            device_id_type=MESH,
        )

    fg[0].start()
    fg[1].start()
    for k in range(2):

        @pl.when(c == 0)
        def _():
            cot_copy(attn_out, k).start()

        @pl.when(c == 1)
        def _():
            cot_copy(query_cot, k).start()

    def factor_swap(h):
        ref = gf.at[c, pl.ds(2 * h, 2)]
        return pltpu.make_async_remote_copy(
            src_ref=ref,
            dst_ref=ref,
            send_sem=fx_send.at[h],
            recv_sem=fx_recv.at[h],
            device_id={C: other},
            device_id_type=MESH,
        )

    def project(h):
        def tile(m, _):
            rows = pl.ds(pl.multiple_of(m * 256, 256), 256)
            right = jnp.concatenate(
                [gf[c, 2 * h].reshape(D, 128), gf[c, 2 * h + 1].reshape(D, 128)], axis=1
            )
            low = jnp.dot(act[rows, :], right, preferred_element_type=F32)
            hi = low.astype(BF)
            low_hi[rows, :] = hi
            low_lo[rows, :] = (low - hi.astype(F32)).astype(BF)
            return 0

        lax.fori_loop(0, TOK // 256, tile, 0)

        def quarter(i, _):
            xb = lax.rem(x + 2 + i, NX)
            side = cot[xb]
            dims = (((0,), (0,)), ((), ()))
            total = lax.dot_general(low_hi[...], side, dims, preferred_element_type=F32)
            total += lax.dot_general(low_lo[...], side, dims, preferred_element_type=F32)
            px[h, xb] = total.astype(BF)
            return 0

        lax.fori_loop(0, NX, quarter, 0)

    x_up, x_down, x_far = lax.rem(x + 1, NX), lax.rem(x + 3, NX), lax.rem(x + 2, NX)
    sides = ((x_up, 0), (x_down, 1))

    def x_first(h, k):
        return pltpu.make_async_remote_copy(
            src_ref=px.at[h, x_far, pl.ds(128 * k, 128)],
            dst_ref=rx1.at[h, k],
            send_sem=rx1_send.at[h, k],
            recv_sem=rx1_recv.at[h, k],
            device_id={X: sides[k][0]},
            device_id_type=MESH,
        )

    def x_second(h, k):
        return pltpu.make_async_remote_copy(
            src_ref=px.at[h, sides[k][0]],
            dst_ref=rx2.at[h, k],
            send_sem=rx2_send.at[h, k],
            recv_sem=rx2_recv.at[h, k],
            device_id={X: sides[k][0]},
            device_id_type=MESH,
        )

    def x_merge(h):
        for to, k in sides:
            x_first(h, k).wait_recv()
            rows = pl.ds(128 * k, 128)
            merged = px[h, to, rows].astype(F32) + rx1[h, k].astype(F32)
            px[h, to, rows] = merged.astype(BF)
            x_second(h, k).start()

    def x_sum(h):
        total = px[h, x].astype(F32)
        for _, k in sides:
            x_second(h, k).wait_recv()
            total += rx2[h, k].astype(F32)
        s1[pl.ds(4 * h, 4)] = total.astype(BF).reshape(4, NY, MINE, 256)

    def y_copy(h, d):
        to = lax.rem(y + d, NY)
        return pltpu.make_async_remote_copy(
            src_ref=s1.at[pl.ds(4 * h, 4), to],
            dst_ref=ry.at[h, d - 1],
            send_sem=ry_send.at[h, d - 1],
            recv_sem=ry_recv.at[h, d - 1],
            device_id={Y: to},
            device_id_type=MESH,
        )

    def y_sum(h):
        total = s1[pl.ds(4 * h, 4), y].astype(F32)
        for d in range(1, NY):
            y_copy(h, d).wait_recv()
            total += ry[h, d - 1].astype(F32)
        s2[pl.ds(4 * h, 4)] = total.astype(BF)

    def z_copy(d):
        to = lax.rem(z + d, NZ)
        return pltpu.make_async_remote_copy(
            src_ref=s2.at[to],
            dst_ref=rz.at[d - 1],
            send_sem=rz_send.at[d - 1],
            recv_sem=rz_recv.at[d - 1],
            device_id={Z: to},
            device_id_type=MESH,
        )

    def sum_copy(d):
        return pltpu.make_async_remote_copy(
            src_ref=sp_out,
            dst_ref=sp.at[c, lax.rem(x, 2)],
            send_sem=sp_send.at[d],
            recv_sem=sp_recv.at[c, lax.rem(x, 2)],
            device_id={X: lax.rem(x + d, NX), C: owner},
            device_id_type=MESH,
        )

    for n in range(1, HOPS + 1):
        arrivals(fg[:2], n)
    fg[2].start()
    fg[3].start()
    factor_swap(0).start()
    act_load.wait()
    for w in cot_loads:
        w.wait()
    for k in range(2):
        cot_copy(attn_out, k).wait_recv()
    project(0)
    for k in range(2):
        x_first(0, k).start()
    for n in range(1, 4):
        arrivals(fg[2:], n)
    x_merge(0)
    for n in range(4, HOPS + 1):
        arrivals(fg[2:], n)
    x_sum(0)
    for d in range(1, NY):
        y_copy(0, d).start()
    for g in wg:
        g.start()
    factor_swap(1).start()
    project(1)
    for k in range(2):
        x_first(1, k).start()
    arrivals(wg, 1)
    x_merge(1)
    y_sum(0)
    arrivals(wg, 2)
    x_sum(1)
    for d in range(1, NY):
        y_copy(1, d).start()
    arrivals(wg, 3)
    y_sum(1)
    for d in range(1, NZ):
        z_copy(d).start()
    arrivals(wg, 4)
    total = s2[z].astype(F32)
    for d in range(1, NZ):
        z_copy(d).wait_recv()
        total += rz[d - 1].astype(F32)

    sp_out[...] = total

    @pl.when(c == owner)
    def _():
        sp[c, lax.rem(x, 2)] = total

    @pl.when(c != owner)
    def _():
        sum_copy(0).start()

    for d in range(1, NX):
        sum_copy(d).start()
    arrivals(wg, 5)
    for w in late:
        w.wait()
    for t in range(2):
        for s in range(2):

            @pl.when(jnp.logical_or(x != 2 * c + s, c != t))
            def _():
                pltpu.make_async_remote_copy(
                    src_ref=sp_out,
                    dst_ref=sp.at[t, s],
                    send_sem=sp_send.at[0],
                    recv_sem=sp_recv.at[t, s],
                    device_id={C: other},
                    device_id_type=MESH,
                ).wait_recv()

    outs = []

    def put(number, src, dst):
        cp = pltpu.make_async_copy(src, dst, out_sem.at[number])
        cp.start()
        outs.append(cp)

    for t, (nf, ns) in enumerate(((nf_q, ns_q), (nf_o, ns_o))):
        proj = jnp.concatenate([sp[t, 0], sp[t, 1]], axis=1) * (1.0 / math.sqrt(TOKENS))
        first = 0.8 * moments[2 * t] + 0.2 * proj
        second = 0.9 * moments[2 * t + 1] + 0.1 * proj * proj
        nm[2 * t] = first
        nm[2 * t + 1] = second
        gd[t, f] = (first / jnp.sqrt(second)).astype(BF)
        dg[t].start()
    for t, (nf, ns) in enumerate(((nf_q, ns_q), (nf_o, ns_o))):
        put(2 * t, nm.at[2 * t], nf)
        put(2 * t + 1, nm.at[2 * t + 1], ns)
    arrivals(wg, HOPS)
    for n in range(1, HOPS + 1):
        arrivals(dg, n)

    dir_q, dir_o = gd[0].reshape(RANK, HALF), gd[1].reshape(RANK, HALF)
    squares = jnp.square(dir_q.astype(F32)) + jnp.square(dir_o.astype(F32))
    norm[...] = jnp.broadcast_to(jnp.sum(squares, axis=(0, 1), keepdims=True), (8, 128))
    norm_copy = pltpu.make_async_remote_copy(
        src_ref=norm,
        dst_ref=norm_in,
        send_sem=nrm_sem.at[0],
        recv_sem=nrm_sem.at[1],
        device_id={C: other},
        device_id_type=MESH,
    )
    norm_copy.start()
    for h in range(2):
        factor_swap(h).wait_recv()
    norm_copy.wait()
    mean = (norm[...] + norm_in[...]) / (2 * RANK * HQ)
    inverse = 1.0 / jnp.sqrt(mean + 1e-06)
    inverse = jnp.concatenate([inverse[0:1]] * 4, axis=1)

    def block(b, _):
        some = pl.ds(4 * b, 4)
        moved = []
        for t in range(2):
            rows = jnp.concatenate(
                [gf[t, j, some].reshape(4 * ROWS, 128) for j in range(4)], axis=1
            )
            step = jnp.dot(rows, gd[t].reshape(RANK, HALF), preferred_element_type=F32)
            old = jnp.concatenate(
                [gw[k, some, t].reshape(4 * ROWS, 256) for k in range(2)], axis=1
            )
            moved.append(old.astype(F32) - (0.01 * inverse) * step)
        outq[b] = moved[0].astype(BF)
        outo[b] = moved[1].T.astype(BF)
        at = pl.ds(pl.multiple_of(256 * b, 256), 256)
        pltpu.make_async_copy(outq.at[b], q_copy.at[at], copy_sem.at[0, b]).start()
        pltpu.make_async_copy(outo.at[b], o_copy.at[:, at], copy_sem.at[1, b]).start()
        return 0

    lax.fori_loop(0, D // 256, block, 0)

    step = jnp.dot(own_f[0], gd[0].reshape(RANK, HALF), preferred_element_type=F32) * inverse
    st_q[...] = step
    nw_q[...] = qw[...] - 0.01 * step
    put(4, st_q, q_step)
    put(5, nw_q, new_qw)
    step = jnp.dot(own_f[1], gd[1].reshape(RANK, HALF), preferred_element_type=F32) * inverse
    step = turned_back(step)
    st_o[...] = step
    nw_o[...] = ow[...] - 0.01 * step
    put(6, st_o, o_step)
    put(7, nw_o, new_ow)

    for g in fg + wg + dg:
        g.finish()
    for k in range(2):
        cot_copy(attn_out, k).wait_send()
        factor_swap(k).wait_send()
        for h in range(2):
            x_first(h, k).wait_send()
            x_second(h, k).wait_send()
    for h in range(2):
        for d in range(1, NY):
            y_copy(h, d).wait_send()
    for d in range(1, NZ):
        z_copy(d).wait_send()
    for d in range(1, NX):
        sum_copy(d).wait_send()

    @pl.when(c != owner)
    def _():
        sum_copy(0).wait_send()

    for cp in outs:
        cp.wait()
    for b in range(D // 256):
        at = pl.ds(256 * b, 256)
        pltpu.make_async_copy(outq.at[b], q_copy.at[at], copy_sem.at[0, b]).wait()
        pltpu.make_async_copy(outo.at[b], o_copy.at[:, at], copy_sem.at[1, b]).wait()


def body(*args):
    struct = jax.ShapeDtypeStruct
    dma = pltpu.SemaphoreType.DMA
    scratch = [
        pltpu.VMEM((2, 4, NF, ROWS, 128), BF),
        pltpu.VMEM((2, NF, 2, ROWS, 256), BF),
        pltpu.VMEM((2, NF, MINE, HALF), BF),
        pltpu.VMEM((TOK, D), BF),
        pltpu.VMEM((4, TOK, 256), BF),
        pltpu.VMEM((2, ROWS, RANK), BF),
        pltpu.VMEM((ROWS, HALF), F32),
        pltpu.VMEM((HALF, ROWS), F32),
        pltpu.VMEM((4, MINE, HALF), F32),
        pltpu.VMEM((TOK, 256), BF),
        pltpu.VMEM((TOK, 256), BF),
        pltpu.VMEM((2, NX, 256, 256), BF),
        pltpu.VMEM((2, 2, 128, 256), BF),
        pltpu.VMEM((2, 2, 256, 256), BF),
        pltpu.VMEM((NZ, NY, MINE, 256), BF),
        pltpu.VMEM((2, NY - 1, 4, MINE, 256), BF),
        pltpu.VMEM((NZ, MINE, 256), BF),
        pltpu.VMEM((NZ - 1, MINE, 256), BF),
        pltpu.VMEM((2, 2, MINE, 256), F32),
        pltpu.VMEM((MINE, 256), F32),
        pltpu.VMEM((8, 128), F32),
        pltpu.VMEM((8, 128), F32),
        pltpu.VMEM((D // 256, 256, HALF), BF),
        pltpu.VMEM((D // 256, HALF, 256), BF),
        pltpu.VMEM((ROWS, HALF), F32),
        pltpu.VMEM((HALF, ROWS), F32),
        pltpu.VMEM((ROWS, HALF), F32),
        pltpu.VMEM((HALF, ROWS), F32),
        pltpu.VMEM((4, MINE, HALF), F32),
        dma((15,)),
        dma((4,)),
        dma((4, PIECES)),
        dma((2,)),
        dma((2, PIECES)),
        dma((2,)),
        dma((2, PIECES)),
        dma((2,)),
        dma((2,)),
        dma((2,)),
        dma((2,)),
        dma((2, 2)),
        dma((2, 2)),
        dma((2, 2)),
        dma((2, 2)),
        dma((2, NY - 1)),
        dma((2, NY - 1)),
        dma((NZ - 1,)),
        dma((NZ - 1,)),
        dma((NX,)),
        dma((2, 2)),
        dma((2,)),
        dma((8,)),
        dma((2, D // 256)),
    ]
    return pl.pallas_call(
        kernel,
        out_shape=(
            struct((ROWS, HALF), F32),
            struct((HALF, ROWS), F32),
            struct((ROWS, HALF), F32),
            struct((HALF, ROWS), F32),
            *[struct((MINE, HALF), F32)] * 4,
            struct((D, HALF), BF),
            struct((HALF, D), BF),
        ),
        in_specs=[pl.BlockSpec(memory_space=pl.ANY)] * 12,
        out_specs=[pl.BlockSpec(memory_space=pl.ANY)] * 10,
        scratch_shapes=scratch,
        compiler_params=pltpu.CompilerParams(
            collective_id=0, has_side_effects=True, vmem_limit_bytes=56 * 1024 * 1024
        ),
        name="moment_update",
    )(*args)


def solution(mesh):
    finer = Mesh(mesh.devices.reshape(NZ, NY, NX, 2), (Z, Y, X, C))
    in_specs = (
        P(FS_REP, None),
        P(FS_REP, C),
        P(FS_REP, None),
        P(FS_REP, C),
        P(FS, C),
        P(C, FS),
        P(FS, None),
        P(FS, None),
        *[P(FS, C)] * 4,
    )
    out_specs = (
        P(FS, C),
        P(C, FS),
        P(FS, C),
        P(C, FS),
        *[P(FS, C)] * 4,
        P(None, C),
        P(C, None),
    )
    return jax.shard_map(body, mesh=finer, in_specs=in_specs, out_specs=out_specs, check_vma=False)
```

```python
import math

import jax
import jax.numpy as jnp
from jax import lax
from jax.experimental import pallas as pl
from jax.experimental.pallas import tpu as pltpu
from jax.sharding import Mesh
from jax.sharding import PartitionSpec as P

NZ, NY, NX = 8, 4, 4
NF = NZ * NY
D, RANK, HQ, TOKENS = 2048, 512, 1024, 98304
HALF = HQ // 2
TOK = TOKENS // (NF * NX)
ROWS = D // NF
MINE = RANK // NF
BLOCKS = 8
Z, Y, X, C = "fs_0", "fs_1", "rep", "tp"
FS = (Z, Y)
FS_REP = (Z, Y, X)
BF, F32 = jnp.bfloat16, jnp.float32
MESH = pl.DeviceIdType.MESH


def reach(n, flip):
    far = (n // 2, n - 1 - n // 2)
    return far[::-1] if flip else far


def ring_plan(axes, sizes, flip):
    first = reach(sizes[0], flip)
    events = []
    for i in range(-first[1], first[0] + 1):
        second = reach(sizes[1], (i + flip) % 2)
        for j in range(-second[1], second[0] + 1):
            on = []
            if j == 0:
                for s, far in ((1, first[0]), (-1, first[1])):
                    if i * s >= 0 and abs(i) < far:
                        on.append((axes[0], s, (i + s, 0)))
                on += [(axes[1], s, (i, s)) for s in (1, -1)]
            else:
                s = 1 if j > 0 else -1
                if abs(j) < second[0 if s > 0 else 1]:
                    on.append((axes[1], s, (i, j + s)))
            events.append((abs(i) + abs(j), (i, j), on))
    events.sort(key=lambda e: e[0])
    slots = {e[1]: n for n, e in enumerate(events[1:])}
    return dict(axes=axes, events=events, slots=slots)


class Gather:
    def __init__(self, plan, piece, share, where, send_sem, recv_sem, pass_sem, give_sem, own=0):
        self.shares = pl.ds(0, PIECES + own)
        self.plan, self.piece, self.share, self.where = plan, piece, share, where
        self.send_sem, self.recv_sem = send_sem, recv_sem
        self.pass_sem, self.give_sem = pass_sem, give_sem

    def index(self, key):
        off = dict(zip(self.plan["axes"], key))
        z = lax.rem(self.where[Z] + (NZ - off[Z]), NZ)
        y = lax.rem(self.where[Y] + (NY - off[Y]), NY)
        return z * NY + y

    def copy(self, ref, axis, sign, slot):
        n = NZ if axis == Z else NY
        return pltpu.make_async_remote_copy(
            src_ref=ref,
            dst_ref=ref,
            send_sem=self.send_sem,
            recv_sem=self.recv_sem.at[slot],
            device_id={axis: lax.rem(self.where[axis] + (n + sign), n)},
            device_id_type=MESH,
        )

    def give(self, ref):
        return pltpu.make_async_remote_copy(
            src_ref=ref,
            dst_ref=ref,
            send_sem=self.pass_sem,
            recv_sem=self.give_sem,
            device_id={C: 0},
            device_id_type=MESH,
        )

    def pass_on(self, event):
        ref = self.piece(self.index(event[1]))
        for axis, sign, landed in event[2]:
            self.copy(ref, axis, sign, self.plan["slots"][landed]).start()

    def start(self):
        self.pass_on(self.plan["events"][0])

    def arrive(self, event):
        f = self.index(event[1])
        self.copy(self.piece(f), self.plan["axes"][0], 1, self.plan["slots"][event[1]]).wait_recv()
        self.pass_on(event)
        self.give(self.share(f)).start()

    def hops(self, number):
        return [(self, e) for e in self.plan["events"] if e[0] == number]

    def finish(self):
        self.copy(self.piece(pl.ds(0, PIECES)), Z, 1, 0).wait_send()
        self.give(self.share(self.shares)).wait_send()

    def given(self):
        self.give(self.share(self.shares)).wait_recv()


ZY = ring_plan((Z, Y), (NZ, NY), 0)
YZ = ring_plan((Y, Z), (NY, NZ), 0)
PIECES = NF - 1
HOPS = ZY["events"][-1][0]


def arrivals(gathers, number):
    todo = [g.hops(number) for g in gathers]
    for k in range(max(len(t) for t in todo)):
        for t in todo:
            if k < len(t):
                t[k][0].arrive(t[k][1])


def reduce_kernel(*refs):
    (
        input_act, query_cot, out_cot, attn_out, query_w, out_w, query_factor, out_factor,
        first_q, second_q, first_o, second_o,
        gf_out, gw_out, gd_out, nm_out, sq_out,
        gf, gw, gd, act, cot, qw, ow, moments, low_hi, low_lo, px, rx1, rx2, s1, ry, s2,
        rz, sp, sp_out, sq, nm,
        load, f_send, f_recv, f_pass, f_give, w_send, w_recv, w_pass, w_give,
        d_send, d_recv, d_pass, d_give, own_send, own_recv, mom_send, mom_recv,
        cot_send, cot_recv,
        rx1_send, rx1_recv, rx2_send, rx2_recv, ry_send, ry_recv, rz_send, rz_recv,
        sp_send, sp_recv, nm_sem, sq_sem, out_sem,
    ) = refs
    z, y, x, c = (lax.axis_index(a) for a in (Z, Y, X, C))
    f = z * NY + y
    where = {Z: z, Y: y}
    other = 1 - c
    leads, follows = pl.when(c == 1), pl.when(c == 0)

    def load_own(number, if_q, if_o, dst):
        @follows
        def _():
            pltpu.make_async_copy(if_q, dst, load.at[number]).start()

        @leads
        def _():
            pltpu.make_async_copy(if_o, dst, load.at[number]).start()

        return pltpu.make_async_copy(if_q, dst, load.at[number])

    def load_plain(number, src, dst):
        cp = pltpu.make_async_copy(src, dst, load.at[number])
        cp.start()
        return cp

    fac = []
    for j in range(4):
        cols = pl.ds(128 * j, 128)
        for t, factor in enumerate((query_factor, out_factor)):
            fac.append(load_plain(2 * j + t, factor.at[:, cols], gf.at[j, f, t]))
    w_loads = [load_plain(8, query_w, qw), load_plain(9, out_w, ow)]
    act_load = load_own(10, input_act, out_cot, act)
    cot_loads = []
    for k in range(2):
        cols = pl.ds(256 * k, 256)
        cot_loads.append(
            load_own(11 + k, query_cot.at[:, cols], attn_out.at[:, cols], cot.at[2 * c + k])
        )

    barrier = pltpu.get_barrier_semaphore()
    peers = [{C: other}]
    for axis, at, n in ((Z, z, NZ), (Y, y, NY), (X, x, NX)):
        peers += [{axis: lax.rem(at + 1, n)}, {axis: lax.rem(at + n - 1, n)}]
    for peer in peers:
        pl.semaphore_signal(barrier, inc=1, device_id=peer, device_id_type=MESH)

    for w in w_loads:
        w.wait()
    for k in range(2):
        gw[k, f, c, 0] = qw[:, 256 * k : 256 * k + 256].astype(BF)
        gw[k, f, c, 1] = ow[:, 256 * k : 256 * k + 256].astype(BF)
    for w in fac:
        w.wait()
    pl.semaphore_wait(barrier, len(peers))

    fg = [
        Gather(
            ZY if j % 2 == 0 else YZ,
            lambda p, j=j: gf.at[j, p],
            lambda p, j=j: gf.at[j, p],
            where, f_send.at[j], f_recv.at[j], f_pass.at[j], f_give.at[j],
        )
        for j in range(4)
    ]
    wg = [
        Gather(
            ZY if k == 0 else YZ,
            lambda p, k=k: gw.at[k, p],
            lambda p, k=k: gw.at[k, p, 0],
            where, w_send.at[k], w_recv.at[k], w_pass.at[k], w_give.at[k],
        )
        for k in range(2)
    ]
    dg = [
        Gather(
            ZY if k == 0 else YZ,
            lambda p, k=k: gd.at[k, p],
            lambda p, k=k: gd.at[k, p, 0],
            where, d_send.at[k], d_recv.at[k], d_pass.at[k], d_give.at[k], 1,
        )
        for k in range(2)
    ]

    @leads
    def _():
        for g in fg:
            g.start()

    def cot_copy(src, k):
        return pltpu.make_async_remote_copy(
            src_ref=src.at[:, pl.ds(256 * k, 256)],
            dst_ref=cot.at[2 * c + k],
            send_sem=cot_send.at[k],
            recv_sem=cot_recv.at[k],
            device_id={C: other},
            device_id_type=MESH,
        )

    def own_weights(k):
        ref = gw.at[k, f, 0]
        return pltpu.make_async_remote_copy(
            src_ref=ref,
            dst_ref=ref,
            send_sem=own_send.at[k],
            recv_sem=own_recv.at[k],
            device_id={C: 1},
            device_id_type=MESH,
        )

    def own_moments(k, m):
        return pltpu.make_async_remote_copy(
            src_ref=m,
            dst_ref=moments.at[k, 0],
            send_sem=mom_send.at[k],
            recv_sem=mom_recv.at[k],
            device_id={C: 1},
            device_id_type=MESH,
        )

    all_moments = (first_q, second_q, first_o, second_o)

    @follows
    def _():
        for k in range(2):
            cot_copy(attn_out, k).start()
        for k in range(2):
            own_weights(k).start()
        for k, m in enumerate(all_moments):
            own_moments(k, m).start()

    @leads
    def _():
        for k in range(2):
            cot_copy(query_cot, k).start()
        for k, m in enumerate(all_moments):
            pltpu.make_async_copy(m, moments.at[k, 1], load.at[13 + k]).start()

    def project(h):
        def tile(m, _):
            rows = pl.ds(pl.multiple_of(m * 256, 256), 256)
            right = jnp.concatenate(
                [gf[2 * h + j, :, c].reshape(D, 128) for j in range(2)], axis=1
            )
            low = jnp.dot(act[rows, :], right, preferred_element_type=F32)
            hi = low.astype(BF)
            low_hi[rows, :] = hi
            low_lo[rows, :] = (low - hi.astype(F32)).astype(BF)
            return 0

        lax.fori_loop(0, TOK // 256, tile, 0)

        def quarter(i, _):
            xb = lax.rem(x + 2 + i, NX)
            side = cot[xb]
            dims = (((0,), (0,)), ((), ()))
            total = lax.dot_general(low_hi[...], side, dims, preferred_element_type=F32)
            total += lax.dot_general(low_lo[...], side, dims, preferred_element_type=F32)
            px[h, xb] = total.astype(BF)
            return 0

        lax.fori_loop(0, NX, quarter, 0)

    x_up, x_down, x_far = lax.rem(x + 1, NX), lax.rem(x + 3, NX), lax.rem(x + 2, NX)
    sides = ((x_up, 0), (x_down, 1))

    def x_first(h, k):
        return pltpu.make_async_remote_copy(
            src_ref=px.at[h, x_far, pl.ds(128 * k, 128)],
            dst_ref=rx1.at[h, k],
            send_sem=rx1_send.at[h, k],
            recv_sem=rx1_recv.at[h, k],
            device_id={X: sides[k][0]},
            device_id_type=MESH,
        )

    def x_second(h, k):
        return pltpu.make_async_remote_copy(
            src_ref=px.at[h, sides[k][0]],
            dst_ref=rx2.at[h, k],
            send_sem=rx2_send.at[h, k],
            recv_sem=rx2_recv.at[h, k],
            device_id={X: sides[k][0]},
            device_id_type=MESH,
        )

    def x_merge(h):
        for to, k in sides:
            x_first(h, k).wait_recv()
            rows = pl.ds(128 * k, 128)
            merged = px[h, to, rows].astype(F32) + rx1[h, k].astype(F32)
            px[h, to, rows] = merged.astype(BF)
            x_second(h, k).start()

    def x_sum(h):
        total = px[h, x].astype(F32)
        for _, k in sides:
            x_second(h, k).wait_recv()
            total += rx2[h, k].astype(F32)
        s1[pl.ds(4 * h, 4)] = total.astype(BF).reshape(4, NY, MINE, 256)

    def y_copy(h, d):
        to = lax.rem(y + d, NY)
        return pltpu.make_async_remote_copy(
            src_ref=s1.at[pl.ds(4 * h, 4), to],
            dst_ref=ry.at[h, d - 1],
            send_sem=ry_send.at[h, d - 1],
            recv_sem=ry_recv.at[h, d - 1],
            device_id={Y: to},
            device_id_type=MESH,
        )

    def y_sum(h):
        total = s1[pl.ds(4 * h, 4), y].astype(F32)
        for d in range(1, NY):
            y_copy(h, d).wait_recv()
            total += ry[h, d - 1].astype(F32)
        s2[pl.ds(4 * h, 4)] = total.astype(BF)

    def z_copy(d):
        to = lax.rem(z + d, NZ)
        return pltpu.make_async_remote_copy(
            src_ref=s2.at[to],
            dst_ref=rz.at[d - 1],
            send_sem=rz_send.at[d - 1],
            recv_sem=rz_recv.at[d - 1],
            device_id={Z: to},
            device_id_type=MESH,
        )

    def sum_copy(d):
        return pltpu.make_async_remote_copy(
            src_ref=sp_out,
            dst_ref=sp.at[c, x],
            send_sem=sp_send.at[d],
            recv_sem=sp_recv.at[c, x],
            device_id={X: lax.rem(x + d, NX), C: 1},
            device_id_type=MESH,
        )

    outs = []

    def put(number, src, dst):
        cp = pltpu.make_async_copy(src, dst, out_sem.at[number])
        cp.start()
        outs.append(cp)

    @leads
    def _():
        for n in range(1, HOPS + 1):
            arrivals(fg[:2], n)
            if n > 1:
                arrivals(fg[2:], n - 1)

    @follows
    def _():
        for g in fg[:2]:
            g.given()

    act_load.wait()
    for w in cot_loads:
        w.wait()
    for k in range(2):
        cot_copy(attn_out, k).wait_recv()
    project(0)
    for k in range(2):
        x_first(0, k).start()

    @leads
    def _():
        for k in range(2):
            own_weights(k).wait_recv()
        for g in wg:
            g.start()
        arrivals(fg[2:], HOPS)

    @follows
    def _():
        for g in fg[2:]:
            g.given()

    def weights(n):
        @leads
        def _():
            arrivals(wg, n)

    project(1)
    put(0, gf, gf_out)
    x_merge(0)
    for k in range(2):
        x_first(1, k).start()
    weights(1)
    x_sum(0)
    for d in range(1, NY):
        y_copy(0, d).start()
    x_merge(1)
    weights(2)
    x_sum(1)
    for d in range(1, NY):
        y_copy(1, d).start()
    y_sum(0)
    weights(3)
    y_sum(1)
    for d in range(1, NZ):
        z_copy(d).start()
    weights(4)
    total = s2[z].astype(F32)
    for d in range(1, NZ):
        z_copy(d).wait_recv()
        total += rz[d - 1].astype(F32)

    sp_out[...] = total

    @leads
    def _():
        sp[1, x] = total

    @follows
    def _():
        sum_copy(0).start()

    for d in range(1, NX):
        sum_copy(d).start()
    weights(5)

    def sums_here(t, q):
        pltpu.make_async_remote_copy(
            src_ref=sp_out,
            dst_ref=sp.at[t, q],
            send_sem=sp_send.at[0],
            recv_sem=sp_recv.at[t, q],
            device_id={C: other},
            device_id_type=MESH,
        ).wait_recv()

    def moments_over(k):
        return pltpu.make_async_remote_copy(
            src_ref=nm.at[k, 0],
            dst_ref=nm_out.at[k],
            send_sem=nm_sem.at[0, k],
            recv_sem=nm_sem.at[1, k],
            device_id={C: 0},
            device_id_type=MESH,
        )

    def own_dirs(t):
        return dg[t].give(gd.at[t, f, 0])

    @leads
    def _():
        for k, m in enumerate(all_moments):
            own_moments(k, m).wait_recv()
            pltpu.make_async_copy(m, moments.at[k, 1], load.at[13 + k]).wait()
        for q in range(NX):
            sums_here(0, q)

            @pl.when(q != x)
            def _():
                sums_here(1, q)

        for t in range(2):
            for p in range(2):
                proj = jnp.concatenate([sp[t, 2 * p], sp[t, 2 * p + 1]], axis=1)
                proj = proj * (1.0 / math.sqrt(TOKENS))
                first = 0.8 * moments[2 * t, p] + 0.2 * proj
                second = 0.9 * moments[2 * t + 1, p] + 0.1 * proj * proj
                nm[2 * t, p] = first
                nm[2 * t + 1, p] = second
                gd[t, f, p] = (first / jnp.sqrt(second)).astype(BF)
            dg[t].start()
            own_dirs(t).start()
        for k in range(4):
            moments_over(k).start()
            pltpu.make_async_copy(nm.at[k, 1], nm_out.at[k], out_sem.at[4 + k]).start()

    weights(HOPS)

    @follows
    def _():
        for g in wg:
            g.given()

    for k in range(2):
        put(1 + k, gw.at[k, :, c], gw_out.at[k])

    @leads
    def _():
        for n in range(1, HOPS + 1):
            arrivals(dg, n)
        squares = jnp.zeros((8, 128), F32)

        def add(i, squares):
            part = jnp.square(gd[:, i].astype(F32)).reshape(2 * 2 * MINE // 8, 8, 4, 128)
            return squares + jnp.sum(jnp.sum(part, axis=0), axis=1)

        squares = lax.fori_loop(0, NF, add, squares)
        sq[...] = jnp.broadcast_to(jnp.sum(squares, axis=(0, 1), keepdims=True), (8, 128))

    squares_over = pltpu.make_async_remote_copy(
        src_ref=sq,
        dst_ref=sq,
        send_sem=sq_sem.at[0],
        recv_sem=sq_sem.at[1],
        device_id={C: 0},
        device_id_type=MESH,
    )

    @leads
    def _():
        squares_over.start()

    @follows
    def _():
        for t in range(2):
            dg[t].given()

    for k in range(2):
        pltpu.make_async_copy(gd.at[k, :, c], gd_out.at[k], out_sem.at[8 + k]).start()

    @follows
    def _():
        squares_over.wait_recv()

    put(3, sq, sq_out)

    @leads
    def _():
        for g in fg + wg + dg:
            g.finish()
        for k in range(4):
            moments_over(k).wait_send()
            pltpu.make_async_copy(nm.at[k, 1], nm_out.at[k], out_sem.at[4 + k]).wait()
        squares_over.wait_send()

    @follows
    def _():
        for k in range(2):
            own_weights(k).wait_send()
        for k, m in enumerate(all_moments):
            own_moments(k, m).wait_send()
            moments_over(k).wait_recv()
        sum_copy(0).wait_send()

    for k in range(2):
        cot_copy(attn_out, k).wait_send()
        for h in range(2):
            x_first(h, k).wait_send()
            x_second(h, k).wait_send()
    for h in range(2):
        for d in range(1, NY):
            y_copy(h, d).wait_send()
    for d in range(1, NZ):
        z_copy(d).wait_send()
    for d in range(1, NX):
        sum_copy(d).wait_send()
    for cp in outs:
        cp.wait()
    for k in range(2):
        pltpu.make_async_copy(gd.at[k, :, c], gd_out.at[k], out_sem.at[8 + k]).wait()


def update_kernel(
    gf, gw, gd, nm, sq, query_factor, out_factor, query_w, out_w,
    new_qw, new_ow, q_step, o_step, nf_q, ns_q, nf_o, ns_o, q_copy, o_copy,
):
    inverse = 1.0 / jnp.sqrt(sq[0:1] / (2 * RANK * HQ) + 1e-06)
    inverse = jnp.concatenate([inverse] * 4, axis=1)
    moved = []
    for t in range(2):
        rows = jnp.concatenate([gf[j, :, t].reshape(-1, 128) for j in range(4)], axis=1)
        step = jnp.dot(rows, gd[t].reshape(RANK, HALF), preferred_element_type=F32)
        old = jnp.concatenate([gw[k, :, t].reshape(-1, 256) for k in range(2)], axis=1)
        moved.append(old.astype(F32) - (0.01 * inverse) * step)
    q_copy[...] = moved[0].astype(BF)
    o_copy[...] = moved[1].T.astype(BF)

    @pl.when(pl.program_id(0) == 0)
    def _():
        for k, out in enumerate((nf_q, ns_q, nf_o, ns_o)):
            out[...] = nm[k]
        for t, factor, w, to_step, to_w in (
            (0, query_factor, query_w, q_step, new_qw),
            (1, out_factor, out_w, o_step, new_ow),
        ):
            step = jnp.dot(factor[...], gd[t].reshape(RANK, HALF), preferred_element_type=F32)
            step = step * inverse
            to_step[...] = step
            to_w[...] = w[...] - 0.01 * step


def body(
    input_act, query_cot, out_cot, attn_out, query_w, out_w, query_factor, out_factor,
    first_q, second_q, first_o, second_o,
):
    struct = jax.ShapeDtypeStruct
    dma = pltpu.SemaphoreType.DMA
    vmem = pltpu.VMEM
    out_w = out_w.T
    scratch = [
        vmem((4, NF, 2, ROWS, 128), BF),
        vmem((2, NF, 2, 2, ROWS, 256), BF),
        vmem((2, NF, 2, MINE, HALF), BF),
        vmem((TOK, D), BF),
        vmem((4, TOK, 256), BF),
        vmem((ROWS, HALF), F32),
        vmem((ROWS, HALF), F32),
        vmem((4, 2, MINE, HALF), F32),
        vmem((TOK, 256), BF),
        vmem((TOK, 256), BF),
        vmem((2, NX, 256, 256), BF),
        vmem((2, 2, 128, 256), BF),
        vmem((2, 2, 256, 256), BF),
        vmem((NZ, NY, MINE, 256), BF),
        vmem((2, NY - 1, 4, MINE, 256), BF),
        vmem((NZ, MINE, 256), BF),
        vmem((NZ - 1, MINE, 256), BF),
        vmem((2, NX, MINE, 256), F32),
        vmem((MINE, 256), F32),
        vmem((8, 128), F32),
        vmem((4, 2, MINE, HALF), F32),
        dma((17,)),
        dma((4,)), dma((4, PIECES)), dma((4,)), dma((4,)),
        dma((2,)), dma((2, PIECES)), dma((2,)), dma((2,)),
        dma((2,)), dma((2, PIECES)), dma((2,)), dma((2,)),
        dma((2,)), dma((2,)),
        dma((4,)), dma((4,)),
        dma((2,)), dma((2,)),
        dma((2, 2)), dma((2, 2)), dma((2, 2)), dma((2, 2)),
        dma((2, NY - 1)), dma((2, NY - 1)),
        dma((NZ - 1,)), dma((NZ - 1,)),
        dma((NX,)), dma((2, NX)),
        dma((2, 4)), dma((2,)), dma((10,)),
    ]
    gf, gw, gd, nm, sq = pl.pallas_call(
        reduce_kernel,
        out_shape=(
            struct((4, NF, 2, ROWS, 128), BF),
            struct((2, NF, 2, ROWS, 256), BF),
            struct((2, NF, MINE, HALF), BF),
            struct((4, MINE, HALF), F32),
            struct((8, 128), F32),
        ),
        in_specs=[pl.BlockSpec(memory_space=pl.ANY)] * 12,
        out_specs=[pl.BlockSpec(memory_space=pl.ANY)] * 5,
        scratch_shapes=scratch,
        compiler_params=pltpu.CompilerParams(
            collective_id=0, has_side_effects=True, vmem_limit_bytes=56 * 1024 * 1024
        ),
        name="reduce",
    )(
        input_act, query_cot, out_cot, attn_out, query_w, out_w, query_factor, out_factor,
        first_q, second_q, first_o, second_o,
    )

    def whole(*shape):
        return pl.BlockSpec(shape, lambda b: (0,) * len(shape))

    per = NF // BLOCKS
    shard, small = struct((ROWS, HALF), F32), struct((MINE, HALF), F32)
    outs = pl.pallas_call(
        update_kernel,
        grid=(BLOCKS,),
        out_shape=(
            *[shard] * 4,
            *[small] * 4,
            struct((D, HALF), BF),
            struct((HALF, D), BF),
        ),
        in_specs=[
            pl.BlockSpec((4, per, 2, ROWS, 128), lambda b: (0, b, 0, 0, 0)),
            pl.BlockSpec((2, per, 2, ROWS, 256), lambda b: (0, b, 0, 0, 0)),
            whole(2, NF, MINE, HALF),
            whole(4, MINE, HALF),
            whole(8, 128),
            whole(ROWS, RANK),
            whole(ROWS, RANK),
            whole(ROWS, HALF),
            whole(ROWS, HALF),
        ],
        out_specs=[
            *[whole(ROWS, HALF)] * 4,
            *[whole(MINE, HALF)] * 4,
            pl.BlockSpec((D // BLOCKS, HALF), lambda b: (b, 0)),
            pl.BlockSpec((HALF, D // BLOCKS), lambda b: (0, b)),
        ],
        compiler_params=pltpu.CompilerParams(dimension_semantics=("arbitrary",)),
        name="update",
    )(gf, gw, gd, nm, sq, query_factor, out_factor, query_w, out_w)
    outs = list(outs)
    outs[1], outs[3] = outs[1].T, outs[3].T
    return tuple(outs)


def solution(mesh):
    finer = Mesh(mesh.devices.reshape(NZ, NY, NX, 2), (Z, Y, X, C))
    in_specs = (
        P(FS_REP, None),
        P(FS_REP, C),
        P(FS_REP, None),
        P(FS_REP, C),
        P(FS, C),
        P(C, FS),
        P(FS, None),
        P(FS, None),
        *[P(FS, C)] * 4,
    )
    out_specs = (
        P(FS, C),
        P(C, FS),
        P(FS, C),
        P(C, FS),
        *[P(FS, C)] * 4,
        P(None, C),
        P(C, None),
    )
    return jax.shard_map(body, mesh=finer, in_specs=in_specs, out_specs=out_specs, check_vma=False)
```

```python
import math

import jax
import jax.numpy as jnp
from jax import lax
from jax.experimental import pallas as pl
from jax.experimental.pallas import tpu as pltpu
from jax.sharding import Mesh
from jax.sharding import PartitionSpec as P

NZ, NY, NX = 8, 4, 4
NF = NZ * NY
D, RANK, HQ, TOKENS = 2048, 512, 1024, 98304
HALF = HQ // 2
TOK = TOKENS // (NF * NX)
ROWS = D // NF
MINE = RANK // NF
BLOCKS = 8
Z, Y, X, C = "fs_0", "fs_1", "rep", "tp"
FS = (Z, Y)
FS_REP = (Z, Y, X)
BF, F32 = jnp.bfloat16, jnp.float32
MESH = pl.DeviceIdType.MESH


def reach(n, flip):
    far = (n // 2, n - 1 - n // 2)
    return far[::-1] if flip else far


def ring_plan(axes, sizes, flip):
    first = reach(sizes[0], flip)
    events = []
    for i in range(-first[1], first[0] + 1):
        second = reach(sizes[1], (i + flip) % 2)
        for j in range(-second[1], second[0] + 1):
            on = []
            if j == 0:
                for s, far in ((1, first[0]), (-1, first[1])):
                    if i * s >= 0 and abs(i) < far:
                        on.append((axes[0], s, (i + s, 0)))
                on += [(axes[1], s, (i, s)) for s in (1, -1)]
            else:
                s = 1 if j > 0 else -1
                if abs(j) < second[0 if s > 0 else 1]:
                    on.append((axes[1], s, (i, j + s)))
            events.append((abs(i) + abs(j), (i, j), on))
    events.sort(key=lambda e: e[0])
    slots = {e[1]: n for n, e in enumerate(events[1:])}
    return dict(axes=axes, events=events, slots=slots)


class Gather:
    def __init__(self, plan, piece, share, where, send_sem, recv_sem, pass_sem, give_sem, core=0, own=0):
        self.core = core
        self.shares = pl.ds(0, PIECES + own)
        self.plan, self.piece, self.share, self.where = plan, piece, share, where
        self.send_sem, self.recv_sem = send_sem, recv_sem
        self.pass_sem, self.give_sem = pass_sem, give_sem

    def index(self, key):
        off = dict(zip(self.plan["axes"], key))
        z = lax.rem(self.where[Z] + (NZ - off[Z]), NZ)
        y = lax.rem(self.where[Y] + (NY - off[Y]), NY)
        return z * NY + y

    def copy(self, ref, axis, sign, slot):
        n = NZ if axis == Z else NY
        return pltpu.make_async_remote_copy(
            src_ref=ref,
            dst_ref=ref,
            send_sem=self.send_sem,
            recv_sem=self.recv_sem.at[slot],
            device_id={axis: lax.rem(self.where[axis] + (n + sign), n)},
            device_id_type=MESH,
        )

    def give(self, ref):
        return pltpu.make_async_remote_copy(
            src_ref=ref,
            dst_ref=ref,
            send_sem=self.pass_sem,
            recv_sem=self.give_sem,
            device_id={C: self.core},
            device_id_type=MESH,
        )

    def pass_on(self, event):
        ref = self.piece(self.index(event[1]))
        for axis, sign, landed in event[2]:
            self.copy(ref, axis, sign, self.plan["slots"][landed]).start()

    def start(self):
        self.pass_on(self.plan["events"][0])

    def arrive(self, event):
        f = self.index(event[1])
        self.copy(self.piece(f), self.plan["axes"][0], 1, self.plan["slots"][event[1]]).wait_recv()
        self.pass_on(event)
        self.give(self.share(f)).start()

    def hops(self, number):
        return [(self, e) for e in self.plan["events"] if e[0] == number]

    def finish(self):
        self.copy(self.piece(pl.ds(0, PIECES)), Z, 1, 0).wait_send()
        self.give(self.share(self.shares)).wait_send()

    def given(self):
        self.give(self.share(self.shares)).wait_recv()


ZY = ring_plan((Z, Y), (NZ, NY), 0)
YZ = ring_plan((Y, Z), (NY, NZ), 0)
PIECES = NF - 1
HOPS = ZY["events"][-1][0]


def arrivals(gathers, number):
    todo = [g.hops(number) for g in gathers]
    for k in range(max(len(t) for t in todo)):
        for t in todo:
            if k < len(t):
                t[k][0].arrive(t[k][1])


def reduce_kernel(*refs):
    (
        input_act, query_cot, out_cot, attn_out, query_w, out_w, query_factor, out_factor,
        first_q, second_q, first_o, second_o,
        gf_out, gw_out, gd_out, nm_out, sq_out,
        gf, gw, gd, act, cot, qw, ow, moments, low_hi, low_lo, px, rx1, rx2, s1, ry, s2,
        rz, sp, sq, nm,
        load, f_send, f_recv, f_pass, f_give, w_send, w_recv, w_pass, w_give,
        d_send, d_recv, d_pass, d_give, own_send, own_recv, mom_send, mom_recv,
        cot_send, cot_recv, px_send, px_recv,
        rx1_send, rx1_recv, rx2_send, rx2_recv, ry_send, ry_recv, rz_send, rz_recv,
        sp_send, sp_recv, nm_sem, sq_sem, out_sem,
    ) = refs
    z, y, x, c = (lax.axis_index(a) for a in (Z, Y, X, C))
    f = z * NY + y
    where = {Z: z, Y: y}
    other = 1 - c
    leads, follows = pl.when(c == 1), pl.when(c == 0)

    def load_own(number, if_q, if_o, dst):
        @follows
        def _():
            pltpu.make_async_copy(if_q, dst, load.at[number]).start()

        @leads
        def _():
            pltpu.make_async_copy(if_o, dst, load.at[number]).start()

        return pltpu.make_async_copy(if_q, dst, load.at[number])

    def load_plain(number, src, dst):
        cp = pltpu.make_async_copy(src, dst, load.at[number])
        cp.start()
        return cp

    fac = []
    for j in range(4):
        cols = pl.ds(128 * j, 128)
        for t, factor in enumerate((query_factor, out_factor)):
            fac.append(load_plain(2 * j + t, factor.at[:, cols], gf.at[j, f, t]))
    w_loads = [load_plain(8, query_w, qw), load_plain(9, out_w, ow)]
    act_load = load_own(10, input_act, out_cot, act)
    cot_loads = []
    for k in range(2):
        cols = pl.ds(256 * k, 256)
        cot_loads.append(
            load_own(11 + k, query_cot.at[:, cols], attn_out.at[:, cols], cot.at[2 * c + k])
        )

    barrier = pltpu.get_barrier_semaphore()
    peers = [{C: other}]
    for axis, at, n in ((Z, z, NZ), (Y, y, NY), (X, x, NX)):
        peers += [{axis: lax.rem(at + 1, n)}, {axis: lax.rem(at + n - 1, n)}]
    for peer in peers:
        pl.semaphore_signal(barrier, inc=1, device_id=peer, device_id_type=MESH)

    for w in w_loads:
        w.wait()
    for k in range(2):
        gw[k, f, c, 0] = qw[:, 256 * k : 256 * k + 256].astype(BF)
        gw[k, f, c, 1] = ow[:, 256 * k : 256 * k + 256].astype(BF)
    for w in fac:
        w.wait()
    pl.semaphore_wait(barrier, len(peers))

    fg = [
        Gather(
            ZY if j % 2 == 0 else YZ,
            lambda p, j=j: gf.at[j, p],
            lambda p, j=j: gf.at[j, p],
            where, f_send.at[j], f_recv.at[j], f_pass.at[j], f_give.at[j],
        )
        for j in range(4)
    ]
    wg = [
        Gather(
            ZY if k == 0 else YZ,
            lambda p, k=k: gw.at[k, p],
            lambda p, k=k: gw.at[k, p, 1],
            where, w_send.at[k], w_recv.at[k], w_pass.at[k], w_give.at[k], 1,
        )
        for k in range(2)
    ]
    dg = [
        Gather(
            ZY if k == 0 else YZ,
            lambda p, k=k: gd.at[k, p],
            lambda p, k=k: gd.at[k, p, 0],
            where, d_send.at[k], d_recv.at[k], d_pass.at[k], d_give.at[k], 0, 1,
        )
        for k in range(2)
    ]

    @leads
    def _():
        for g in fg:
            g.start()

    def cot_copy(src, k):
        return pltpu.make_async_remote_copy(
            src_ref=src.at[:, pl.ds(256 * k, 256)],
            dst_ref=cot.at[2 * c + k],
            send_sem=cot_send.at[k],
            recv_sem=cot_recv.at[k],
            device_id={C: other},
            device_id_type=MESH,
        )

    def own_weights(k):
        ref = gw.at[k, f, 1]
        return pltpu.make_async_remote_copy(
            src_ref=ref,
            dst_ref=ref,
            send_sem=own_send.at[k],
            recv_sem=own_recv.at[k],
            device_id={C: 0},
            device_id_type=MESH,
        )

    def own_moments(k, m):
        return pltpu.make_async_remote_copy(
            src_ref=m,
            dst_ref=moments.at[k, 0],
            send_sem=mom_send.at[k],
            recv_sem=mom_recv.at[k],
            device_id={C: 1},
            device_id_type=MESH,
        )

    all_moments = (first_q, second_q, first_o, second_o)

    @follows
    def _():
        for k in range(2):
            cot_copy(attn_out, k).start()
        for k, m in enumerate(all_moments):
            own_moments(k, m).start()

    @leads
    def _():
        for k in range(2):
            cot_copy(query_cot, k).start()
        for k in range(2):
            own_weights(k).start()
        for k, m in enumerate(all_moments):
            pltpu.make_async_copy(m, moments.at[k, 1], load.at[13 + k]).start()

    def project(h):
        def tile(m, _):
            rows = pl.ds(pl.multiple_of(m * 256, 256), 256)
            right = jnp.concatenate(
                [gf[2 * h + j, :, c].reshape(D, 128) for j in range(2)], axis=1
            )
            low = jnp.dot(act[rows, :], right, preferred_element_type=F32)
            hi = low.astype(BF)
            low_hi[rows, :] = hi
            low_lo[rows, :] = (low - hi.astype(F32)).astype(BF)
            return 0

        lax.fori_loop(0, TOK // 256, tile, 0)

        def quarter(i, _):
            xb = lax.rem(x + 2 + i, NX)
            side = cot[xb]
            dims = (((0,), (0,)), ((), ()))
            total = lax.dot_general(low_hi[...], side, dims, preferred_element_type=F32)
            total += lax.dot_general(low_lo[...], side, dims, preferred_element_type=F32)
            px[h, xb, c] = total.astype(BF)
            return 0

        lax.fori_loop(0, NX, quarter, 0)

    x_up, x_down, x_far = lax.rem(x + 1, NX), lax.rem(x + 3, NX), lax.rem(x + 2, NX)
    sides = ((x_up, 0), (x_down, 1))

    def partial_over(h, i):
        ref = px.at[h, lax.rem(x + 2 + i, NX), 0]
        return pltpu.make_async_remote_copy(
            src_ref=ref,
            dst_ref=ref,
            send_sem=px_send.at[h, i],
            recv_sem=px_recv.at[h, i],
            device_id={C: 1},
            device_id_type=MESH,
        )

    def x_first(h, k):
        return pltpu.make_async_remote_copy(
            src_ref=px.at[h, x_far, :, pl.ds(128 * k, 128)],
            dst_ref=rx1.at[h, k],
            send_sem=rx1_send.at[h, k],
            recv_sem=rx1_recv.at[h, k],
            device_id={X: sides[k][0]},
            device_id_type=MESH,
        )

    def x_second(h, k):
        return pltpu.make_async_remote_copy(
            src_ref=px.at[h, sides[k][0]],
            dst_ref=rx2.at[h, k],
            send_sem=rx2_send.at[h, k],
            recv_sem=rx2_recv.at[h, k],
            device_id={X: sides[k][0]},
            device_id_type=MESH,
        )

    def x_start(h):
        partial_over(h, 0).wait_recv()
        for k in range(2):
            x_first(h, k).start()

    def x_merge(h):
        for i in (1, 3):
            partial_over(h, i).wait_recv()
        for to, k in sides:
            x_first(h, k).wait_recv()
            rows = pl.ds(128 * k, 128)
            merged = px[h, to, :, rows].astype(F32) + rx1[h, k].astype(F32)
            px[h, to, :, rows] = merged.astype(BF)
            x_second(h, k).start()

    def x_sum(h):
        partial_over(h, 2).wait_recv()
        for _, k in sides:
            x_second(h, k).wait_recv()
        for t in range(2):
            total = px[h, x, t].astype(F32)
            for k in range(2):
                total += rx2[h, k, t].astype(F32)
            s1[pl.ds(4 * h, 4), :, t] = total.astype(BF).reshape(4, NY, MINE, 256)
        for d in range(1, NY):
            y_copy(h, d).start()

    def y_copy(h, d):
        to = lax.rem(y + d, NY)
        return pltpu.make_async_remote_copy(
            src_ref=s1.at[pl.ds(4 * h, 4), to],
            dst_ref=ry.at[h, d - 1],
            send_sem=ry_send.at[h, d - 1],
            recv_sem=ry_recv.at[h, d - 1],
            device_id={Y: to},
            device_id_type=MESH,
        )

    def y_sum(h):
        total = s1[pl.ds(4 * h, 4), y].astype(F32)
        for d in range(1, NY):
            y_copy(h, d).wait_recv()
            total += ry[h, d - 1].astype(F32)
        s2[pl.ds(4 * h, 4)] = total.astype(BF)

    def z_copy(d):
        to = lax.rem(z + d, NZ)
        return pltpu.make_async_remote_copy(
            src_ref=s2.at[to],
            dst_ref=rz.at[d - 1],
            send_sem=rz_send.at[d - 1],
            recv_sem=rz_recv.at[d - 1],
            device_id={Z: to},
            device_id_type=MESH,
        )

    def sum_copy(d):
        return pltpu.make_async_remote_copy(
            src_ref=sp.at[0],
            dst_ref=sp.at[d],
            send_sem=sp_send.at[d - 1],
            recv_sem=sp_recv.at[d - 1],
            device_id={X: lax.rem(x + d, NX)},
            device_id_type=MESH,
        )

    def moments_over(k):
        return pltpu.make_async_remote_copy(
            src_ref=nm.at[k, 0],
            dst_ref=nm_out.at[k],
            send_sem=nm_sem.at[0, k],
            recv_sem=nm_sem.at[1, k],
            device_id={C: 0},
            device_id_type=MESH,
        )

    def own_dirs(t):
        return dg[t].give(gd.at[t, f, 0])

    outs = []

    def put(number, src, dst):
        cp = pltpu.make_async_copy(src, dst, out_sem.at[number])
        cp.start()
        outs.append(cp)

    @leads
    def _():
        for n in range(1, HOPS + 1):
            arrivals(fg[:2], n)
            if n > 1:
                arrivals(fg[2:], n - 1)

    @follows
    def _():
        for g in fg[:2]:
            g.given()
        for k in range(2):
            own_weights(k).wait_recv()
        for g in wg:
            g.start()

    act_load.wait()
    for w in cot_loads:
        w.wait()
    for k in range(2):
        cot_copy(attn_out, k).wait_recv()
    project(0)

    @leads
    def _():
        x_start(0)
        arrivals(fg[2:], HOPS)

    @follows
    def _():
        for i in range(NX):
            partial_over(0, i).start()
        arrivals(wg, 1)
        for g in fg[2:]:
            g.given()

    project(1)
    put(0, gf, gf_out)

    @leads
    def _():
        x_merge(0)
        x_start(1)
        x_sum(0)
        x_merge(1)
        y_sum(0)
        x_sum(1)
        y_sum(1)
        for d in range(1, NZ):
            z_copy(d).start()
        total = s2[z].astype(F32)
        for d in range(1, NZ):
            z_copy(d).wait_recv()
            total += rz[d - 1].astype(F32)
        sp[0] = total
        for d in range(1, NX):
            sum_copy(d).start()
        for k, m in enumerate(all_moments):
            own_moments(k, m).wait_recv()
            pltpu.make_async_copy(m, moments.at[k, 1], load.at[13 + k]).wait()
        for d in range(1, NX):
            sum_copy(d).wait_recv()

        for t in range(2):
            for p in range(2):
                proj = jnp.concatenate(
                    [sp[lax.rem(x + (NX - q), NX), t] for q in (2 * p, 2 * p + 1)], axis=1
                )
                proj = proj * (1.0 / math.sqrt(TOKENS))
                first = 0.8 * moments[2 * t, p] + 0.2 * proj
                second = 0.9 * moments[2 * t + 1, p] + 0.1 * proj * proj
                nm[2 * t, p] = first
                nm[2 * t + 1, p] = second
                gd[t, f, p] = (first / jnp.sqrt(second)).astype(BF)
            dg[t].start()
            own_dirs(t).start()
        for k in range(4):
            moments_over(k).start()
            pltpu.make_async_copy(nm.at[k, 1], nm_out.at[k], out_sem.at[4 + k]).start()
        for n in range(1, HOPS + 1):
            arrivals(dg, n)
        for g in wg:
            g.given()

    @follows
    def _():
        for i in range(NX):
            partial_over(1, i).start()
        for n in range(2, HOPS + 1):
            arrivals(wg, n)

    for k in range(2):
        put(1 + k, gw.at[k, :, c], gw_out.at[k])

    @leads
    def _():
        squares = jnp.zeros((8, 128), F32)

        def add(i, squares):
            part = jnp.square(gd[:, i].astype(F32)).reshape(2 * 2 * MINE // 8, 8, 4, 128)
            return squares + jnp.sum(jnp.sum(part, axis=0), axis=1)

        squares = lax.fori_loop(0, NF, add, squares)
        sq[...] = jnp.broadcast_to(jnp.sum(squares, axis=(0, 1), keepdims=True), (8, 128))

    squares_over = pltpu.make_async_remote_copy(
        src_ref=sq,
        dst_ref=sq,
        send_sem=sq_sem.at[0],
        recv_sem=sq_sem.at[1],
        device_id={C: 0},
        device_id_type=MESH,
    )

    @leads
    def _():
        squares_over.start()

    @follows
    def _():
        for t in range(2):
            dg[t].given()

    for k in range(2):
        pltpu.make_async_copy(gd.at[k, :, c], gd_out.at[k], out_sem.at[8 + k]).start()

    @follows
    def _():
        squares_over.wait_recv()

    put(3, sq, sq_out)

    @leads
    def _():
        for g in fg + dg:
            g.finish()
        for k in range(2):
            own_weights(k).wait_send()
        for h in range(2):
            for k in range(2):
                x_first(h, k).wait_send()
                x_second(h, k).wait_send()
            for d in range(1, NY):
                y_copy(h, d).wait_send()
        for d in range(1, NZ):
            z_copy(d).wait_send()
        for d in range(1, NX):
            sum_copy(d).wait_send()
        for k in range(4):
            moments_over(k).wait_send()
            pltpu.make_async_copy(nm.at[k, 1], nm_out.at[k], out_sem.at[4 + k]).wait()
        squares_over.wait_send()

    @follows
    def _():
        for g in wg:
            g.finish()
        for k, m in enumerate(all_moments):
            own_moments(k, m).wait_send()
            moments_over(k).wait_recv()
        for h in range(2):
            for i in range(NX):
                partial_over(h, i).wait_send()

    for k in range(2):
        cot_copy(attn_out, k).wait_send()
    for cp in outs:
        cp.wait()
    for k in range(2):
        pltpu.make_async_copy(gd.at[k, :, c], gd_out.at[k], out_sem.at[8 + k]).wait()


def update_kernel(
    gf_in, gw_in, gd_in, nm_in, sq_in, query_factor, out_factor, query_w, out_w,
    new_qw, new_ow, q_step, o_step, nf_q, ns_q, nf_o, ns_o, q_copy, o_copy,
    gf, gw, gd, nm, sq, factor, w, steps, new_w, new_q, new_o,
    first_sem, block_sem, small_sem, copy_sem, out_sem,
):
    copy = pltpu.make_async_copy
    per = NF // BLOCKS
    size = D // BLOCKS
    first = [copy(gd_in, gd, first_sem.at[0]), copy(sq_in, sq, first_sem.at[1])]
    small = [copy(nm_in, nm, small_sem.at[0])]
    for t, (fac, old) in enumerate(((query_factor, query_w), (out_factor, out_w))):
        small.append(copy(fac, factor.at[t], small_sem.at[1 + 2 * t]))
        small.append(copy(old, w.at[t], small_sem.at[2 + 2 * t]))

    def block_loads(b):
        some = pl.ds(per * b, per)
        return (
            copy(gf_in.at[:, some], gf.at[:, some], block_sem.at[0, b]),
            copy(gw_in.at[:, some], gw.at[:, some], block_sem.at[1, b]),
        )

    def block_stores(b):
        at = pl.ds(pl.multiple_of(size * b, size), size)
        return (
            copy(new_q.at[b], q_copy.at[at], copy_sem.at[0, b]),
            copy(new_o.at[b], o_copy.at[:, at], copy_sem.at[1, b]),
        )

    for cp in first + small:
        cp.start()
    for b in range(BLOCKS):
        for cp in block_loads(b):
            cp.start()
    for cp in first:
        cp.wait()
    inverse = 1.0 / jnp.sqrt(sq[0:1] / (2 * RANK * HQ) + 1e-06)
    inverse = jnp.concatenate([inverse] * 4, axis=1)
    for cp in small:
        cp.wait()
    stores = [copy(nm.at[k], o, out_sem.at[k]) for k, o in enumerate((nf_q, ns_q, nf_o, ns_o))]
    for t, (to_step, to_w) in enumerate(((q_step, new_qw), (o_step, new_ow))):
        step = jnp.dot(factor[t], gd[t].reshape(RANK, HALF), preferred_element_type=F32)
        step = step * inverse
        steps[t] = step
        new_w[t] = w[t] - 0.01 * step
        stores.append(copy(steps.at[t], to_step, out_sem.at[4 + 2 * t]))
        stores.append(copy(new_w.at[t], to_w, out_sem.at[5 + 2 * t]))
    for cp in stores:
        cp.start()

    def block(b, _):
        some = pl.ds(per * b, per)
        for cp in block_loads(b):
            cp.wait()
        moved = []
        for t in range(2):
            rows = jnp.concatenate([gf[j, some, t].reshape(size, 128) for j in range(4)], axis=1)
            step = jnp.dot(rows, gd[t].reshape(RANK, HALF), preferred_element_type=F32)
            old = jnp.concatenate([gw[k, some, t].reshape(size, 256) for k in range(2)], axis=1)
            moved.append(old.astype(F32) - (0.01 * inverse) * step)
        new_q[b] = moved[0].astype(BF)
        new_o[b] = moved[1].T.astype(BF)
        for cp in block_stores(b):
            cp.start()
        return 0

    lax.fori_loop(0, BLOCKS, block, 0)
    for cp in stores:
        cp.wait()
    for b in range(BLOCKS):
        for cp in block_stores(b):
            cp.wait()


def body(
    input_act, query_cot, out_cot, attn_out, query_w, out_w, query_factor, out_factor,
    first_q, second_q, first_o, second_o,
):
    struct = jax.ShapeDtypeStruct
    dma = pltpu.SemaphoreType.DMA
    vmem = pltpu.VMEM
    out_w = out_w.T
    scratch = [
        vmem((4, NF, 2, ROWS, 128), BF),
        vmem((2, NF, 2, 2, ROWS, 256), BF),
        vmem((2, NF, 2, MINE, HALF), BF),
        vmem((TOK, D), BF),
        vmem((4, TOK, 256), BF),
        vmem((ROWS, HALF), F32),
        vmem((ROWS, HALF), F32),
        vmem((4, 2, MINE, HALF), F32),
        vmem((TOK, 256), BF),
        vmem((TOK, 256), BF),
        vmem((2, NX, 2, 256, 256), BF),
        vmem((2, 2, 2, 128, 256), BF),
        vmem((2, 2, 2, 256, 256), BF),
        vmem((NZ, NY, 2, MINE, 256), BF),
        vmem((2, NY - 1, 4, 2, MINE, 256), BF),
        vmem((NZ, 2, MINE, 256), BF),
        vmem((NZ - 1, 2, MINE, 256), BF),
        vmem((NX, 2, MINE, 256), F32),
        vmem((8, 128), F32),
        vmem((4, 2, MINE, HALF), F32),
        dma((17,)),
        dma((4,)), dma((4, PIECES)), dma((4,)), dma((4,)),
        dma((2,)), dma((2, PIECES)), dma((2,)), dma((2,)),
        dma((2,)), dma((2, PIECES)), dma((2,)), dma((2,)),
        dma((2,)), dma((2,)),
        dma((4,)), dma((4,)),
        dma((2,)), dma((2,)),
        dma((2, NX)), dma((2, NX)),
        dma((2, 2)), dma((2, 2)), dma((2, 2)), dma((2, 2)),
        dma((2, NY - 1)), dma((2, NY - 1)),
        dma((NZ - 1,)), dma((NZ - 1,)),
        dma((NX - 1,)), dma((NX - 1,)),
        dma((2, 4)), dma((2,)), dma((10,)),
    ]
    gf, gw, gd, nm, sq = pl.pallas_call(
        reduce_kernel,
        out_shape=(
            struct((4, NF, 2, ROWS, 128), BF),
            struct((2, NF, 2, ROWS, 256), BF),
            struct((2, NF, MINE, HALF), BF),
            struct((4, MINE, HALF), F32),
            struct((8, 128), F32),
        ),
        in_specs=[pl.BlockSpec(memory_space=pl.ANY)] * 12,
        out_specs=[pl.BlockSpec(memory_space=pl.ANY)] * 5,
        scratch_shapes=scratch,
        compiler_params=pltpu.CompilerParams(
            collective_id=0, has_side_effects=True, vmem_limit_bytes=56 * 1024 * 1024
        ),
        name="reduce",
    )(
        input_act, query_cot, out_cot, attn_out, query_w, out_w, query_factor, out_factor,
        first_q, second_q, first_o, second_o,
    )

    anywhere = pl.BlockSpec(memory_space=pl.ANY)
    shard, small = struct((ROWS, HALF), F32), struct((MINE, HALF), F32)
    outs = pl.pallas_call(
        update_kernel,
        out_shape=(
            *[shard] * 4,
            *[small] * 4,
            struct((D, HALF), BF),
            struct((HALF, D), BF),
        ),
        in_specs=[anywhere] * 9,
        out_specs=[anywhere] * 10,
        scratch_shapes=[
            vmem((4, NF, 2, ROWS, 128), BF),
            vmem((2, NF, 2, ROWS, 256), BF),
            vmem((2, NF, MINE, HALF), BF),
            vmem((4, MINE, HALF), F32),
            vmem((8, 128), F32),
            vmem((2, ROWS, RANK), BF),
            vmem((2, ROWS, HALF), F32),
            vmem((2, ROWS, HALF), F32),
            vmem((2, ROWS, HALF), F32),
            vmem((BLOCKS, D // BLOCKS, HALF), BF),
            vmem((BLOCKS, HALF, D // BLOCKS), BF),
            dma((2,)),
            dma((2, BLOCKS)),
            dma((5,)),
            dma((2, BLOCKS)),
            dma((8,)),
        ],
        compiler_params=pltpu.CompilerParams(vmem_limit_bytes=56 * 1024 * 1024),
        name="update",
    )(gf, gw, gd, nm, sq, query_factor, out_factor, query_w, out_w)
    outs = list(outs)
    outs[1], outs[3] = outs[1].T, outs[3].T
    return tuple(outs)


def solution(mesh):
    finer = Mesh(mesh.devices.reshape(NZ, NY, NX, 2), (Z, Y, X, C))
    in_specs = (
        P(FS_REP, None),
        P(FS_REP, C),
        P(FS_REP, None),
        P(FS_REP, C),
        P(FS, C),
        P(C, FS),
        P(FS, None),
        P(FS, None),
        *[P(FS, C)] * 4,
    )
    out_specs = (
        P(FS, C),
        P(C, FS),
        P(FS, C),
        P(C, FS),
        *[P(FS, C)] * 4,
        P(None, C),
        P(C, None),
    )
    return jax.shard_map(body, mesh=finer, in_specs=in_specs, out_specs=out_specs, check_vma=False)
```

```python
import math

import jax
import jax.numpy as jnp
from jax import lax
from jax.experimental import pallas as pl
from jax.experimental.pallas import tpu as pltpu
from jax.sharding import Mesh
from jax.sharding import PartitionSpec as P

NZ, NY, NX = 8, 4, 4
NF = NZ * NY
D, RANK, HQ, TOKENS = 2048, 512, 1024, 98304
HALF = HQ // 2
TOK = TOKENS // (NF * NX)
ROWS = D // NF
MINE = RANK // NF
BLOCKS = 8
Z, Y, X, C = "fs_0", "fs_1", "rep", "tp"
FS = (Z, Y)
FS_REP = (Z, Y, X)
BF, F32 = jnp.bfloat16, jnp.float32
MESH = pl.DeviceIdType.MESH


def along(n, mode, flip):
    up, down = (n // 2, n - 1 - n // 2)[:: -1 if flip else 1]
    tree = {}
    for s, far in ((1, up), (-1, down)):
        if mode == "ring":
            hops = [(k, 1) for k in range(far)]
        elif mode == "direct":
            hops = [(0, k) for k in range(far, 0, -1)]
        else:
            hops = [(0, 2), (0, 1), (2, 2), (2, 1)]
        for at, by in hops:
            if at + by <= far:
                tree.setdefault(s * at, []).append((s, by, s * (at + by)))
    return tree, range(-down, up + 1)


def broadcast(axes, flip):
    (axis_1, mode_1), (axis_2, mode_2) = axes
    sizes = {Z: NZ, Y: NY}
    tree_1, span = along(sizes[axis_1], mode_1, flip)
    events = {}
    for i in span:
        tree_2, across = along(sizes[axis_2], mode_2, (i + flip) % 2)
        for j in across:
            on = [(axis_2, s, d, (i, to)) for s, d, to in tree_2.get(j, [])]
            if j == 0:
                on = [(axis_1, s, d, (to, 0)) for s, d, to in tree_1.get(i, [])] + on
            events[i, j] = on
    return events


def expected_order(gathers):
    free, now, order = {}, 0.0, []
    heap = [(0.01 * g.number, g.number, (0, 0)) for g in gathers]
    by_number = {g.number: g for g in gathers}
    while heap:
        heap.sort()
        when, number, key = heap.pop(0)
        now, g = max(now, when), by_number[number]
        if key != (0, 0):
            order.append((g, key))
        for axis, sign, distance, landed in g.events[key]:
            now += 0.02
            begin = max(free.get((axis, sign), 0.0), now)
            wire = g.kib / 91.0
            free[axis, sign] = begin + wire * distance
            heap.append((begin + wire + 2.0 + 0.75 * (distance - 1), number, landed))
    return order


class Gather:
    def __init__(self, number, axes, flip, kib, pieces, many, share, shares, where, sems, core):
        self.number, self.axes, self.kib = number, [a for a, _ in axes], kib
        self.events = broadcast(axes, flip)
        self.slots = {key: n for n, key in enumerate(k for k in self.events if k != (0, 0))}
        self.pieces, self.many, self.share, self.shares = pieces, many, share, shares
        self.where, self.core = where, core
        self.send_sem, self.recv_sem, self.pass_sem, self.give_sem = sems

    def index(self, key):
        off = dict(zip(self.axes, key))
        z = lax.rem(self.where[Z] + (NZ - off[Z]), NZ)
        y = lax.rem(self.where[Y] + (NY - off[Y]), NY)
        return z * NY + y

    def copy(self, ref, axis, by, slot):
        n = NZ if axis == Z else NY
        return pltpu.make_async_remote_copy(
            src_ref=ref,
            dst_ref=ref,
            send_sem=self.send_sem,
            recv_sem=self.recv_sem.at[slot],
            device_id={axis: lax.rem(self.where[axis] + (n + by), n)},
            device_id_type=MESH,
        )

    def give(self, ref):
        return pltpu.make_async_remote_copy(
            src_ref=ref,
            dst_ref=ref,
            send_sem=self.pass_sem,
            recv_sem=self.give_sem,
            device_id={C: self.core},
            device_id_type=MESH,
        )

    def pass_on(self, key):
        f = self.index(key)
        for axis, sign, distance, landed in self.events[key]:
            for ref in self.pieces(f):
                self.copy(ref, axis, sign * distance, self.slots[landed]).start()

    def start(self):
        self.pass_on((0, 0))

    def arrive(self, key):
        f = self.index(key)
        self.copy(self.many(1), Z, 1, self.slots[key]).wait_recv()
        self.pass_on(key)
        if self.share is not None:
            self.give(self.share(f)).start()
        return f

    def finish(self):
        self.copy(self.many(PIECES), Z, 1, 0).wait_send()
        if self.share is not None:
            self.give(self.shares()).wait_send()

    def given(self):
        self.give(self.shares()).wait_recv()


PIECES = NF - 1
ZY_RING, YZ_RING = ((Z, "ring"), (Y, "ring")), ((Y, "ring"), (Z, "ring"))
ZY_FAST, YZ_FAST = ((Z, "skip"), (Y, "ring")), ((Y, "direct"), (Z, "skip"))
YZ_LEAN = ((Y, "direct"), (Z, "ring"))


def reduce_kernel(*refs):
    (
        input_act, query_cot, out_cot, attn_out, query_w, out_w, query_factor, out_factor,
        first_q, second_q, first_o, second_o,
        gf_out, gw_out, gd_out, nm_out, sq_out,
        gf, gw, gd, act, cot, qw, ow, moments, low, px, rx1, rx2, s1, ry, s2,
        rz, sp, sq, sq_parts, nm, stage,
        load, f_send, f_recv, f_pass, f_give, w_send, w_recv, w_pass, w_give,
        wx_send, wx_recv, wy_send, wy_recv,
        d_send, d_pass, d_give, own_send, own_recv, mom_send, mom_recv,
        cot_send, cot_recv, px_send, px_recv,
        rx1_send, rx1_recv, rx2_send, rx2_recv, ry_send, ry_recv, rz_send, rz_recv,
        sp_send, sp_recv, nm_sem, sq_sem, out_sem,
    ) = refs
    z, y, x, c = (lax.axis_index(a) for a in (Z, Y, X, C))
    f = z * NY + y
    where = {Z: z, Y: y}
    other = 1 - c
    leads, follows = pl.when(c == 1), pl.when(c == 0)

    def load_own(number, if_q, if_o, dst):
        @follows
        def _():
            pltpu.make_async_copy(if_q, dst, load.at[number]).start()

        @leads
        def _():
            pltpu.make_async_copy(if_o, dst, load.at[number]).start()

        return pltpu.make_async_copy(if_q, dst, load.at[number])

    def load_plain(number, src, dst):
        cp = pltpu.make_async_copy(src, dst, load.at[number])
        cp.start()
        return cp

    for j in range(4):
        cols = pl.ds(128 * j, 128)
        for t, factor in enumerate((query_factor, out_factor)):
            load_plain(0, factor.at[:, cols], gf.at[j, f, t])
    w_loads = [load_plain(1, query_w, qw), load_plain(2, out_w, ow)]
    act_load = load_own(3, input_act, out_cot, act)
    for k in range(2):
        cols = pl.ds(256 * k, 256)
        load_own(4, query_cot.at[:, cols], attn_out.at[:, cols], cot.at[2 * c + k])

    barrier = pltpu.get_barrier_semaphore()
    peers = [{C: other}]
    for axis, at, n in ((Z, z, NZ), (Y, y, NY), (X, x, NX)):
        peers += [{axis: lax.rem(at + 1, n)}, {axis: lax.rem(at + n - 1, n)}]
    peers += [{Z: lax.rem(z + 2, NZ)}, {Z: lax.rem(z + NZ - 2, NZ)}, {Y: lax.rem(y + 2, NY)}]
    for peer in peers:
        pl.semaphore_signal(barrier, inc=1, device_id=peer, device_id_type=MESH)

    for w in w_loads:
        w.wait()
    gw[2 * c, f] = qw[:, :256].astype(BF)
    gw[2 * c + 1, f] = ow[:, :256].astype(BF)
    stage[...] = jnp.where(lax.rem(x, 2) == 0, qw[:, 256:], ow[:, 256:]).astype(BF)
    from_lead = x >= NX // 2

    @pl.when(jnp.logical_and(c == 0, jnp.logical_not(from_lead)))
    def _():
        gw[4 + x, f] = stage[...]

    factors = gf.at[0, pl.ds(0, 4)]
    pltpu.make_async_copy(factors, factors, load.at[0]).wait()
    pl.semaphore_wait(barrier, len(peers))

    def factor_gather(j):
        return Gather(
            j, ZY_FAST if j % 2 == 0 else YZ_LEAN, (j % 2) ^ (j // 2), 32,
            lambda p: (gf.at[j, p],), lambda n: gf.at[j, pl.ds(0, n)],
            lambda p: gf.at[j, p], lambda: gf.at[j, pl.ds(0, PIECES)],
            where, [a.at[j] for a in (f_send, f_recv, f_pass, f_give)], 0,
        )

    def weight_gather(k):
        return Gather(
            k, (ZY_RING, YZ_RING)[k], k, (96, 64)[k],
            lambda p: (gw.at[pl.ds(2 * k, 2), p], gw.at[4 + x, p])[: 2 - k],
            lambda n: gw.at[pl.ds(0, 3 - k), pl.ds(0, n)],
            (lambda p: gw.at[pl.ds(2, 2), p]) if k else None,
            lambda: gw.at[pl.ds(2, 2), pl.ds(0, PIECES)],
            where, (w_send.at[k], w_recv.at[k], w_pass, w_give), 1,
        )

    def dir_gather(k):
        return Gather(
            k, ZY_FAST if k == 0 else YZ_FAST, k, 32,
            lambda p: (gd.at[k, p],), lambda n: gd.at[k, pl.ds(0, n)],
            lambda p: gd.at[k, p, 0], lambda: gd.at[k, :, 0],
            where, (d_send.at[k], f_recv.at[k], d_pass.at[k], d_give.at[k]), 0,
        )

    fg = [factor_gather(j) for j in range(4)]
    wg = [weight_gather(k) for k in range(2)]
    dg = [dir_gather(k) for k in range(2)]
    f_order, w_order, d_order = (expected_order(g) for g in (fg, wg, dg))

    def chunk(b, back):
        q = lax.rem(x + (NX - back), NX)
        return gw.at[4 + q, pl.ds(8 * b, 8)]

    def row_copy(b, back, by):
        ref = chunk(b, back)
        return pltpu.make_async_remote_copy(
            src_ref=ref,
            dst_ref=ref,
            send_sem=wx_send,
            recv_sem=wx_recv.at[b, (back + by) % NX - 1],
            device_id={X: lax.rem(x + (NX + by), NX)},
            device_id_type=MESH,
        )

    def row_give(b, back):
        ref = chunk(b, back)
        return pltpu.make_async_remote_copy(
            src_ref=ref,
            dst_ref=ref,
            send_sem=wy_send,
            recv_sem=wy_recv,
            device_id={C: 1},
            device_id_type=MESH,
        )

    @leads
    def _():
        for g in fg:
            g.start()

    def cot_copy(src, k):
        return pltpu.make_async_remote_copy(
            src_ref=src.at[:, pl.ds(256 * k, 256)],
            dst_ref=cot.at[2 * c + k],
            send_sem=cot_send,
            recv_sem=cot_recv,
            device_id={C: other},
            device_id_type=MESH,
        )

    def every(ref, send_sem, recv_sem):
        return pltpu.make_async_remote_copy(
            src_ref=ref,
            dst_ref=ref,
            send_sem=send_sem,
            recv_sem=recv_sem,
            device_id={C: other},
            device_id_type=MESH,
        )

    def both_cots():
        return every(cot.at[pl.ds(0, 2)], cot_send, cot_recv)

    def own_weights():
        ref = gw.at[pl.ds(2, 2), f]
        return pltpu.make_async_remote_copy(
            src_ref=ref,
            dst_ref=ref,
            send_sem=own_send.at[0],
            recv_sem=own_recv.at[0],
            device_id={C: 0},
            device_id_type=MESH,
        )

    def own_quarter():
        return pltpu.make_async_remote_copy(
            src_ref=stage,
            dst_ref=gw.at[4 + x, f],
            send_sem=own_send.at[1],
            recv_sem=own_recv.at[1],
            device_id={C: 0},
            device_id_type=MESH,
        )

    def own_moments(k, m):
        return pltpu.make_async_remote_copy(
            src_ref=m,
            dst_ref=moments.at[k, 0],
            send_sem=mom_send,
            recv_sem=mom_recv,
            device_id={C: 1},
            device_id_type=MESH,
        )

    all_moments = (first_q, second_q, first_o, second_o)

    @follows
    def _():
        for k in range(2):
            cot_copy(attn_out, k).start()
        for k, m in enumerate(all_moments):
            own_moments(k, m).start()

    @leads
    def _():
        for k in range(2):
            cot_copy(query_cot, k).start()
        own_weights().start()

        @pl.when(from_lead)
        def _():
            own_quarter().start()

        for k, m in enumerate(all_moments):
            pltpu.make_async_copy(m, moments.at[k, 1], load.at[5]).start()

    def project(h):
        def tile(m, _):
            rows = pl.ds(pl.multiple_of(m * 256, 256), 256)
            right = jnp.concatenate(
                [gf[2 * h + j, :, c].reshape(D, 128) for j in range(2)], axis=1
            )
            low[rows, :] = jnp.dot(act[rows, :], right, preferred_element_type=F32).astype(BF)
            return 0

        lax.fori_loop(0, TOK // 256, tile, 0)

        def quarter(i, _):
            xb = lax.rem(x + 2 + i, NX)
            side = cot[xb]
            dims = (((0,), (0,)), ((), ()))
            total = lax.dot_general(low[...], side, dims, preferred_element_type=F32)
            px[h, xb, c] = total.astype(BF)
            return 0

        lax.fori_loop(0, NX, quarter, 0)

    x_up, x_down, x_far = lax.rem(x + 1, NX), lax.rem(x + 3, NX), lax.rem(x + 2, NX)
    sides = ((x_up, 0), (x_down, 1))

    def partial_over(h, i):
        ref = px.at[h, lax.rem(x + 2 + i, NX), 0]
        return pltpu.make_async_remote_copy(
            src_ref=ref,
            dst_ref=ref,
            send_sem=px_send,
            recv_sem=px_recv.at[h, i],
            device_id={C: 1},
            device_id_type=MESH,
        )

    def x_first(h, k):
        return pltpu.make_async_remote_copy(
            src_ref=px.at[h, x_far, :, pl.ds(128 * k, 128)],
            dst_ref=rx1.at[h, k],
            send_sem=rx1_send,
            recv_sem=rx1_recv.at[h, k],
            device_id={X: sides[k][0]},
            device_id_type=MESH,
        )

    def x_second(h, k):
        return pltpu.make_async_remote_copy(
            src_ref=px.at[h, sides[k][0]],
            dst_ref=rx2.at[h, k],
            send_sem=rx2_send,
            recv_sem=rx2_recv.at[h],
            device_id={X: sides[k][0]},
            device_id_type=MESH,
        )

    def x_start(h):
        partial_over(h, 0).wait_recv()
        for k in range(2):
            x_first(h, k).start()

    def x_merge(h):
        for i in (1, 3):
            partial_over(h, i).wait_recv()
        for to, k in sides:
            x_first(h, k).wait_recv()
            rows = pl.ds(128 * k, 128)
            merged = px[h, to, :, rows].astype(F32) + rx1[h, k].astype(F32)
            px[h, to, :, rows] = merged.astype(BF)
            x_second(h, k).start()

    def x_sum(h):
        partial_over(h, 2).wait_recv()
        every(rx2.at[h], rx2_send, rx2_recv.at[h]).wait_recv()
        for t in range(2):
            total = px[h, x, t].astype(F32)
            for k in range(2):
                total += rx2[h, k, t].astype(F32)
            s1[pl.ds(4 * h, 4), :, t] = total.astype(BF).reshape(4, NY, MINE, 256)
        for d in range(1, NY):
            y_copy(h, d).start()

    def y_copy(h, d):
        to = lax.rem(y + d, NY)
        return pltpu.make_async_remote_copy(
            src_ref=s1.at[pl.ds(4 * h, 4), to],
            dst_ref=ry.at[h, d - 1],
            send_sem=ry_send,
            recv_sem=ry_recv.at[h],
            device_id={Y: to},
            device_id_type=MESH,
        )

    def y_sum(h):
        total = s1[pl.ds(4 * h, 4), y].astype(F32)
        every(ry.at[h], ry_send, ry_recv.at[h]).wait_recv()
        for d in range(1, NY):
            total += ry[h, d - 1].astype(F32)
        s2[pl.ds(4 * h, 4)] = total.astype(BF)

    def z_copy(d):
        to = lax.rem(z + d, NZ)
        return pltpu.make_async_remote_copy(
            src_ref=s2.at[to],
            dst_ref=rz.at[d - 1],
            send_sem=rz_send,
            recv_sem=rz_recv,
            device_id={Z: to},
            device_id_type=MESH,
        )

    def sum_copy(d):
        return pltpu.make_async_remote_copy(
            src_ref=sp.at[0],
            dst_ref=sp.at[d],
            send_sem=sp_send,
            recv_sem=sp_recv,
            device_id={X: lax.rem(x + d, NX)},
            device_id_type=MESH,
        )

    def all_sums():
        return every(sp.at[pl.ds(1, NX - 1)], sp_send, sp_recv)

    def moments_over():
        return pltpu.make_async_remote_copy(
            src_ref=nm.at[:, 0],
            dst_ref=nm_out,
            send_sem=nm_sem.at[0],
            recv_sem=nm_sem.at[1],
            device_id={C: 0},
            device_id_type=MESH,
        )

    def squares(t, at):
        part = jnp.square(gd[t, at].astype(F32)).reshape(2 * MINE // 8, 8, HALF)
        part = jnp.sum(part, axis=0)
        return part[:, :128] + part[:, 128:256] + part[:, 256:384] + part[:, 384:]

    def own_dirs(t):
        return dg[t].give(gd.at[t, f, 0])

    outs = []

    def put(number, src, dst):
        cp = pltpu.make_async_copy(src, dst, out_sem.at[number])
        cp.start()
        outs.append(cp)

    @leads
    def _():
        for g, key in f_order:
            g.arrive(key)

    @follows
    def _():
        for g in fg[:2]:
            g.given()
        own_weights().wait_recv()

        @pl.when(from_lead)
        def _():
            own_quarter().wait_recv()

        for g in wg:
            g.start()

    act_load.wait()
    cot_half = cot.at[pl.ds(0, 2)]
    pltpu.make_async_copy(cot_half, cot_half, load.at[4]).wait()
    both_cots().wait_recv()
    project(0)

    @leads
    def _():
        x_start(0)

    @follows
    def _():
        for i in range(NX):
            partial_over(0, i).start()
        for g, key in w_order[:10]:
            g.arrive(key)
        for g in fg[2:]:
            g.given()

    project(1)
    put(0, gf, gf_out)

    @leads
    def _():
        x_merge(0)
        x_start(1)
        x_sum(0)
        x_merge(1)
        y_sum(0)
        x_sum(1)
        y_sum(1)
        for d in range(1, NZ):
            z_copy(d).start()
        total = s2[z].astype(F32)
        every(rz, rz_send, rz_recv).wait_recv()
        for d in range(1, NZ):
            total += rz[d - 1].astype(F32)
        sp[0] = total
        for d in range(1, NX):
            sum_copy(d).start()
        every(moments.at[:, 0], mom_send, mom_recv).wait_recv()
        pltpu.make_async_copy(moments.at[:, 1], moments.at[:, 1], load.at[5]).wait()
        all_sums().wait_recv()

        for t in range(2):
            for p in range(2):
                proj = jnp.concatenate(
                    [sp[lax.rem(x + (NX - q), NX), t] for q in (2 * p, 2 * p + 1)], axis=1
                )
                proj = proj * (1.0 / math.sqrt(TOKENS))
                first = 0.8 * moments[2 * t, p] + 0.2 * proj
                second = 0.9 * moments[2 * t + 1, p] + 0.1 * proj * proj
                nm[2 * t, p] = first
                nm[2 * t + 1, p] = second
                gd[t, f, p] = (first / jnp.sqrt(second)).astype(BF)
            dg[t].start()
            own_dirs(t).start()
            sq_parts[t, f] = squares(t, f)
        moments_over().start()
        pltpu.make_async_copy(nm.at[:, 1], nm_out, out_sem.at[4]).start()
        for g, key in d_order:
            at = g.arrive(key)
            sq_parts[g.number, at] = squares(g.number, at)
        wg[1].given()
        every(gw.at[pl.ds(4, 4)], wy_send, wy_recv).wait_recv()

    @follows
    def _():
        for i in range(NX):
            partial_over(1, i).start()
        for g, key in w_order[10:]:
            g.arrive(key)
        for b in range(NZ // 2):
            for by in (1, -1):
                row_copy(b, 0, by).start()
            row_give(b, 0).start()
        for b in range(NZ // 2):
            for back in (1, 3):
                row_copy(b, 0, back).wait_recv()
                if back == (1, 3)[b % 2]:
                    row_copy(b, back, 1 if back == 1 else -1).start()
                row_give(b, back).start()
        for b in range(NZ // 2):
            row_copy(b, 0, 2).wait_recv()
            row_give(b, 2).start()

    put(1, gw.at[pl.ds(2 * c, 2)], gw_out.at[pl.ds(0, 2)])
    put(3, gw.at[pl.ds(4 + 2 * c, 2)], gw_out.at[pl.ds(2, 2)])

    @leads
    def _():
        total = jnp.sum(sq_parts[...].reshape(2 * NF, 8, 128), axis=0)
        sq[...] = jnp.broadcast_to(jnp.sum(total, axis=(0, 1), keepdims=True), (8, 128))

    squares_over = pltpu.make_async_remote_copy(
        src_ref=sq,
        dst_ref=sq,
        send_sem=sq_sem.at[0],
        recv_sem=sq_sem.at[1],
        device_id={C: 0},
        device_id_type=MESH,
    )

    @leads
    def _():
        squares_over.start()

    @follows
    def _():
        for t in range(2):
            dg[t].given()

    pltpu.make_async_copy(gd.at[:, :, c], gd_out, out_sem.at[5]).start()

    @follows
    def _():
        squares_over.wait_recv()

    put(2, sq, sq_out)

    @leads
    def _():
        for g in fg + dg:
            g.finish()
        own_weights().wait_send()

        @pl.when(from_lead)
        def _():
            own_quarter().wait_send()

        every(rx1, rx1_send, rx1_recv.at[0, 0]).wait_send()
        every(rx2, rx2_send, rx2_recv.at[0]).wait_send()
        every(ry, ry_send, ry_recv.at[0]).wait_send()
        every(rz, rz_send, rz_recv).wait_send()
        all_sums().wait_send()
        moments_over().wait_send()
        pltpu.make_async_copy(nm.at[:, 1], nm_out, out_sem.at[4]).wait()
        squares_over.wait_send()

    @follows
    def _():
        for g in wg:
            g.finish()
        every(gw.at[pl.ds(0, 3)], wx_send, wx_recv.at[0, 0]).wait_send()
        every(gw.at[pl.ds(4, 4)], wy_send, wy_recv).wait_send()
        every(moments.at[:, 0], mom_send, mom_recv).wait_send()
        moments_over().wait_recv()
        every(px.at[:, :, 0], px_send, px_recv.at[0, 0]).wait_send()

    both_cots().wait_send()
    for cp in outs:
        cp.wait()
    pltpu.make_async_copy(gd.at[:, :, c], gd_out, out_sem.at[5]).wait()


def update_kernel(
    gf_in, gw_in, gd_in, nm_in, sq_in, query_factor, out_factor, query_w, out_w,
    new_qw, new_ow, q_step, o_step, nf_q, ns_q, nf_o, ns_o, q_copy, o_copy,
    gf, gw, gd, nm, sq, factor, w, steps, new_w, new_q, new_o,
    first_sem, block_sem, small_sem, copy_sem, out_sem,
):
    copy = pltpu.make_async_copy
    per = NF // BLOCKS
    size = D // BLOCKS
    first = [copy(gd_in, gd, first_sem.at[0]), copy(sq_in, sq, first_sem.at[1])]
    small = [copy(nm_in, nm, small_sem.at[0])]
    for t, (fac, old) in enumerate(((query_factor, query_w), (out_factor, out_w))):
        small.append(copy(fac, factor.at[t], small_sem.at[1 + 2 * t]))
        small.append(copy(old, w.at[t], small_sem.at[2 + 2 * t]))

    def block_loads(b):
        some = pl.ds(per * b, per)
        return (
            copy(gf_in.at[:, some], gf.at[:, some], block_sem.at[0, b]),
            copy(gw_in.at[:, some], gw.at[:, some], block_sem.at[1, b]),
        )

    def block_stores(b):
        at = pl.ds(pl.multiple_of(size * b, size), size)
        return (
            copy(new_q.at[b], q_copy.at[at], copy_sem.at[0]),
            copy(new_o.at[b], o_copy.at[:, at], copy_sem.at[1]),
        )

    for cp in first + small:
        cp.start()
    for cp in block_loads(0):
        cp.start()
    for cp in first:
        cp.wait()
    for cp in block_loads(1) + block_loads(2):
        cp.start()
    inverse = 1.0 / jnp.sqrt(sq[0:1] / (2 * RANK * HQ) + 1e-06)
    inverse = jnp.concatenate([inverse] * 4, axis=1)
    for cp in small:
        cp.wait()
    stores = [copy(nm.at[k], o, out_sem.at[k]) for k, o in enumerate((nf_q, ns_q, nf_o, ns_o))]
    for t, (to_step, to_w) in enumerate(((q_step, new_qw), (o_step, new_ow))):
        step = jnp.dot(factor[t], gd[t].reshape(RANK, HALF), preferred_element_type=F32)
        step = step * inverse
        steps[t] = step
        new_w[t] = w[t] - 0.01 * step
        stores.append(copy(steps.at[t], to_step, out_sem.at[4 + 2 * t]))
        stores.append(copy(new_w.at[t], to_w, out_sem.at[5 + 2 * t]))
    for cp in stores:
        cp.start()

    def block(b, _):
        some = pl.ds(per * b, per)
        @pl.when(b + 3 < BLOCKS)
        def _():
            for cp in block_loads(b + 3):
                cp.start()

        for cp in block_loads(b):
            cp.wait()
        moved = []
        for t in range(2):
            rows = jnp.concatenate([gf[j, some, t].reshape(size, 128) for j in range(4)], axis=1)
            step = jnp.dot(rows, gd[t].reshape(RANK, HALF), preferred_element_type=F32)
            old = jnp.concatenate([gw[i, some].reshape(size, 256) for i in (t, 2 + t)], axis=1)
            moved.append(old.astype(F32) - (0.01 * inverse) * step)
        new_q[b] = moved[0].astype(BF)
        new_o[b] = moved[1].T.astype(BF)
        for cp in block_stores(b):
            cp.start()
        return 0

    lax.fori_loop(0, BLOCKS, block, 0)
    for cp in stores:
        cp.wait()
    copy(new_q, new_q, copy_sem.at[0]).wait()
    copy(new_o, new_o, copy_sem.at[1]).wait()


def body(
    input_act, query_cot, out_cot, attn_out, query_w, out_w, query_factor, out_factor,
    first_q, second_q, first_o, second_o,
):
    struct = jax.ShapeDtypeStruct
    dma = pltpu.SemaphoreType.DMA
    vmem = pltpu.VMEM
    out_w = out_w.T
    scratch = [
        vmem((4, NF, 2, ROWS, 128), BF),
        vmem((8, NF, ROWS, 256), BF),
        vmem((2, NF, 2, MINE, HALF), BF),
        vmem((TOK, D), BF),
        vmem((4, TOK, 256), BF),
        vmem((ROWS, HALF), F32),
        vmem((ROWS, HALF), F32),
        vmem((4, 2, MINE, HALF), F32),
        vmem((TOK, 256), BF),
        vmem((2, NX, 2, 256, 256), BF),
        vmem((2, 2, 2, 128, 256), BF),
        vmem((2, 2, 2, 256, 256), BF),
        vmem((NZ, NY, 2, MINE, 256), BF),
        vmem((2, NY - 1, 4, 2, MINE, 256), BF),
        vmem((NZ, 2, MINE, 256), BF),
        vmem((NZ - 1, 2, MINE, 256), BF),
        vmem((NX, 2, MINE, 256), F32),
        vmem((8, 128), F32),
        vmem((2, NF, 8, 128), F32),
        vmem((4, 2, MINE, HALF), F32),
        vmem((ROWS, 256), BF),
        dma((6,)),
        dma((4,)), dma((4, PIECES)), dma((4,)), dma((4,)),
        dma((2,)), dma((2, PIECES)), dma, dma,
        dma, dma((NZ // 2, 3)), dma, dma,
        dma((2,)), dma((2,)), dma((2,)),
        dma((2,)), dma((2,)), dma, dma, dma, dma,
        dma, dma((2, NX)),
        dma, dma((2, 2)), dma, dma((2,)),
        dma, dma((2,)), dma, dma, dma, dma,
        dma((2,)), dma((2,)), dma((6,)),
    ]
    gf, gw, gd, nm, sq = pl.pallas_call(
        reduce_kernel,
        out_shape=(
            struct((4, NF, 2, ROWS, 128), BF),
            struct((4, NF, ROWS, 256), BF),
            struct((2, NF, MINE, HALF), BF),
            struct((4, MINE, HALF), F32),
            struct((8, 128), F32),
        ),
        in_specs=[pl.BlockSpec(memory_space=pl.ANY)] * 12,
        out_specs=[pl.BlockSpec(memory_space=pl.ANY)] * 5,
        scratch_shapes=scratch,
        compiler_params=pltpu.CompilerParams(
            collective_id=0, has_side_effects=True, vmem_limit_bytes=56 * 1024 * 1024
        ),
        name="reduce",
    )(
        input_act, query_cot, out_cot, attn_out, query_w, out_w, query_factor, out_factor,
        first_q, second_q, first_o, second_o,
    )

    anywhere = pl.BlockSpec(memory_space=pl.ANY)
    shard, small = struct((ROWS, HALF), F32), struct((MINE, HALF), F32)
    outs = pl.pallas_call(
        update_kernel,
        out_shape=(
            *[shard] * 4,
            *[small] * 4,
            struct((D, HALF), BF),
            struct((HALF, D), BF),
        ),
        in_specs=[anywhere] * 9,
        out_specs=[anywhere] * 10,
        scratch_shapes=[
            vmem((4, NF, 2, ROWS, 128), BF),
            vmem((4, NF, ROWS, 256), BF),
            vmem((2, NF, MINE, HALF), BF),
            vmem((4, MINE, HALF), F32),
            vmem((8, 128), F32),
            vmem((2, ROWS, RANK), BF),
            vmem((2, ROWS, HALF), F32),
            vmem((2, ROWS, HALF), F32),
            vmem((2, ROWS, HALF), F32),
            vmem((BLOCKS, D // BLOCKS, HALF), BF),
            vmem((BLOCKS, HALF, D // BLOCKS), BF),
            dma((2,)),
            dma((2, BLOCKS)),
            dma((5,)),
            dma((2,)),
            dma((8,)),
        ],
        compiler_params=pltpu.CompilerParams(vmem_limit_bytes=56 * 1024 * 1024),
        name="update",
    )(gf, gw, gd, nm, sq, query_factor, out_factor, query_w, out_w)
    outs = list(outs)
    outs[1], outs[3] = outs[1].T, outs[3].T
    return tuple(outs)


def solution(mesh):
    finer = Mesh(mesh.devices.reshape(NZ, NY, NX, 2), (Z, Y, X, C))
    in_specs = (
        P(FS_REP, None),
        P(FS_REP, C),
        P(FS_REP, None),
        P(FS_REP, C),
        P(FS, C),
        P(C, FS),
        P(FS, None),
        P(FS, None),
        *[P(FS, C)] * 4,
    )
    out_specs = (
        P(FS, C),
        P(C, FS),
        P(FS, C),
        P(C, FS),
        *[P(FS, C)] * 4,
        P(None, C),
        P(C, None),
    )
    return jax.shard_map(body, mesh=finer, in_specs=in_specs, out_specs=out_specs, check_vma=False)
```

```python
import math

import jax
import jax.numpy as jnp
from jax import lax
from jax.experimental import pallas as pl
from jax.experimental.pallas import tpu as pltpu
from jax.sharding import Mesh
from jax.sharding import PartitionSpec as P

NZ, NY, NX = 8, 4, 4
NF = NZ * NY
D, RANK, HQ, TOKENS = 2048, 512, 1024, 98304
HALF = HQ // 2
TOK = TOKENS // (NF * NX)
ROWS = D // NF
MINE = RANK // NF
BLOCKS = 8
Z, Y, X, C = "fs_0", "fs_1", "rep", "tp"
FS = (Z, Y)
FS_REP = (Z, Y, X)
BF, F32 = jnp.bfloat16, jnp.float32
MESH = pl.DeviceIdType.MESH


def along(n, mode, flip):
    up, down = (n // 2, n - 1 - n // 2)[:: -1 if flip else 1]
    tree = {}
    for s, far in ((1, up), (-1, down)):
        if mode == "ring":
            hops = [(k, 1) for k in range(far)]
        elif mode == "direct":
            hops = [(0, k) for k in range(far, 0, -1)]
        else:
            hops = [(0, 2), (0, 1), (2, 2), (2, 1)]
        for at, by in hops:
            if at + by <= far:
                tree.setdefault(s * at, []).append((s, by, s * (at + by)))
    return tree, range(-down, up + 1)


def broadcast(axes, flip):
    (axis_1, mode_1), (axis_2, mode_2) = axes
    sizes = {Z: NZ, Y: NY}
    tree_1, span = along(sizes[axis_1], mode_1, flip)
    events = {}
    for i in span:
        tree_2, across = along(sizes[axis_2], mode_2, (i + flip) % 2)
        for j in across:
            on = [(axis_2, s, d, (i, to)) for s, d, to in tree_2.get(j, [])]
            if j == 0:
                on = [(axis_1, s, d, (to, 0)) for s, d, to in tree_1.get(i, [])] + on
            events[i, j] = on
    return events


def expected_order(gathers):
    free, now, order = {}, 0.0, []
    heap = [(0.01 * g.number, g.number, (0, 0)) for g in gathers]
    by_number = {g.number: g for g in gathers}
    while heap:
        heap.sort()
        when, number, key = heap.pop(0)
        now, g = max(now, when), by_number[number]
        if key != (0, 0):
            order.append((when, g, key))
        for axis, sign, distance, landed in g.events[key]:
            now += 0.02
            begin = max(free.get((axis, sign), 0.0), now)
            wire = g.kib / 91.0
            free[axis, sign] = begin + wire * distance
            heap.append((begin + wire + 2.0 + 0.75 * (distance - 1), number, landed))
    return order


class Gather:
    def __init__(self, number, axes, flip, kib, pieces, many, share, shares, where, sems, core):
        self.number, self.axes, self.kib = number, [a for a, _ in axes], kib
        self.events = broadcast(axes, flip)
        self.slots = {key: n for n, key in enumerate(k for k in self.events if k != (0, 0))}
        self.pieces, self.many, self.share, self.shares = pieces, many, share, shares
        self.where, self.core = where, core
        self.send_sem, self.recv_sem, self.pass_sem, self.give_sem = sems

    def index(self, key):
        off = dict(zip(self.axes, key))
        z = lax.rem(self.where[Z] + (NZ - off[Z]), NZ)
        y = lax.rem(self.where[Y] + (NY - off[Y]), NY)
        return z * NY + y

    def copy(self, ref, axis, by, slot):
        n = NZ if axis == Z else NY
        return pltpu.make_async_remote_copy(
            src_ref=ref,
            dst_ref=ref,
            send_sem=self.send_sem,
            recv_sem=self.recv_sem.at[slot],
            device_id={axis: lax.rem(self.where[axis] + (n + by), n)},
            device_id_type=MESH,
        )

    def give(self, ref):
        return pltpu.make_async_remote_copy(
            src_ref=ref,
            dst_ref=ref,
            send_sem=self.pass_sem,
            recv_sem=self.give_sem,
            device_id={C: self.core},
            device_id_type=MESH,
        )

    def pass_on(self, key):
        f = self.index(key)
        for axis, sign, distance, landed in self.events[key]:
            for ref in self.pieces(f):
                self.copy(ref, axis, sign * distance, self.slots[landed]).start()

    def start(self):
        self.pass_on((0, 0))

    def arrive(self, key):
        f = self.index(key)
        self.copy(self.many(1), Z, 1, self.slots[key]).wait_recv()
        self.pass_on(key)
        if self.share is not None:
            self.give(self.share(f)).start()
        return f

    def finish(self):
        self.copy(self.many(PIECES), Z, 1, 0).wait_send()
        if self.shares is not None:
            self.give(self.shares()).wait_send()

    def given(self):
        self.give(self.shares()).wait_recv()


PIECES = NF - 1
ZY_RING, YZ_RING = ((Z, "ring"), (Y, "ring")), ((Y, "ring"), (Z, "ring"))
ZY_FAST, YZ_FAST = ((Z, "skip"), (Y, "ring")), ((Y, "direct"), (Z, "skip"))
YZ_LEAN = ((Y, "direct"), (Z, "ring"))


def reduce_kernel(*refs):
    (
        input_act, query_cot, out_cot, attn_out, query_w, out_w, query_factor, out_factor,
        first_q, second_q, first_o, second_o,
        gf_out, gw_out, gd_out, nm_out, sq_out,
        gf, gw, gd, act, cot, qw, ow, moments, low, px, rx1, rx2, s1, ry, s2,
        rz, sp, sq, sq_parts, nm,
        load, f_send, f_recv, f_pass, f_give, w_send, w_pass, w_give,
        d_send, d_pass, d_give, own_send, own_recv, mom_send, mom_recv,
        cot_send, cot_recv, px_send, px_recv,
        rx1_send, rx1_recv, rx2_send, rx2_recv, ry_send, ry_recv, rz_send, rz_recv,
        sp_send, sp_recv, nm_sem, sq_sem, out_sem,
    ) = refs
    z, y, x, c = (lax.axis_index(a) for a in (Z, Y, X, C))
    f = z * NY + y
    where = {Z: z, Y: y}
    other = 1 - c
    leads, follows = pl.when(c == 1), pl.when(c == 0)

    def load_own(number, if_q, if_o, dst):
        @follows
        def _():
            pltpu.make_async_copy(if_q, dst, load.at[number]).start()

        @leads
        def _():
            pltpu.make_async_copy(if_o, dst, load.at[number]).start()

        return pltpu.make_async_copy(if_q, dst, load.at[number])

    def load_plain(number, src, dst):
        cp = pltpu.make_async_copy(src, dst, load.at[number])
        cp.start()
        return cp

    for j in range(4):
        cols = pl.ds(128 * j, 128)
        for t, factor in enumerate((query_factor, out_factor)):
            load_plain(0, factor.at[:, cols], gf.at[j, f, t])
    w_loads = [load_plain(1, query_w, qw), load_plain(2, out_w, ow)]
    act_load = load_own(3, input_act, out_cot, act)
    for k in range(2):
        cols = pl.ds(256 * k, 256)
        _ = load_own(4, query_cot.at[:, cols], attn_out.at[:, cols], cot.at[2 * c + k])

    barrier = pltpu.get_barrier_semaphore()
    peers = [{C: other}]
    for axis, at, n in ((Z, z, NZ), (Y, y, NY), (X, x, NX)):
        peers += [{axis: lax.rem(at + 1, n)}, {axis: lax.rem(at + n - 1, n)}]
    peers += [{Z: lax.rem(z + 2, NZ)}, {Z: lax.rem(z + NZ - 2, NZ)}, {Y: lax.rem(y + 2, NY)}]
    for peer in peers:
        pl.semaphore_signal(barrier, inc=1, device_id=peer, device_id_type=MESH)

    for w in w_loads:
        w.wait()
    for k in range(2):
        gw[4 * k + 2 * c, f] = qw[:, 256 * k : 256 * k + 256].astype(BF)
        gw[4 * k + 2 * c + 1, f] = ow[:, 256 * k : 256 * k + 256].astype(BF)
    factors = gf.at[0, pl.ds(0, 4)]
    pltpu.make_async_copy(factors, factors, load.at[0]).wait()
    pl.semaphore_wait(barrier, len(peers))

    def factor_gather(j):
        return Gather(
            j, ZY_FAST if j % 2 == 0 else YZ_LEAN, (j % 2) ^ (j // 2), 32,
            lambda p: (gf.at[j, p],), lambda n: gf.at[j, pl.ds(0, n)],
            lambda p: gf.at[j, p], lambda: gf.at[j, pl.ds(0, PIECES)],
            where, [a.at[j] for a in (f_send, f_recv, f_pass, f_give)], 0,
        )

    blocks = ((0, 2, 6), (2, 2, None), (4, 2, None), (7, 1, None))

    def weight_gather(k):
        first, count, more = blocks[k]

        def pieces(p):
            refs = (gw.at[pl.ds(first, count), p],)
            return refs if more is None else refs + (gw.at[more, p],)

        total = count + (more is not None)
        give = (lambda p: gw.at[6, p]) if k == 0 else (lambda p: pieces(p)[0])
        return Gather(
            k, (ZY_RING, YZ_RING)[k % 2] if k != 2 else ZY_RING, (0, 1, 1, 0)[k], 32 * total,
            pieces, lambda n: gw.at[pl.ds(0, total), pl.ds(0, n)],
            None if k == 2 else give, None,
            where, (w_send.at[k], f_recv.at[k], w_pass, w_give), 1,
        )

    def all_shares():
        return every(gw.at[pl.ds(0, 4), pl.ds(0, PIECES)], w_pass, w_give)

    def dir_gather(k):
        return Gather(
            k, ZY_FAST if k == 0 else YZ_FAST, k, 32,
            lambda p: (gd.at[k, p],), lambda n: gd.at[k, pl.ds(0, n)],
            lambda p: gd.at[k, p, 0], lambda: gd.at[k, :, 0],
            where, (d_send.at[k], f_recv.at[k], d_pass.at[k], d_give.at[k]), 0,
        )

    fg = [factor_gather(j) for j in range(4)]
    wg = [weight_gather(k) for k in range(4)]
    dg = [dir_gather(k) for k in range(2)]
    f_order, w_order, d_order = (expected_order(g) for g in (fg, wg, dg))

    @leads
    def _():
        for g in fg:
            g.start()

    def cot_copy(src, k):
        return pltpu.make_async_remote_copy(
            src_ref=src.at[:, pl.ds(256 * k, 256)],
            dst_ref=cot.at[2 * c + k],
            send_sem=cot_send,
            recv_sem=cot_recv,
            device_id={C: other},
            device_id_type=MESH,
        )

    def every(ref, send_sem, recv_sem):
        return pltpu.make_async_remote_copy(
            src_ref=ref,
            dst_ref=ref,
            send_sem=send_sem,
            recv_sem=recv_sem,
            device_id={C: other},
            device_id_type=MESH,
        )

    def both_cots():
        return every(cot.at[pl.ds(0, 2)], cot_send, cot_recv)

    def own_weights(k):
        ref = gw.at[pl.ds(4 * k + 2, 2), f]
        return pltpu.make_async_remote_copy(
            src_ref=ref,
            dst_ref=ref,
            send_sem=own_send,
            recv_sem=own_recv,
            device_id={C: 0},
            device_id_type=MESH,
        )

    def both_weights():
        return every(gw.at[pl.ds(0, 4), f], own_send, own_recv)

    def own_moments(k, m):
        return pltpu.make_async_remote_copy(
            src_ref=m,
            dst_ref=moments.at[k, 0],
            send_sem=mom_send,
            recv_sem=mom_recv,
            device_id={C: 1},
            device_id_type=MESH,
        )

    all_moments = (first_q, second_q, first_o, second_o)

    @follows
    def _():
        for k in range(2):
            cot_copy(attn_out, k).start()
        for k, m in enumerate(all_moments):
            own_moments(k, m).start()

    @leads
    def _():
        for k in range(2):
            cot_copy(query_cot, k).start()
        for k in range(2):
            own_weights(k).start()
        for k, m in enumerate(all_moments):
            pltpu.make_async_copy(m, moments.at[k, 1], load.at[5]).start()

    def project(h):
        def tile(m, _):
            rows = pl.ds(pl.multiple_of(m * 256, 256), 256)
            right = jnp.concatenate(
                [gf[2 * h + j, :, c].reshape(D, 128) for j in range(2)], axis=1
            )
            low[rows, :] = jnp.dot(act[rows, :], right, preferred_element_type=F32).astype(BF)
            return 0

        lax.fori_loop(0, TOK // 256, tile, 0)

        for i in range(NX):
            xb = lax.rem(x + 2 + i, NX)
            dims = (((0,), (0,)), ((), ()))
            total = lax.dot_general(low[...], cot[xb], dims, preferred_element_type=F32)
            px[h, xb, c] = total.astype(BF)

            @follows
            def _():
                partial_over(h, i).start()

            if i == NX - 1:

                @leads
                def _():
                    x_start(h)

    x_up, x_down, x_far = lax.rem(x + 1, NX), lax.rem(x + 3, NX), lax.rem(x + 2, NX)
    sides = ((x_up, 0), (x_down, 1))

    def partial_over(h, i):
        ref = px.at[h, lax.rem(x + 2 + i, NX), 0]
        return pltpu.make_async_remote_copy(
            src_ref=ref,
            dst_ref=ref,
            send_sem=px_send,
            recv_sem=px_recv.at[h, i],
            device_id={C: 1},
            device_id_type=MESH,
        )

    def x_first(h, k):
        return pltpu.make_async_remote_copy(
            src_ref=px.at[h, x_far, :, pl.ds(128 * k, 128)],
            dst_ref=rx1.at[h, k],
            send_sem=rx1_send,
            recv_sem=rx1_recv.at[h, k],
            device_id={X: sides[k][0]},
            device_id_type=MESH,
        )

    def x_second(h, k):
        return pltpu.make_async_remote_copy(
            src_ref=px.at[h, sides[k][0]],
            dst_ref=rx2.at[h, k],
            send_sem=rx2_send,
            recv_sem=rx2_recv.at[h],
            device_id={X: sides[k][0]},
            device_id_type=MESH,
        )

    def x_start(h):
        partial_over(h, 0).wait_recv()
        for k in range(2):
            x_first(h, k).start()

    def x_merge(h):
        for i in (1, 3):
            partial_over(h, i).wait_recv()
        for to, k in sides:
            x_first(h, k).wait_recv()
            rows = pl.ds(128 * k, 128)
            merged = px[h, to, :, rows].astype(F32) + rx1[h, k].astype(F32)
            px[h, to, :, rows] = merged.astype(BF)
            x_second(h, k).start()

    def x_sum(h):
        partial_over(h, 2).wait_recv()
        every(rx2.at[h], rx2_send, rx2_recv.at[h]).wait_recv()
        for t in range(2):
            total = px[h, x, t].astype(F32)
            for k in range(2):
                total += rx2[h, k, t].astype(F32)
            s1[pl.ds(4 * h, 4), :, t] = total.astype(BF).reshape(4, NY, MINE, 256)
        for d in range(1, NY):
            y_copy(h, d).start()

    def y_copy(h, d):
        to = lax.rem(y + d, NY)
        return pltpu.make_async_remote_copy(
            src_ref=s1.at[pl.ds(4 * h, 4), to],
            dst_ref=ry.at[h, d - 1],
            send_sem=ry_send,
            recv_sem=ry_recv.at[h],
            device_id={Y: to},
            device_id_type=MESH,
        )

    def y_sum(h):
        total = s1[pl.ds(4 * h, 4), y].astype(F32)
        every(ry.at[h], ry_send, ry_recv.at[h]).wait_recv()
        for d in range(1, NY):
            total += ry[h, d - 1].astype(F32)
        s2[pl.ds(4 * h, 4)] = total.astype(BF)

    def z_copy(d):
        to = lax.rem(z + d, NZ)
        return pltpu.make_async_remote_copy(
            src_ref=s2.at[to],
            dst_ref=rz.at[d - 1],
            send_sem=rz_send,
            recv_sem=rz_recv,
            device_id={Z: to},
            device_id_type=MESH,
        )

    def sum_copy(d):
        return pltpu.make_async_remote_copy(
            src_ref=sp.at[0],
            dst_ref=sp.at[d],
            send_sem=sp_send,
            recv_sem=sp_recv,
            device_id={X: lax.rem(x + d, NX)},
            device_id_type=MESH,
        )

    def all_sums():
        return every(sp.at[pl.ds(1, NX - 1)], sp_send, sp_recv)

    def moments_over():
        return pltpu.make_async_remote_copy(
            src_ref=nm.at[:, 0],
            dst_ref=nm_out,
            send_sem=nm_sem.at[0],
            recv_sem=nm_sem.at[1],
            device_id={C: 0},
            device_id_type=MESH,
        )

    def squares(t, at):
        part = jnp.square(gd[t, at].astype(F32)).reshape(2 * MINE // 8, 8, HALF)
        part = jnp.sum(part, axis=0)
        return part[:, :128] + part[:, 128:256] + part[:, 256:384] + part[:, 384:]

    def own_dirs(t):
        return dg[t].give(gd.at[t, f, 0])

    outs = []

    def put(number, src, dst):
        cp = pltpu.make_async_copy(src, dst, out_sem.at[number])
        cp.start()
        outs.append(cp)

    @leads
    def _():
        for _, g, key in f_order:
            g.arrive(key)

    @follows
    def _():
        both_weights().wait_recv()
        fg[0].given()
        for g in wg:
            g.start()
        fg[1].given()

    act_load.wait()
    cot_half = cot.at[pl.ds(0, 2)]
    pltpu.make_async_copy(cot_half, cot_half, load.at[4]).wait()
    both_cots().wait_recv()
    project(0)

    @follows
    def _():
        for g in fg[2:]:
            g.given()

    project(1)
    put(0, gf, gf_out)

    @leads
    def _():
        x_merge(0)
        x_sum(0)
        x_merge(1)
        y_sum(0)
        x_sum(1)
        y_sum(1)
        for d in range(1, NZ):
            z_copy(d).start()
        total = s2[z].astype(F32)
        every(rz, rz_send, rz_recv).wait_recv()
        for d in range(1, NZ):
            total += rz[d - 1].astype(F32)
        sp[0] = total
        for d in range(1, NX):
            sum_copy(d).start()
        every(moments.at[:, 0], mom_send, mom_recv).wait_recv()
        pltpu.make_async_copy(moments.at[:, 1], moments.at[:, 1], load.at[5]).wait()
        all_sums().wait_recv()

        for t in range(2):
            for p in range(2):
                proj = jnp.concatenate(
                    [sp[lax.rem(x + (NX - q), NX), t] for q in (2 * p, 2 * p + 1)], axis=1
                )
                proj = proj * (1.0 / math.sqrt(TOKENS))
                first = 0.8 * moments[2 * t, p] + 0.2 * proj
                second = 0.9 * moments[2 * t + 1, p] + 0.1 * proj * proj
                nm[2 * t, p] = first
                nm[2 * t + 1, p] = second
                gd[t, f, p] = (first / jnp.sqrt(second)).astype(BF)
            dg[t].start()
            own_dirs(t).start()
            sq_parts[t, f] = squares(t, f)
        moments_over().start()
        pltpu.make_async_copy(nm.at[:, 1], nm_out, out_sem.at[4]).start()
        for _, g, key in d_order:
            at = g.arrive(key)
            sq_parts[g.number, at] = squares(g.number, at)
        all_shares().wait_recv()

    @follows
    def _():
        for _, g, key in w_order:
            g.arrive(key)

    put(1, gw.at[pl.ds(2 * c, 2)], gw_out.at[pl.ds(0, 2)])
    put(3, gw.at[pl.ds(4 + 2 * c, 2)], gw_out.at[pl.ds(2, 2)])

    @leads
    def _():
        total = jnp.sum(sq_parts[...].reshape(2 * NF, 8, 128), axis=0)
        sq[...] = jnp.broadcast_to(jnp.sum(total, axis=(0, 1), keepdims=True), (8, 128))

    squares_over = pltpu.make_async_remote_copy(
        src_ref=sq,
        dst_ref=sq,
        send_sem=sq_sem.at[0],
        recv_sem=sq_sem.at[1],
        device_id={C: 0},
        device_id_type=MESH,
    )

    @leads
    def _():
        squares_over.start()

    @follows
    def _():
        for t in range(2):
            dg[t].given()

    pltpu.make_async_copy(gd.at[:, :, c], gd_out, out_sem.at[5]).start()

    @follows
    def _():
        squares_over.wait_recv()

    put(2, sq, sq_out)

    @leads
    def _():
        for g in fg + dg:
            g.finish()
        both_weights().wait_send()
        every(rx1, rx1_send, rx1_recv.at[0, 0]).wait_send()
        every(rx2, rx2_send, rx2_recv.at[0]).wait_send()
        every(ry, ry_send, ry_recv.at[0]).wait_send()
        every(rz, rz_send, rz_recv).wait_send()
        all_sums().wait_send()
        moments_over().wait_send()
        pltpu.make_async_copy(nm.at[:, 1], nm_out, out_sem.at[4]).wait()
        squares_over.wait_send()

    @follows
    def _():
        for g in wg:
            g.finish()
        all_shares().wait_send()
        every(moments.at[:, 0], mom_send, mom_recv).wait_send()
        moments_over().wait_recv()
        every(px.at[:, :, 0], px_send, px_recv.at[0, 0]).wait_send()

    both_cots().wait_send()
    for cp in outs:
        cp.wait()
    pltpu.make_async_copy(gd.at[:, :, c], gd_out, out_sem.at[5]).wait()


def update_kernel(
    gf_in, gw_in, gd_in, nm_in, sq_in, query_factor, out_factor, query_w, out_w,
    new_qw, new_ow, q_step, o_step, nf_q, ns_q, nf_o, ns_o, q_copy, o_copy,
    gf, gw, gd, nm, sq, factor, w, steps, new_w, new_q, new_o,
    first_sem, block_sem, small_sem, copy_sem, out_sem,
):
    copy = pltpu.make_async_copy
    per = NF // BLOCKS
    size = D // BLOCKS
    first = [copy(gd_in, gd, first_sem.at[0]), copy(sq_in, sq, first_sem.at[1])]
    small = [copy(nm_in, nm, small_sem.at[0])]
    for t, (fac, old) in enumerate(((query_factor, query_w), (out_factor, out_w))):
        small.append(copy(fac, factor.at[t], small_sem.at[1 + 2 * t]))
        small.append(copy(old, w.at[t], small_sem.at[2 + 2 * t]))

    def block_loads(b):
        some = pl.ds(per * b, per)
        return (
            copy(gf_in.at[:, some], gf.at[:, some], block_sem.at[0, b]),
            copy(gw_in.at[:, some], gw.at[:, some], block_sem.at[1, b]),
        )

    def block_stores(b):
        at = pl.ds(pl.multiple_of(size * b, size), size)
        return (
            copy(new_q.at[b], q_copy.at[at], copy_sem.at[0]),
            copy(new_o.at[b], o_copy.at[:, at], copy_sem.at[1]),
        )

    for cp in first + small:
        cp.start()
    for cp in block_loads(0):
        cp.start()
    for cp in first:
        cp.wait()
    for cp in block_loads(1) + block_loads(2):
        cp.start()
    inverse = 1.0 / jnp.sqrt(sq[0:1] / (2 * RANK * HQ) + 1e-06)
    inverse = jnp.concatenate([inverse] * 4, axis=1)
    for cp in small:
        cp.wait()
    stores = [copy(nm.at[k], o, out_sem.at[k]) for k, o in enumerate((nf_q, ns_q, nf_o, ns_o))]
    for t, (to_step, to_w) in enumerate(((q_step, new_qw), (o_step, new_ow))):
        step = jnp.dot(factor[t], gd[t].reshape(RANK, HALF), preferred_element_type=F32)
        step = step * inverse
        steps[t] = step
        new_w[t] = w[t] - 0.01 * step
        stores.append(copy(steps.at[t], to_step, out_sem.at[4 + 2 * t]))
        stores.append(copy(new_w.at[t], to_w, out_sem.at[5 + 2 * t]))
    for cp in stores:
        cp.start()

    def block(b, _):
        some = pl.ds(per * b, per)
        @pl.when(b + 3 < BLOCKS)
        def _():
            for cp in block_loads(b + 3):
                cp.start()

        for cp in block_loads(b):
            cp.wait()
        moved = []
        for t in range(2):
            rows = jnp.concatenate([gf[j, some, t].reshape(size, 128) for j in range(4)], axis=1)
            step = jnp.dot(rows, gd[t].reshape(RANK, HALF), preferred_element_type=F32)
            old = jnp.concatenate([gw[i, some].reshape(size, 256) for i in (t, 2 + t)], axis=1)
            moved.append(old.astype(F32) - (0.01 * inverse) * step)
        new_q[b] = moved[0].astype(BF)
        new_o[b] = moved[1].astype(BF).T
        for cp in block_stores(b):
            cp.start()
        return 0

    lax.fori_loop(0, BLOCKS, block, 0)
    for cp in stores:
        cp.wait()
    copy(new_q, new_q, copy_sem.at[0]).wait()
    copy(new_o, new_o, copy_sem.at[1]).wait()


def body(
    input_act, query_cot, out_cot, attn_out, query_w, out_w, query_factor, out_factor,
    first_q, second_q, first_o, second_o,
):
    struct = jax.ShapeDtypeStruct
    dma = pltpu.SemaphoreType.DMA
    vmem = pltpu.VMEM
    out_w = out_w.T
    scratch = [
        vmem((4, NF, 2, ROWS, 128), BF),
        vmem((8, NF, ROWS, 256), BF),
        vmem((2, NF, 2, MINE, HALF), BF),
        vmem((TOK, D), BF),
        vmem((4, TOK, 256), BF),
        vmem((ROWS, HALF), F32),
        vmem((ROWS, HALF), F32),
        vmem((4, 2, MINE, HALF), F32),
        vmem((TOK, 256), BF),
        vmem((2, NX, 2, 256, 256), BF),
        vmem((2, 2, 2, 128, 256), BF),
        vmem((2, 2, 2, 256, 256), BF),
        vmem((NZ, NY, 2, MINE, 256), BF),
        vmem((2, NY - 1, 4, 2, MINE, 256), BF),
        vmem((NZ, 2, MINE, 256), BF),
        vmem((NZ - 1, 2, MINE, 256), BF),
        vmem((NX, 2, MINE, 256), F32),
        vmem((8, 128), F32),
        vmem((2, NF, 8, 128), F32),
        vmem((4, 2, MINE, HALF), F32),
        dma((6,)),
        dma((4,)), dma((4, PIECES)), dma((4,)), dma((4,)),
        dma((4,)), dma, dma,
        dma((2,)), dma((2,)), dma((2,)),
        dma, dma, dma, dma, dma, dma,
        dma, dma((2, NX)),
        dma, dma((2, 2)), dma, dma((2,)),
        dma, dma((2,)), dma, dma, dma, dma,
        dma((2,)), dma((2,)), dma((6,)),
    ]
    gf, gw, gd, nm, sq = pl.pallas_call(
        reduce_kernel,
        out_shape=(
            struct((4, NF, 2, ROWS, 128), BF),
            struct((4, NF, ROWS, 256), BF),
            struct((2, NF, MINE, HALF), BF),
            struct((4, MINE, HALF), F32),
            struct((8, 128), F32),
        ),
        in_specs=[pl.BlockSpec(memory_space=pl.ANY)] * 12,
        out_specs=[pl.BlockSpec(memory_space=pl.ANY)] * 5,
        scratch_shapes=scratch,
        compiler_params=pltpu.CompilerParams(
            collective_id=0, has_side_effects=True, vmem_limit_bytes=56 * 1024 * 1024
        ),
        name="reduce",
    )(
        input_act, query_cot, out_cot, attn_out, query_w, out_w, query_factor, out_factor,
        first_q, second_q, first_o, second_o,
    )

    anywhere = pl.BlockSpec(memory_space=pl.ANY)
    shard, small = struct((ROWS, HALF), F32), struct((MINE, HALF), F32)
    outs = pl.pallas_call(
        update_kernel,
        out_shape=(
            *[shard] * 4,
            *[small] * 4,
            struct((D, HALF), BF),
            struct((HALF, D), BF),
        ),
        in_specs=[anywhere] * 9,
        out_specs=[anywhere] * 10,
        scratch_shapes=[
            vmem((4, NF, 2, ROWS, 128), BF),
            vmem((4, NF, ROWS, 256), BF),
            vmem((2, NF, MINE, HALF), BF),
            vmem((4, MINE, HALF), F32),
            vmem((8, 128), F32),
            vmem((2, ROWS, RANK), BF),
            vmem((2, ROWS, HALF), F32),
            vmem((2, ROWS, HALF), F32),
            vmem((2, ROWS, HALF), F32),
            vmem((BLOCKS, D // BLOCKS, HALF), BF),
            vmem((BLOCKS, HALF, D // BLOCKS), BF),
            dma((2,)),
            dma((2, BLOCKS)),
            dma((5,)),
            dma((2,)),
            dma((8,)),
        ],
        compiler_params=pltpu.CompilerParams(vmem_limit_bytes=56 * 1024 * 1024),
        name="update",
    )(gf, gw, gd, nm, sq, query_factor, out_factor, query_w, out_w)
    outs = list(outs)
    outs[1], outs[3] = outs[1].T, outs[3].T
    return tuple(outs)


def solution(mesh):
    finer = Mesh(mesh.devices.reshape(NZ, NY, NX, 2), (Z, Y, X, C))
    in_specs = (
        P(FS_REP, None),
        P(FS_REP, C),
        P(FS_REP, None),
        P(FS_REP, C),
        P(FS, C),
        P(C, FS),
        P(FS, None),
        P(FS, None),
        *[P(FS, C)] * 4,
    )
    out_specs = (
        P(FS, C),
        P(C, FS),
        P(FS, C),
        P(C, FS),
        *[P(FS, C)] * 4,
        P(None, C),
        P(C, None),
    )
    return jax.shard_map(body, mesh=finer, in_specs=in_specs, out_specs=out_specs, check_vma=False)
```

```python
import math

import jax
import jax.numpy as jnp
from jax import lax
from jax.experimental import pallas as pl
from jax.experimental.pallas import tpu as pltpu
from jax.sharding import Mesh
from jax.sharding import PartitionSpec as P

NZ, NY, NX = 8, 4, 4
NF = NZ * NY
D, RANK, HQ, TOKENS = 2048, 512, 1024, 98304
HALF = HQ // 2
TOK = TOKENS // (NF * NX)
ROWS = D // NF
MINE = RANK // NF
BLOCKS = 4
Z, Y, X, C = "fs_0", "fs_1", "rep", "tp"
FS = (Z, Y)
FS_REP = (Z, Y, X)
BF, F32 = jnp.bfloat16, jnp.float32
MESH = pl.DeviceIdType.MESH


def along(n, mode, flip):
    up, down = (n // 2, n - 1 - n // 2)[:: -1 if flip else 1]
    tree = {}
    for s, far in ((1, up), (-1, down)):
        if mode == "ring":
            hops = [(k, 1) for k in range(far)]
        elif mode == "direct":
            hops = [(0, k) for k in range(far, 0, -1)]
        else:
            hops = [(0, 2), (0, 1), (2, 2), (2, 1)]
        for at, by in hops:
            if at + by <= far:
                tree.setdefault(s * at, []).append((s, by, s * (at + by)))
    return tree, range(-down, up + 1)


def broadcast(axes, flip):
    (axis_1, mode_1), (axis_2, mode_2) = axes
    sizes = {Z: NZ, Y: NY}
    tree_1, span = along(sizes[axis_1], mode_1, flip)
    events = {}
    for i in span:
        tree_2, across = along(sizes[axis_2], mode_2, (i + flip) % 2)
        for j in across:
            on = [(axis_2, s, d, (i, to)) for s, d, to in tree_2.get(j, [])]
            if j == 0:
                on = [(axis_1, s, d, (to, 0)) for s, d, to in tree_1.get(i, [])] + on
            events[i, j] = on
    return events


def expected_order(gathers):
    free, now, order = {}, 0.0, []
    heap = [(0.01 * g.number, g.number, (0, 0)) for g in gathers]
    by_number = {g.number: g for g in gathers}
    while heap:
        heap.sort()
        when, number, key = heap.pop(0)
        now, g = max(now, when), by_number[number]
        if key != (0, 0):
            order.append((when, g, key))
        for axis, sign, distance, landed in g.events[key]:
            now += 0.02
            begin = max(free.get((axis, sign), 0.0), now)
            wire = g.kib / 91.0
            free[axis, sign] = begin + wire * distance
            heap.append((begin + wire + 2.0 + 0.75 * (distance - 1), number, landed))
    return order


class Gather:
    def __init__(self, number, axes, flip, kib, pieces, many, share, shares, where, sems, core):
        self.number, self.axes, self.kib = number, [a for a, _ in axes], kib
        self.events = broadcast(axes, flip)
        self.slots = {key: n for n, key in enumerate(k for k in self.events if k != (0, 0))}
        self.pieces, self.many, self.share, self.shares = pieces, many, share, shares
        self.where, self.core = where, core
        self.send_sem, self.recv_sem, self.pass_sem, self.give_sem = sems

    def index(self, key):
        off = dict(zip(self.axes, key))
        z = lax.rem(self.where[Z] + (NZ - off[Z]), NZ)
        y = lax.rem(self.where[Y] + (NY - off[Y]), NY)
        return z * NY + y

    def copy(self, ref, axis, by, slot):
        n = NZ if axis == Z else NY
        return pltpu.make_async_remote_copy(
            src_ref=ref,
            dst_ref=ref,
            send_sem=self.send_sem,
            recv_sem=self.recv_sem.at[slot],
            device_id={axis: lax.rem(self.where[axis] + (n + by), n)},
            device_id_type=MESH,
        )

    def give(self, ref):
        return pltpu.make_async_remote_copy(
            src_ref=ref,
            dst_ref=ref,
            send_sem=self.pass_sem,
            recv_sem=self.give_sem,
            device_id={C: self.core},
            device_id_type=MESH,
        )

    def pass_on(self, key):
        f = self.index(key)
        for axis, sign, distance, landed in self.events[key]:
            for ref in self.pieces(f):
                self.copy(ref, axis, sign * distance, self.slots[landed]).start()

    def start(self):
        self.pass_on((0, 0))

    def arrive(self, key):
        f = self.index(key)
        self.copy(self.many(1), Z, 1, self.slots[key]).wait_recv()
        self.pass_on(key)
        if self.share is not None:
            self.give(self.share(f)).start()
        return f

    def finish(self):
        self.copy(self.many(PIECES), Z, 1, 0).wait_send()
        if self.shares is not None:
            self.give(self.shares()).wait_send()

    def given(self):
        self.give(self.shares()).wait_recv()


PIECES = NF - 1
ZY_RING, YZ_RING = ((Z, "ring"), (Y, "ring")), ((Y, "ring"), (Z, "ring"))
ZY_FAST, YZ_FAST = ((Z, "skip"), (Y, "ring")), ((Y, "direct"), (Z, "skip"))
YZ_LEAN = ((Y, "direct"), (Z, "ring"))


def reduce_kernel(*refs):
    (
        input_act, query_cot, out_cot, attn_out, query_w, out_w, query_factor, out_factor,
        first_q, second_q, first_o, second_o,
        gf_out, gw_out, gd_out, nm_out, sq_out,
        gf, gw, gd, act, cot, qw, ow, moments, low, px, rx1, rx2, s1, ry, s2,
        rz, sp, sq, sq_parts, nm,
        load, f_send, f_recv, f_pass, f_give, w_send, w_pass, w_give,
        d_send, d_pass, d_give, own_send, own_recv, mom_send, mom_recv,
        cot_send, cot_recv, px_send, px_recv,
        rx1_send, rx1_recv, rx2_send, rx2_recv, ry_send, ry_recv, rz_send, rz_recv,
        sp_send, sp_recv, nm_sem, sq_sem, out_sem,
    ) = refs
    z, y, x, c = (lax.axis_index(a) for a in (Z, Y, X, C))
    f = z * NY + y
    where = {Z: z, Y: y}
    other = 1 - c
    leads, follows = pl.when(c == 1), pl.when(c == 0)

    def load_own(number, if_q, if_o, dst):
        @follows
        def _():
            pltpu.make_async_copy(if_q, dst, load.at[number]).start()

        @leads
        def _():
            pltpu.make_async_copy(if_o, dst, load.at[number]).start()

        return pltpu.make_async_copy(if_q, dst, load.at[number])

    def load_plain(number, src, dst):
        cp = pltpu.make_async_copy(src, dst, load.at[number])
        cp.start()
        return cp

    for j in range(4):
        cols = pl.ds(128 * j, 128)
        for t, factor in enumerate((query_factor, out_factor)):
            load_plain(0, factor.at[:, cols], gf.at[j, f, t])
    w_loads = [load_plain(1, query_w, qw), load_plain(2, out_w, ow)]
    act_load = load_own(3, input_act, out_cot, act)
    for k in range(2):
        cols = pl.ds(256 * k, 256)
        _ = load_own(4, query_cot.at[:, cols], attn_out.at[:, cols], cot.at[2 * c + k])

    barrier = pltpu.get_barrier_semaphore()
    peers = [{C: other}]
    for axis, at, n in ((Z, z, NZ), (Y, y, NY), (X, x, NX)):
        peers += [{axis: lax.rem(at + 1, n)}, {axis: lax.rem(at + n - 1, n)}]
    peers += [{Z: lax.rem(z + 2, NZ)}, {Z: lax.rem(z + NZ - 2, NZ)}, {Y: lax.rem(y + 2, NY)}]
    for peer in peers:
        pl.semaphore_signal(barrier, inc=1, device_id=peer, device_id_type=MESH)

    for w in w_loads:
        w.wait()
    for k in range(2):
        gw[4 * k + 2 * c, f] = qw[:, 256 * k : 256 * k + 256].astype(BF)
        gw[4 * k + 2 * c + 1, f] = ow[:, 256 * k : 256 * k + 256].astype(BF)
    factors = gf.at[0, pl.ds(0, 4)]
    pltpu.make_async_copy(factors, factors, load.at[0]).wait()
    pl.semaphore_wait(barrier, len(peers))

    def factor_gather(j):
        return Gather(
            j, ZY_FAST if j % 2 == 0 else YZ_LEAN, (j % 2) ^ (j // 2), 32,
            lambda p: (gf.at[j, p],), lambda n: gf.at[j, pl.ds(0, n)],
            lambda p: gf.at[j, p], lambda: gf.at[j, pl.ds(0, PIECES)],
            where, [a.at[j] for a in (f_send, f_recv, f_pass, f_give)], 0,
        )

    blocks = ((0, 2, 6), (2, 2, None), (4, 2, None), (7, 1, None))

    def weight_gather(k):
        first, count, more = blocks[k]

        def pieces(p):
            refs = (gw.at[pl.ds(first, count), p],)
            return refs if more is None else refs + (gw.at[more, p],)

        total = count + (more is not None)
        give = (lambda p: gw.at[6, p]) if k == 0 else (lambda p: pieces(p)[0])
        return Gather(
            k, (ZY_RING, YZ_RING)[k % 2] if k != 2 else ZY_RING, (0, 1, 1, 0)[k], 32 * total,
            pieces, lambda n: gw.at[pl.ds(0, total), pl.ds(0, n)],
            None if k == 2 else give, None,
            where, (w_send.at[k], f_recv.at[k], w_pass, w_give), 1,
        )

    def all_shares():
        return every(gw.at[pl.ds(0, 4), pl.ds(0, PIECES)], w_pass, w_give)

    def dir_gather(k):
        return Gather(
            k, ZY_FAST if k == 0 else YZ_FAST, k, 32,
            lambda p: (gd.at[k, p],), lambda n: gd.at[k, pl.ds(0, n)],
            lambda p: gd.at[k, p, 0], lambda: gd.at[k, :, 0],
            where, (d_send.at[k], f_recv.at[k], d_pass.at[k], d_give.at[k]), 0,
        )

    fg = [factor_gather(j) for j in range(4)]
    wg = [weight_gather(k) for k in range(4)]
    dg = [dir_gather(k) for k in range(2)]
    f_order, w_order, d_order = (expected_order(g) for g in (fg, wg, dg))

    @leads
    def _():
        for g in fg:
            g.start()

    def cot_copy(src, k):
        return pltpu.make_async_remote_copy(
            src_ref=src.at[:, pl.ds(256 * k, 256)],
            dst_ref=cot.at[2 * c + k],
            send_sem=cot_send,
            recv_sem=cot_recv,
            device_id={C: other},
            device_id_type=MESH,
        )

    def every(ref, send_sem, recv_sem):
        return pltpu.make_async_remote_copy(
            src_ref=ref,
            dst_ref=ref,
            send_sem=send_sem,
            recv_sem=recv_sem,
            device_id={C: other},
            device_id_type=MESH,
        )

    def both_cots():
        return every(cot.at[pl.ds(0, 2)], cot_send, cot_recv)

    def own_weights(k):
        ref = gw.at[pl.ds(4 * k + 2, 2), f]
        return pltpu.make_async_remote_copy(
            src_ref=ref,
            dst_ref=ref,
            send_sem=own_send,
            recv_sem=own_recv,
            device_id={C: 0},
            device_id_type=MESH,
        )

    def both_weights():
        return every(gw.at[pl.ds(0, 4), f], own_send, own_recv)

    def own_moments(k, m):
        return pltpu.make_async_remote_copy(
            src_ref=m,
            dst_ref=moments.at[k, 0],
            send_sem=mom_send,
            recv_sem=mom_recv,
            device_id={C: 1},
            device_id_type=MESH,
        )

    all_moments = (first_q, second_q, first_o, second_o)

    @follows
    def _():
        for k in range(2):
            cot_copy(attn_out, k).start()
        for k, m in enumerate(all_moments):
            own_moments(k, m).start()

    @leads
    def _():
        for k in range(2):
            cot_copy(query_cot, k).start()
        for k in range(2):
            own_weights(k).start()
        for k, m in enumerate(all_moments):
            pltpu.make_async_copy(m, moments.at[k, 1], load.at[5]).start()

    def project(h):
        def tile(m, _):
            rows = pl.ds(pl.multiple_of(m * 256, 256), 256)
            right = jnp.concatenate(
                [gf[2 * h + j, :, c].reshape(D, 128) for j in range(2)], axis=1
            )
            low[rows, :] = jnp.dot(act[rows, :], right, preferred_element_type=F32).astype(BF)
            return 0

        lax.fori_loop(0, TOK // 256, tile, 0)

        for i in range(NX):
            xb = lax.rem(x + 2 + i, NX)
            dims = (((0,), (0,)), ((), ()))
            total = lax.dot_general(low[...], cot[xb], dims, preferred_element_type=F32)
            px[h, xb, c] = total.astype(BF)

            @follows
            def _():
                partial_over(h, i).start()

            if i == NX - 2:

                @leads
                def _():
                    x_start(h)

    x_up, x_down, x_far = lax.rem(x + 1, NX), lax.rem(x + 3, NX), lax.rem(x + 2, NX)
    sides = ((x_up, 0), (x_down, 1))

    def partial_over(h, i):
        ref = px.at[h, lax.rem(x + 2 + i, NX), 0]
        return pltpu.make_async_remote_copy(
            src_ref=ref,
            dst_ref=ref,
            send_sem=px_send,
            recv_sem=px_recv.at[h, i],
            device_id={C: 1},
            device_id_type=MESH,
        )

    def x_first(h, k):
        return pltpu.make_async_remote_copy(
            src_ref=px.at[h, x_far, :, pl.ds(128 * k, 128)],
            dst_ref=rx1.at[h, k],
            send_sem=rx1_send,
            recv_sem=rx1_recv.at[h, k],
            device_id={X: sides[k][0]},
            device_id_type=MESH,
        )

    def x_second(h, k):
        return pltpu.make_async_remote_copy(
            src_ref=px.at[h, sides[k][0]],
            dst_ref=rx2.at[h, k],
            send_sem=rx2_send,
            recv_sem=rx2_recv.at[h],
            device_id={X: sides[k][0]},
            device_id_type=MESH,
        )

    def x_start(h):
        partial_over(h, 0).wait_recv()
        for k in range(2):
            x_first(h, k).start()

    def x_merge(h):
        for i in (1, 3):
            partial_over(h, i).wait_recv()
        for to, k in sides:
            x_first(h, k).wait_recv()
            rows = pl.ds(128 * k, 128)
            merged = px[h, to, :, rows].astype(F32) + rx1[h, k].astype(F32)
            px[h, to, :, rows] = merged.astype(BF)
            x_second(h, k).start()

    def x_sum(h):
        partial_over(h, 2).wait_recv()
        every(rx2.at[h], rx2_send, rx2_recv.at[h]).wait_recv()
        for t in range(2):
            total = px[h, x, t].astype(F32)
            for k in range(2):
                total += rx2[h, k, t].astype(F32)
            s1[pl.ds(4 * h, 4), :, t] = total.astype(BF).reshape(4, NY, MINE, 256)
        for d in range(1, NY):
            y_copy(h, d).start()

    def y_copy(h, d):
        to = lax.rem(y + d, NY)
        return pltpu.make_async_remote_copy(
            src_ref=s1.at[pl.ds(4 * h, 4), to],
            dst_ref=ry.at[h, d - 1],
            send_sem=ry_send,
            recv_sem=ry_recv.at[h],
            device_id={Y: to},
            device_id_type=MESH,
        )

    def y_sum(h):
        total = s1[pl.ds(4 * h, 4), y].astype(F32)
        every(ry.at[h], ry_send, ry_recv.at[h]).wait_recv()
        for d in range(1, NY):
            total += ry[h, d - 1].astype(F32)
        s2[pl.ds(4 * h, 4)] = total.astype(BF)

    def z_copy(d):
        to = lax.rem(z + d, NZ)
        return pltpu.make_async_remote_copy(
            src_ref=s2.at[to],
            dst_ref=rz.at[d - 1],
            send_sem=rz_send,
            recv_sem=rz_recv,
            device_id={Z: to},
            device_id_type=MESH,
        )

    def sum_copy(d):
        return pltpu.make_async_remote_copy(
            src_ref=sp.at[0],
            dst_ref=sp.at[d],
            send_sem=sp_send,
            recv_sem=sp_recv,
            device_id={X: lax.rem(x + d, NX)},
            device_id_type=MESH,
        )

    def all_sums():
        return every(sp.at[pl.ds(1, NX - 1)], sp_send, sp_recv)

    def moments_over():
        return pltpu.make_async_remote_copy(
            src_ref=nm.at[:, 0],
            dst_ref=nm_out,
            send_sem=nm_sem.at[0],
            recv_sem=nm_sem.at[1],
            device_id={C: 0},
            device_id_type=MESH,
        )

    def squares(t, at):
        part = jnp.square(gd[t, at].astype(F32)).reshape(2 * MINE // 8, 8, HALF)
        part = jnp.sum(part, axis=0)
        return part[:, :128] + part[:, 128:256] + part[:, 256:384] + part[:, 384:]

    def dir_out(t, at):
        return pltpu.make_async_copy(gd.at[t, at, 1], gd_out.at[t, at], out_sem.at[5])

    def own_dirs(t):
        return dg[t].give(gd.at[t, f, 0])

    outs = []

    def put(number, src, dst):
        cp = pltpu.make_async_copy(src, dst, out_sem.at[number])
        cp.start()
        outs.append(cp)

    @leads
    def _():
        for _, g, key in f_order:
            g.arrive(key)

    @follows
    def _():
        both_weights().wait_recv()
        fg[0].given()
        for g in wg:
            g.start()
        fg[1].given()

    act_load.wait()
    cot_half = cot.at[pl.ds(0, 2)]
    pltpu.make_async_copy(cot_half, cot_half, load.at[4]).wait()
    both_cots().wait_recv()
    project(0)

    @follows
    def _():
        for g in fg[2:]:
            g.given()

    project(1)
    put(0, gf, gf_out)

    @leads
    def _():
        x_merge(0)
        x_merge(1)
        x_sum(0)
        x_sum(1)
        y_sum(0)
        y_sum(1)
        for d in range(1, NZ):
            z_copy(d).start()
        total = s2[z].astype(F32)
        every(rz, rz_send, rz_recv).wait_recv()
        for d in range(1, NZ):
            total += rz[d - 1].astype(F32)
        sp[0] = total
        for d in range(1, NX):
            sum_copy(d).start()
        every(moments.at[:, 0], mom_send, mom_recv).wait_recv()
        pltpu.make_async_copy(moments.at[:, 1], moments.at[:, 1], load.at[5]).wait()
        all_sums().wait_recv()

        for t in range(2):
            for p in range(2):
                proj = jnp.concatenate(
                    [sp[lax.rem(x + (NX - q), NX), t] for q in (2 * p, 2 * p + 1)], axis=1
                )
                proj = proj * (1.0 / math.sqrt(TOKENS))
                first = 0.8 * moments[2 * t, p] + 0.2 * proj
                second = 0.9 * moments[2 * t + 1, p] + 0.1 * proj * proj
                nm[2 * t, p] = first
                nm[2 * t + 1, p] = second
                gd[t, f, p] = (first / jnp.sqrt(second)).astype(BF)
            dg[t].start()
            own_dirs(t).start()
            dir_out(t, f).start()
            sq_parts[t, f] = squares(t, f)
        moments_over().start()
        pltpu.make_async_copy(nm.at[:, 1], nm_out, out_sem.at[4]).start()
        for _, g, key in d_order:
            at = g.arrive(key)
            dir_out(g.number, at).start()
            sq_parts[g.number, at] = squares(g.number, at)
        all_shares().wait_recv()

    @follows
    def _():
        for _, g, key in w_order:
            g.arrive(key)

    put(1, gw.at[pl.ds(2 * c, 2)], gw_out.at[pl.ds(0, 2)])
    put(3, gw.at[pl.ds(4 + 2 * c, 2)], gw_out.at[pl.ds(2, 2)])

    @leads
    def _():
        total = jnp.sum(sq_parts[...].reshape(2 * NF, 8, 128), axis=0)
        sq[...] = jnp.broadcast_to(jnp.sum(total, axis=(0, 1), keepdims=True), (8, 128))

    squares_over = pltpu.make_async_remote_copy(
        src_ref=sq,
        dst_ref=sq,
        send_sem=sq_sem.at[0],
        recv_sem=sq_sem.at[1],
        device_id={C: 0},
        device_id_type=MESH,
    )

    @leads
    def _():
        squares_over.start()

    @follows
    def _():
        for t in range(2):
            dg[t].given()

    @follows
    def _():
        pltpu.make_async_copy(gd.at[:, :, 0], gd_out, out_sem.at[5]).start()


    @follows
    def _():
        squares_over.wait_recv()

    put(2, sq, sq_out)

    @leads
    def _():
        for g in fg + dg:
            g.finish()
        both_weights().wait_send()
        every(rx1, rx1_send, rx1_recv.at[0, 0]).wait_send()
        every(rx2, rx2_send, rx2_recv.at[0]).wait_send()
        every(ry, ry_send, ry_recv.at[0]).wait_send()
        every(rz, rz_send, rz_recv).wait_send()
        all_sums().wait_send()
        moments_over().wait_send()
        pltpu.make_async_copy(nm.at[:, 1], nm_out, out_sem.at[4]).wait()
        squares_over.wait_send()

    @follows
    def _():
        for g in wg:
            g.finish()
        all_shares().wait_send()
        every(moments.at[:, 0], mom_send, mom_recv).wait_send()
        moments_over().wait_recv()
        every(px.at[:, :, 0], px_send, px_recv.at[0, 0]).wait_send()

    both_cots().wait_send()
    for cp in outs:
        cp.wait()
    pltpu.make_async_copy(gd.at[:, :, c], gd_out, out_sem.at[5]).wait()


def update_kernel(
    gf_in, gw_in, gd_in, nm_in, sq_in, query_factor, out_factor, query_w, out_w,
    new_qw, new_ow, q_step, o_step, nf_q, ns_q, nf_o, ns_o, q_copy, o_copy,
    gf, gw, gd, nm, sq, factor, w, steps, new_w, new_q, new_o,
    first_sem, block_sem, small_sem, copy_sem, out_sem,
):
    copy = pltpu.make_async_copy
    per = NF // BLOCKS
    size = D // BLOCKS
    first = [copy(gd_in, gd, first_sem.at[0]), copy(sq_in, sq, first_sem.at[1])]
    small = [copy(nm_in, nm, small_sem.at[0])]
    for t, (fac, old) in enumerate(((query_factor, query_w), (out_factor, out_w))):
        small.append(copy(fac, factor.at[t], small_sem.at[1 + 2 * t]))
        small.append(copy(old, w.at[t], small_sem.at[2 + 2 * t]))

    def block_loads(b):
        some = pl.ds(per * b, per)
        return (
            copy(gf_in.at[:, some], gf.at[:, some], block_sem.at[0, b]),
            copy(gw_in.at[:, some], gw.at[:, some], block_sem.at[1, b]),
        )

    def block_stores(b):
        at = pl.ds(pl.multiple_of(size * b, size), size)
        return (
            copy(new_q.at[b], q_copy.at[at], copy_sem.at[0]),
            copy(new_o.at[b], o_copy.at[:, at], copy_sem.at[1]),
        )

    for cp in first + small:
        cp.start()
    for cp in block_loads(0):
        cp.start()
    for cp in first:
        cp.wait()
    for cp in block_loads(1) + block_loads(2):
        cp.start()
    inverse = 1.0 / jnp.sqrt(sq[0:1] / (2 * RANK * HQ) + 1e-06)
    inverse = jnp.concatenate([inverse] * 4, axis=1)
    def block(b, _):
        some = pl.ds(per * b, per)
        @pl.when(b + 3 < BLOCKS)
        def _():
            for cp in block_loads(b + 3):
                cp.start()

        for cp in block_loads(b):
            cp.wait()
        moved = []
        for t in range(2):
            rows = jnp.concatenate([gf[j, some, t].reshape(size, 128) for j in range(4)], axis=1)
            step = jnp.dot(rows, gd[t].reshape(RANK, HALF), preferred_element_type=F32)
            old = jnp.concatenate([gw[i, some].reshape(size, 256) for i in (t, 2 + t)], axis=1)
            moved.append(old.astype(F32) - (0.01 * inverse) * step)
        new_q[b] = moved[0].astype(BF)
        new_o[b] = moved[1].astype(BF).T
        for cp in block_stores(b):
            cp.start()
        return 0

    lax.fori_loop(0, BLOCKS, block, 0)
    for cp in small:
        cp.wait()
    stores = [copy(nm.at[k], o, out_sem.at[k]) for k, o in enumerate((nf_q, ns_q, nf_o, ns_o))]
    for t, (to_step, to_w) in enumerate(((q_step, new_qw), (o_step, new_ow))):
        step = jnp.dot(factor[t], gd[t].reshape(RANK, HALF), preferred_element_type=F32)
        step = step * inverse
        steps[t] = step
        new_w[t] = w[t] - 0.01 * step
        stores.append(copy(steps.at[t], to_step, out_sem.at[4 + 2 * t]))
        stores.append(copy(new_w.at[t], to_w, out_sem.at[5 + 2 * t]))
    for cp in stores:
        cp.start()
    for cp in stores:
        cp.wait()
    copy(new_q, new_q, copy_sem.at[0]).wait()
    copy(new_o, new_o, copy_sem.at[1]).wait()


def body(
    input_act, query_cot, out_cot, attn_out, query_w, out_w, query_factor, out_factor,
    first_q, second_q, first_o, second_o,
):
    struct = jax.ShapeDtypeStruct
    dma = pltpu.SemaphoreType.DMA
    vmem = pltpu.VMEM
    out_w = out_w.T
    scratch = [
        vmem((4, NF, 2, ROWS, 128), BF),
        vmem((8, NF, ROWS, 256), BF),
        vmem((2, NF, 2, MINE, HALF), BF),
        vmem((TOK, D), BF),
        vmem((4, TOK, 256), BF),
        vmem((ROWS, HALF), F32),
        vmem((ROWS, HALF), F32),
        vmem((4, 2, MINE, HALF), F32),
        vmem((TOK, 256), BF),
        vmem((2, NX, 2, 256, 256), BF),
        vmem((2, 2, 2, 128, 256), BF),
        vmem((2, 2, 2, 256, 256), BF),
        vmem((NZ, NY, 2, MINE, 256), BF),
        vmem((2, NY - 1, 4, 2, MINE, 256), BF),
        vmem((NZ, 2, MINE, 256), BF),
        vmem((NZ - 1, 2, MINE, 256), BF),
        vmem((NX, 2, MINE, 256), F32),
        vmem((8, 128), F32),
        vmem((2, NF, 8, 128), F32),
        vmem((4, 2, MINE, HALF), F32),
        dma((6,)),
        dma((4,)), dma((4, PIECES)), dma((4,)), dma((4,)),
        dma((4,)), dma, dma,
        dma((2,)), dma((2,)), dma((2,)),
        dma, dma, dma, dma, dma, dma,
        dma, dma((2, NX)),
        dma, dma((2, 2)), dma, dma((2,)),
        dma, dma((2,)), dma, dma, dma, dma,
        dma((2,)), dma((2,)), dma((6,)),
    ]
    gf, gw, gd, nm, sq = pl.pallas_call(
        reduce_kernel,
        out_shape=(
            struct((4, NF, 2, ROWS, 128), BF),
            struct((4, NF, ROWS, 256), BF),
            struct((2, NF, MINE, HALF), BF),
            struct((4, MINE, HALF), F32),
            struct((8, 128), F32),
        ),
        in_specs=[pl.BlockSpec(memory_space=pl.ANY)] * 12,
        out_specs=[pl.BlockSpec(memory_space=pl.ANY)] * 5,
        scratch_shapes=scratch,
        compiler_params=pltpu.CompilerParams(
            collective_id=0, has_side_effects=True, vmem_limit_bytes=56 * 1024 * 1024
        ),
        name="reduce",
    )(
        input_act, query_cot, out_cot, attn_out, query_w, out_w, query_factor, out_factor,
        first_q, second_q, first_o, second_o,
    )

    anywhere = pl.BlockSpec(memory_space=pl.ANY)
    shard, small = struct((ROWS, HALF), F32), struct((MINE, HALF), F32)
    outs = pl.pallas_call(
        update_kernel,
        out_shape=(
            *[shard] * 4,
            *[small] * 4,
            struct((D, HALF), BF),
            struct((HALF, D), BF),
        ),
        in_specs=[anywhere] * 9,
        out_specs=[anywhere] * 10,
        scratch_shapes=[
            vmem((4, NF, 2, ROWS, 128), BF),
            vmem((4, NF, ROWS, 256), BF),
            vmem((2, NF, MINE, HALF), BF),
            vmem((4, MINE, HALF), F32),
            vmem((8, 128), F32),
            vmem((2, ROWS, RANK), BF),
            vmem((2, ROWS, HALF), F32),
            vmem((2, ROWS, HALF), F32),
            vmem((2, ROWS, HALF), F32),
            vmem((BLOCKS, D // BLOCKS, HALF), BF),
            vmem((BLOCKS, HALF, D // BLOCKS), BF),
            dma((2,)),
            dma((2, BLOCKS)),
            dma((5,)),
            dma((2,)),
            dma((8,)),
        ],
        compiler_params=pltpu.CompilerParams(vmem_limit_bytes=56 * 1024 * 1024),
        name="update",
    )(gf, gw, gd, nm, sq, query_factor, out_factor, query_w, out_w)
    outs = list(outs)
    outs[1], outs[3] = outs[1].T, outs[3].T
    return tuple(outs)


def solution(mesh):
    finer = Mesh(mesh.devices.reshape(NZ, NY, NX, 2), (Z, Y, X, C))
    in_specs = (
        P(FS_REP, None),
        P(FS_REP, C),
        P(FS_REP, None),
        P(FS_REP, C),
        P(FS, C),
        P(C, FS),
        P(FS, None),
        P(FS, None),
        *[P(FS, C)] * 4,
    )
    out_specs = (
        P(FS, C),
        P(C, FS),
        P(FS, C),
        P(C, FS),
        *[P(FS, C)] * 4,
        P(None, C),
        P(C, None),
    )
    return jax.shard_map(body, mesh=finer, in_specs=in_specs, out_specs=out_specs, check_vma=False)
```

```python
import math

import jax
import jax.numpy as jnp
from jax import lax
from jax.experimental import pallas as pl
from jax.experimental.pallas import tpu as pltpu
from jax.sharding import Mesh
from jax.sharding import PartitionSpec as P

NZ, NY, NX = 8, 4, 4
NF = NZ * NY
D, RANK, HQ, TOKENS = 2048, 512, 1024, 98304
HALF = HQ // 2
TOK = TOKENS // (NF * NX)
ROWS = D // NF
MINE = RANK // NF
BLOCKS = 4
Z, Y, X, C = "fs_0", "fs_1", "rep", "tp"
FS = (Z, Y)
FS_REP = (Z, Y, X)
BF, F32 = jnp.bfloat16, jnp.float32
MESH = pl.DeviceIdType.MESH


def along(n, mode, flip):
    up, down = (n // 2, n - 1 - n // 2)[:: -1 if flip else 1]
    tree = {}
    for s, far in ((1, up), (-1, down)):
        if mode == "ring":
            hops = [(k, 1) for k in range(far)]
        elif mode == "direct":
            hops = [(0, k) for k in range(far, 0, -1)]
        else:
            hops = [(0, 2), (0, 1), (2, 2), (2, 1)]
        for at, by in hops:
            if at + by <= far:
                tree.setdefault(s * at, []).append((s, by, s * (at + by)))
    return tree, range(-down, up + 1)


def broadcast(axes, flip):
    (axis_1, mode_1), (axis_2, mode_2) = axes
    sizes = {Z: NZ, Y: NY}
    tree_1, span = along(sizes[axis_1], mode_1, flip)
    events = {}
    for i in span:
        tree_2, across = along(sizes[axis_2], mode_2, (i + flip) % 2)
        for j in across:
            on = [(axis_2, s, d, (i, to)) for s, d, to in tree_2.get(j, [])]
            if j == 0:
                on = [(axis_1, s, d, (to, 0)) for s, d, to in tree_1.get(i, [])] + on
            events[i, j] = on
    return events


def expected_order(gathers):
    free, now, order = {}, 0.0, []
    heap = [(0.01 * g.number, g.number, (0, 0)) for g in gathers]
    by_number = {g.number: g for g in gathers}
    while heap:
        heap.sort()
        when, number, key = heap.pop(0)
        now, g = max(now, when), by_number[number]
        if key != (0, 0):
            order.append((when, g, key))
        for axis, sign, distance, landed in g.events[key]:
            now += 0.02
            begin = max(free.get((axis, sign), 0.0), now)
            wire = g.kib / 91.0
            free[axis, sign] = begin + wire * distance
            heap.append((begin + wire + 2.0 + 0.75 * (distance - 1), number, landed))
    return order


class Gather:
    def __init__(self, number, axes, flip, kib, pieces, many, share, shares, where, sems, core):
        self.number, self.axes, self.kib = number, [a for a, _ in axes], kib
        self.events = broadcast(axes, flip)
        self.slots = {key: n for n, key in enumerate(k for k in self.events if k != (0, 0))}
        self.pieces, self.many, self.share, self.shares = pieces, many, share, shares
        self.where, self.core = where, core
        self.send_sem, self.recv_sem, self.pass_sem, self.give_sem = sems

    def index(self, key):
        off = dict(zip(self.axes, key))
        z = lax.rem(self.where[Z] + (NZ - off[Z]), NZ)
        y = lax.rem(self.where[Y] + (NY - off[Y]), NY)
        return z * NY + y

    def copy(self, ref, axis, by, slot):
        n = NZ if axis == Z else NY
        return pltpu.make_async_remote_copy(
            src_ref=ref,
            dst_ref=ref,
            send_sem=self.send_sem,
            recv_sem=self.recv_sem.at[slot],
            device_id={axis: lax.rem(self.where[axis] + (n + by), n)},
            device_id_type=MESH,
        )

    def give(self, ref):
        return pltpu.make_async_remote_copy(
            src_ref=ref,
            dst_ref=ref,
            send_sem=self.pass_sem,
            recv_sem=self.give_sem,
            device_id={C: self.core},
            device_id_type=MESH,
        )

    def pass_on(self, key):
        f = self.index(key)
        for axis, sign, distance, landed in self.events[key]:
            for ref in self.pieces(f):
                self.copy(ref, axis, sign * distance, self.slots[landed]).start()

    def start(self):
        self.pass_on((0, 0))

    def arrive(self, key):
        f = self.index(key)
        self.copy(self.many(1), Z, 1, self.slots[key]).wait_recv()
        self.pass_on(key)
        if self.share is not None:
            self.give(self.share(f)).start()
        return f

    def finish(self):
        self.copy(self.many(PIECES), Z, 1, 0).wait_send()
        if self.shares is not None:
            self.give(self.shares()).wait_send()

    def given(self):
        self.give(self.shares()).wait_recv()


PIECES = NF - 1
EARLY = 6
ZY_RING, YZ_RING = ((Z, "ring"), (Y, "ring")), ((Y, "ring"), (Z, "ring"))
ZY_FAST, YZ_FAST = ((Z, "skip"), (Y, "ring")), ((Y, "direct"), (Z, "skip"))


def reduce_kernel(*refs):
    (
        input_act, query_cot, out_cot, attn_out, query_w, out_w, query_factor, out_factor,
        first_q, second_q, first_o, second_o,
        gf_out, gw_out, gd_out, nm_out, sq_out,
        gf, gw, gd, act, cot, qw, ow, moments, low, px, rx1, rx2, s1, ry, s2,
        rz, sp, sq, sq_parts, nm,
        load, f_send, f_recv, f_pass, f_give, w_send, w_pass, w_give, near_end,
        d_send, d_pass, d_give, own_send, own_recv, mom_send, mom_recv,
        cot_send, cot_recv, px_send, px_recv,
        rx1_send, rx1_recv, rx2_send, rx2_recv, ry_send, ry_recv, rz_send, rz_recv,
        sp_send, sp_recv, nm_sem, sq_sem, out_sem,
    ) = refs
    z, y, x, c = (lax.axis_index(a) for a in (Z, Y, X, C))
    f = z * NY + y
    where = {Z: z, Y: y}
    other = 1 - c
    leads, follows = pl.when(c == 1), pl.when(c == 0)

    def load_own(number, if_q, if_o, dst):
        @follows
        def _():
            pltpu.make_async_copy(if_q, dst, load.at[number]).start()

        @leads
        def _():
            pltpu.make_async_copy(if_o, dst, load.at[number]).start()

        return pltpu.make_async_copy(if_q, dst, load.at[number])

    def load_plain(number, src, dst):
        cp = pltpu.make_async_copy(src, dst, load.at[number])
        cp.start()
        return cp

    for j in range(4):
        cols = pl.ds(128 * j, 128)
        for t, factor in enumerate((query_factor, out_factor)):
            load_plain(0, factor.at[:, cols], gf.at[2 * j + t, f])
    w_loads = [load_plain(1, query_w, qw), load_plain(2, out_w, ow)]
    act_load = load_own(3, input_act, out_cot, act)
    for k in range(2):
        cols = pl.ds(256 * k, 256)
        _ = load_own(4, query_cot.at[:, cols], attn_out.at[:, cols], cot.at[2 * c + k])

    barrier = pltpu.get_barrier_semaphore()
    peers = [{C: other}]
    for axis, at, n in ((Z, z, NZ), (Y, y, NY), (X, x, NX)):
        peers += [{axis: lax.rem(at + 1, n)}, {axis: lax.rem(at + n - 1, n)}]
    peers += [{Z: lax.rem(z + 2, NZ)}, {Z: lax.rem(z + NZ - 2, NZ)}, {Y: lax.rem(y + 2, NY)}]
    for peer in peers:
        pl.semaphore_signal(barrier, inc=1, device_id=peer, device_id_type=MESH)

    for w in w_loads:
        w.wait()
    for k in range(2):
        gw[4 * c + 2 * k, f] = qw[:, 256 * k : 256 * k + 256].astype(BF)
        gw[4 * c + 2 * k + 1, f] = ow[:, 256 * k : 256 * k + 256].astype(BF)
    factors = gf.at[:, f]
    pltpu.make_async_copy(factors, factors, load.at[0]).wait()
    pl.semaphore_wait(barrier, len(peers))

    parts = (pl.ds(0, 5), pl.ds(5, 3))

    def factor_gather(k):
        return Gather(
            k, (ZY_FAST, YZ_RING)[k], 1 - k, (80, 48)[k],
            lambda p: (gf.at[parts[k], p],), lambda n: gf.at[parts[k], pl.ds(0, n)],
            lambda p: gf.at[parts[k], p], lambda: gf.at[parts[k], pl.ds(0, PIECES)],
            where, [a.at[k] for a in (f_send, f_recv, f_pass, f_give)], 0,
        )

    def weight_gather(k):
        give = (pl.ds(4, 1), parts[1])[k]
        return Gather(
            k, (ZY_RING, YZ_RING)[k], k, (160, 96)[k],
            lambda p: (gw.at[parts[k], p],), lambda n: gw.at[parts[k], pl.ds(0, n)],
            lambda p: gw.at[give, p], None,
            where, (w_send.at[k], f_recv.at[k], w_pass, w_give), 1,
        )

    def all_shares():
        return every(gw.at[pl.ds(4, 4), pl.ds(0, PIECES)], w_pass, w_give)

    def dir_gather(k):
        return Gather(
            k, ZY_FAST if k == 0 else YZ_FAST, k, 32,
            lambda p: (gd.at[k, p],), lambda n: gd.at[k, pl.ds(0, n)],
            lambda p: gd.at[k, p, 0], lambda: gd.at[k, :, 0],
            where, (d_send.at[k], f_recv.at[k], d_pass.at[k], d_give.at[k]), 0,
        )

    fg = [factor_gather(k) for k in range(2)]
    wg = [weight_gather(k) for k in range(2)]
    dg = [dir_gather(k) for k in range(2)]
    f_order, w_order, d_order = (expected_order(g) for g in (fg, wg, dg))

    @leads
    def _():
        for g in fg:
            g.start()

    def cot_copy(src, k):
        return pltpu.make_async_remote_copy(
            src_ref=src.at[:, pl.ds(256 * k, 256)],
            dst_ref=cot.at[2 * c + k],
            send_sem=cot_send,
            recv_sem=cot_recv,
            device_id={C: other},
            device_id_type=MESH,
        )

    def every(ref, send_sem, recv_sem):
        return pltpu.make_async_remote_copy(
            src_ref=ref,
            dst_ref=ref,
            send_sem=send_sem,
            recv_sem=recv_sem,
            device_id={C: other},
            device_id_type=MESH,
        )

    def both_cots():
        return every(cot.at[pl.ds(0, 2)], cot_send, cot_recv)

    def own_weights():
        return every(gw.at[pl.ds(4, 4), f], own_send, own_recv)

    def own_moments(k, m):
        return pltpu.make_async_remote_copy(
            src_ref=m,
            dst_ref=moments.at[k, 0],
            send_sem=mom_send,
            recv_sem=mom_recv,
            device_id={C: 1},
            device_id_type=MESH,
        )

    all_moments = (first_q, second_q, first_o, second_o)

    @follows
    def _():
        for k in range(2):
            cot_copy(attn_out, k).start()
        for k, m in enumerate(all_moments):
            own_moments(k, m).start()

    @leads
    def _():
        for k in range(2):
            cot_copy(query_cot, k).start()
        own_weights().start()
        for k, m in enumerate(all_moments):
            pltpu.make_async_copy(m, moments.at[k, 1], load.at[5]).start()

    def project(h):
        def tile(m, _):
            rows = pl.ds(pl.multiple_of(m * 256, 256), 256)
            right = jnp.concatenate(
                [gf[2 * (2 * h + j) + c].reshape(D, 128) for j in range(2)], axis=1
            )
            low[rows, :] = jnp.dot(act[rows, :], right, preferred_element_type=F32).astype(BF)
            return 0

        lax.fori_loop(0, TOK // 256, tile, 0)
        if h:
            @leads
            def _():
                x_start(0)

        for i in range(NX):
            xb = lax.rem(x + 2 + i, NX)
            dims = (((0,), (0,)), ((), ()))
            total = lax.dot_general(low[...], cot[xb], dims, preferred_element_type=F32)
            px[h, xb, c] = total.astype(BF)

            @follows
            def _():
                partial_over(h, i).start()

        if h:

            @leads
            def _():
                x_start(1)

    x_up, x_down, x_far = lax.rem(x + 1, NX), lax.rem(x + 3, NX), lax.rem(x + 2, NX)
    sides = ((x_up, 0), (x_down, 1))

    def partial_over(h, i):
        ref = px.at[h, lax.rem(x + 2 + i, NX), 0]
        return pltpu.make_async_remote_copy(
            src_ref=ref,
            dst_ref=ref,
            send_sem=px_send,
            recv_sem=px_recv.at[h, i],
            device_id={C: 1},
            device_id_type=MESH,
        )

    def x_first(h, k):
        return pltpu.make_async_remote_copy(
            src_ref=px.at[h, x_far, :, pl.ds(128 * k, 128)],
            dst_ref=rx1.at[h, k],
            send_sem=rx1_send,
            recv_sem=rx1_recv.at[h, k],
            device_id={X: sides[k][0]},
            device_id_type=MESH,
        )

    def x_second(h, k):
        return pltpu.make_async_remote_copy(
            src_ref=px.at[h, sides[k][0]],
            dst_ref=rx2.at[h, k],
            send_sem=rx2_send,
            recv_sem=rx2_recv.at[h],
            device_id={X: sides[k][0]},
            device_id_type=MESH,
        )

    def x_start(h):
        partial_over(h, 0).wait_recv()
        for k in range(2):
            x_first(h, k).start()

    def x_merge(h):
        for i in (1, 3):
            partial_over(h, i).wait_recv()
        for to, k in sides:
            x_first(h, k).wait_recv()
            rows = pl.ds(128 * k, 128)
            merged = px[h, to, :, rows].astype(F32) + rx1[h, k].astype(F32)
            px[h, to, :, rows] = merged.astype(BF)
            x_second(h, k).start()

    def x_sum(h):
        partial_over(h, 2).wait_recv()
        every(rx2.at[h], rx2_send, rx2_recv.at[h]).wait_recv()
        for t in range(2):
            total = px[h, x, t].astype(F32)
            for k in range(2):
                total += rx2[h, k, t].astype(F32)
            s1[pl.ds(4 * h, 4), :, t] = total.astype(BF).reshape(4, NY, MINE, 256)
        for d in (2, 1, 3):
            y_copy(h, d).start()

    def y_copy(h, d):
        to = lax.rem(y + d, NY)
        return pltpu.make_async_remote_copy(
            src_ref=s1.at[pl.ds(4 * h, 4), to],
            dst_ref=ry.at[h, d - 1],
            send_sem=ry_send,
            recv_sem=ry_recv.at[h],
            device_id={Y: to},
            device_id_type=MESH,
        )

    def y_sum(h):
        total = s1[pl.ds(4 * h, 4), y].astype(F32)
        every(ry.at[h], ry_send, ry_recv.at[h]).wait_recv()
        for d in range(1, NY):
            total += ry[h, d - 1].astype(F32)
        s2[pl.ds(4 * h, 4)] = total.astype(BF)

    def z_copy(d):
        to = lax.rem(z + d, NZ)
        return pltpu.make_async_remote_copy(
            src_ref=s2.at[to],
            dst_ref=rz.at[d - 1],
            send_sem=rz_send,
            recv_sem=rz_recv,
            device_id={Z: to},
            device_id_type=MESH,
        )

    def sum_copy(d):
        return pltpu.make_async_remote_copy(
            src_ref=sp.at[0],
            dst_ref=sp.at[d],
            send_sem=sp_send,
            recv_sem=sp_recv,
            device_id={X: lax.rem(x + d, NX)},
            device_id_type=MESH,
        )

    def all_sums():
        return every(sp.at[pl.ds(1, NX - 1)], sp_send, sp_recv)

    def moments_over():
        return pltpu.make_async_remote_copy(
            src_ref=nm.at[:, 0],
            dst_ref=nm_out,
            send_sem=nm_sem.at[0],
            recv_sem=nm_sem.at[1],
            device_id={C: 0},
            device_id_type=MESH,
        )

    def squares(t, at):
        part = jnp.square(gd[t, at].astype(F32)).reshape(2 * MINE // 8, 8, HALF)
        part = jnp.sum(part, axis=0)
        return part[:, :128] + part[:, 128:256] + part[:, 256:384] + part[:, 384:]

    def weights_out():
        return pltpu.make_async_copy(gw.at[pl.ds(4 * c, 4)], gw_out, out_sem.at[1])

    def dir_out(t, at):
        return pltpu.make_async_copy(gd.at[t, at, 1], gd_out.at[t, at], out_sem.at[5])

    def own_dirs(t):
        return dg[t].give(gd.at[t, f, 0])

    outs = []

    def put(number, src, dst):
        cp = pltpu.make_async_copy(src, dst, out_sem.at[number])
        cp.start()
        outs.append(cp)

    @leads
    def _():
        cue = sum(when < f_order[-1][0] - 2.5 for when, _, _ in f_order)
        for n, (_, g, key) in enumerate(f_order):
            if n == cue:
                pl.semaphore_signal(near_end, inc=1, device_id={C: 0}, device_id_type=MESH)
            g.arrive(key)

    @follows
    def _():
        own_weights().wait_recv()
        pl.semaphore_wait(near_end, 1)
        for g in wg:
            g.start()
        fg[0].given()

    act_load.wait()
    cot_half = cot.at[pl.ds(0, 2)]
    pltpu.make_async_copy(cot_half, cot_half, load.at[4]).wait()
    both_cots().wait_recv()
    project(0)

    @follows
    def _():
        fg[1].given()
        for _, g, key in w_order[:EARLY]:
            g.arrive(key)

    project(1)
    put(0, gf, gf_out)

    @leads
    def _():
        x_merge(0)
        x_merge(1)
        x_sum(0)
        x_sum(1)
        y_sum(0)
        y_sum(1)
        for d in (4, 3, 5, 2, 6, 1, 7):
            z_copy(d).start()
        total = s2[z].astype(F32)
        every(rz, rz_send, rz_recv).wait_recv()
        for d in range(1, NZ):
            total += rz[d - 1].astype(F32)
        sp[0] = total
        for d in (2, 1, 3):
            sum_copy(d).start()
        every(moments.at[:, 0], mom_send, mom_recv).wait_recv()
        pltpu.make_async_copy(moments.at[:, 1], moments.at[:, 1], load.at[5]).wait()
        all_sums().wait_recv()

        for t in range(2):
            for p in range(2):
                proj = jnp.concatenate(
                    [sp[lax.rem(x + (NX - q), NX), t] for q in (2 * p, 2 * p + 1)], axis=1
                )
                proj = proj * (1.0 / math.sqrt(TOKENS))
                first = 0.8 * moments[2 * t, p] + 0.2 * proj
                second = 0.9 * moments[2 * t + 1, p] + 0.1 * proj * proj
                nm[2 * t, p] = first
                nm[2 * t + 1, p] = second
                gd[t, f, p] = (first / jnp.sqrt(second)).astype(BF)
            dg[t].start()
            own_dirs(t).start()
            dir_out(t, f).start()
            sq_parts[t, f] = squares(t, f)
        moments_over().start()
        pltpu.make_async_copy(nm.at[:, 1], nm_out, out_sem.at[4]).start()
        for n, (_, g, key) in enumerate(d_order):
            if n == 3 * len(d_order) // 4:
                all_shares().wait_recv()
                weights_out().start()
            at = g.arrive(key)
            dir_out(g.number, at).start()
            sq_parts[g.number, at] = squares(g.number, at)


    @follows
    def _():
        for _, g, key in w_order[EARLY:]:
            g.arrive(key)

    @follows
    def _():
        weights_out().start()


    @leads
    def _():
        total = jnp.sum(sq_parts[...].reshape(2 * NF, 8, 128), axis=0)
        sq[...] = jnp.broadcast_to(jnp.sum(total, axis=(0, 1), keepdims=True), (8, 128))

    squares_over = pltpu.make_async_remote_copy(
        src_ref=sq,
        dst_ref=sq,
        send_sem=sq_sem.at[0],
        recv_sem=sq_sem.at[1],
        device_id={C: 0},
        device_id_type=MESH,
    )

    @leads
    def _():
        squares_over.start()

    @follows
    def _():
        for t in range(2):
            dg[t].given()
            pltpu.make_async_copy(gd.at[t, :, 0], gd_out.at[t], out_sem.at[5]).start()

    @follows
    def _():
        squares_over.wait_recv()

    put(2, sq, sq_out)

    @leads
    def _():
        for g in fg + dg:
            g.finish()
        own_weights().wait_send()
        every(rx1, rx1_send, rx1_recv.at[0, 0]).wait_send()
        every(rx2, rx2_send, rx2_recv.at[0]).wait_send()
        every(ry, ry_send, ry_recv.at[0]).wait_send()
        every(rz, rz_send, rz_recv).wait_send()
        all_sums().wait_send()
        moments_over().wait_send()
        pltpu.make_async_copy(nm.at[:, 1], nm_out, out_sem.at[4]).wait()
        squares_over.wait_send()

    @follows
    def _():
        for g in wg:
            g.finish()
        all_shares().wait_send()
        every(moments.at[:, 0], mom_send, mom_recv).wait_send()
        moments_over().wait_recv()
        every(px.at[:, :, 0], px_send, px_recv.at[0, 0]).wait_send()

    both_cots().wait_send()
    weights_out().wait()
    for cp in outs:
        cp.wait()
    pltpu.make_async_copy(gd.at[:, :, c], gd_out, out_sem.at[5]).wait()


def update_kernel(
    gf_in, gw_in, gd_in, nm_in, sq_in, query_factor, out_factor, query_w, out_w,
    new_qw, new_ow, q_step, o_step, nf_q, ns_q, nf_o, ns_o, q_copy, o_copy,
    gf, gw, gd, nm, sq, factor, w, steps, new_w, new_q, new_o,
    first_sem, block_sem, small_sem, copy_sem, out_sem,
):
    copy = pltpu.make_async_copy
    per = NF // BLOCKS
    size = D // BLOCKS
    first = [copy(gd_in, gd, first_sem.at[0]), copy(sq_in, sq, first_sem.at[1])]
    small = [copy(nm_in, nm, small_sem.at[0])]
    for t, (fac, old) in enumerate(((query_factor, query_w), (out_factor, out_w))):
        small.append(copy(fac, factor.at[t], small_sem.at[1 + 2 * t]))
        small.append(copy(old, w.at[t], small_sem.at[2 + 2 * t]))

    def block_loads(b):
        some = pl.ds(per * b, per)
        return (
            copy(gf_in.at[:, some], gf.at[:, some], block_sem.at[0, b]),
            copy(gw_in.at[:, some], gw.at[:, some], block_sem.at[1, b]),
        )

    def block_stores(b):
        at = pl.ds(pl.multiple_of(size * b, size), size)
        return (
            copy(new_q.at[b], q_copy.at[at], copy_sem.at[0]),
            copy(new_o.at[b], o_copy.at[:, at], copy_sem.at[1]),
        )

    for cp in first + small:
        cp.start()
    for cp in block_loads(0):
        cp.start()
    for cp in first:
        cp.wait()
    for cp in block_loads(1) + block_loads(2):
        cp.start()
    inverse = 1.0 / jnp.sqrt(sq[0:1] / (2 * RANK * HQ) + 1e-06)
    inverse = jnp.concatenate([inverse] * 4, axis=1)
    def block(b, _):
        some = pl.ds(per * b, per)
        @pl.when(b + 3 < BLOCKS)
        def _():
            for cp in block_loads(b + 3):
                cp.start()

        for cp in block_loads(b):
            cp.wait()
        moved = []
        for t in range(2):
            rows = jnp.concatenate(
                [gf[2 * j + t, some].reshape(size, 128) for j in range(4)], axis=1
            )
            step = jnp.dot(rows, gd[t].reshape(RANK, HALF), preferred_element_type=F32)
            old = jnp.concatenate([gw[i, some].reshape(size, 256) for i in (t, 2 + t)], axis=1)
            moved.append(old.astype(F32) - (0.01 * inverse) * step)
        new_q[b] = moved[0].astype(BF)
        new_o[b] = moved[1].astype(BF).T
        for cp in block_stores(b):
            cp.start()
        return 0

    lax.fori_loop(0, BLOCKS, block, 0)
    for cp in small:
        cp.wait()
    stores = [copy(nm.at[k], o, out_sem.at[k]) for k, o in enumerate((nf_q, ns_q, nf_o, ns_o))]
    for t, (to_step, to_w) in enumerate(((q_step, new_qw), (o_step, new_ow))):
        step = jnp.dot(factor[t], gd[t].reshape(RANK, HALF), preferred_element_type=F32)
        step = step * inverse
        steps[t] = step
        new_w[t] = w[t] - 0.01 * step
        stores.append(copy(steps.at[t], to_step, out_sem.at[4 + 2 * t]))
        stores.append(copy(new_w.at[t], to_w, out_sem.at[5 + 2 * t]))
    for cp in stores:
        cp.start()
    for cp in stores:
        cp.wait()
    copy(new_q, new_q, copy_sem.at[0]).wait()
    copy(new_o, new_o, copy_sem.at[1]).wait()


def body(
    input_act, query_cot, out_cot, attn_out, query_w, out_w, query_factor, out_factor,
    first_q, second_q, first_o, second_o,
):
    struct = jax.ShapeDtypeStruct
    dma = pltpu.SemaphoreType.DMA
    vmem = pltpu.VMEM
    out_w = out_w.T
    scratch = [
        vmem((8, NF, ROWS, 128), BF),
        vmem((8, NF, ROWS, 256), BF),
        vmem((2, NF, 2, MINE, HALF), BF),
        vmem((TOK, D), BF),
        vmem((4, TOK, 256), BF),
        vmem((ROWS, HALF), F32),
        vmem((ROWS, HALF), F32),
        vmem((4, 2, MINE, HALF), F32),
        vmem((TOK, 256), BF),
        vmem((2, NX, 2, 256, 256), BF),
        vmem((2, 2, 2, 128, 256), BF),
        vmem((2, 2, 2, 256, 256), BF),
        vmem((NZ, NY, 2, MINE, 256), BF),
        vmem((2, NY - 1, 4, 2, MINE, 256), BF),
        vmem((NZ, 2, MINE, 256), BF),
        vmem((NZ - 1, 2, MINE, 256), BF),
        vmem((NX, 2, MINE, 256), F32),
        vmem((8, 128), F32),
        vmem((2, NF, 8, 128), F32),
        vmem((4, 2, MINE, HALF), F32),
        dma((6,)),
        dma((2,)), dma((2, PIECES)), dma((2,)), dma((2,)),
        dma((2,)), dma, dma, pltpu.SemaphoreType.REGULAR,
        dma((2,)), dma((2,)), dma((2,)),
        dma, dma, dma, dma, dma, dma,
        dma, dma((2, NX)),
        dma, dma((2, 2)), dma, dma((2,)),
        dma, dma((2,)), dma, dma, dma, dma,
        dma((2,)), dma((2,)), dma((6,)),
    ]
    gf, gw, gd, nm, sq = pl.pallas_call(
        reduce_kernel,
        out_shape=(
            struct((8, NF, ROWS, 128), BF),
            struct((4, NF, ROWS, 256), BF),
            struct((2, NF, MINE, HALF), BF),
            struct((4, MINE, HALF), F32),
            struct((8, 128), F32),
        ),
        in_specs=[pl.BlockSpec(memory_space=pl.ANY)] * 12,
        out_specs=[pl.BlockSpec(memory_space=pl.ANY)] * 5,
        scratch_shapes=scratch,
        compiler_params=pltpu.CompilerParams(
            collective_id=0, has_side_effects=True, vmem_limit_bytes=56 * 1024 * 1024
        ),
        name="reduce",
    )(
        input_act, query_cot, out_cot, attn_out, query_w, out_w, query_factor, out_factor,
        first_q, second_q, first_o, second_o,
    )

    anywhere = pl.BlockSpec(memory_space=pl.ANY)
    shard, small = struct((ROWS, HALF), F32), struct((MINE, HALF), F32)
    outs = pl.pallas_call(
        update_kernel,
        out_shape=(
            *[shard] * 4,
            *[small] * 4,
            struct((D, HALF), BF),
            struct((HALF, D), BF),
        ),
        in_specs=[anywhere] * 9,
        out_specs=[anywhere] * 10,
        scratch_shapes=[
            vmem((8, NF, ROWS, 128), BF),
            vmem((4, NF, ROWS, 256), BF),
            vmem((2, NF, MINE, HALF), BF),
            vmem((4, MINE, HALF), F32),
            vmem((8, 128), F32),
            vmem((2, ROWS, RANK), BF),
            vmem((2, ROWS, HALF), F32),
            vmem((2, ROWS, HALF), F32),
            vmem((2, ROWS, HALF), F32),
            vmem((BLOCKS, D // BLOCKS, HALF), BF),
            vmem((BLOCKS, HALF, D // BLOCKS), BF),
            dma((2,)),
            dma((2, BLOCKS)),
            dma((5,)),
            dma((2,)),
            dma((8,)),
        ],
        compiler_params=pltpu.CompilerParams(vmem_limit_bytes=56 * 1024 * 1024),
        name="update",
    )(gf, gw, gd, nm, sq, query_factor, out_factor, query_w, out_w)
    outs = list(outs)
    outs[1], outs[3] = outs[1].T, outs[3].T
    return tuple(outs)


def solution(mesh):
    finer = Mesh(mesh.devices.reshape(NZ, NY, NX, 2), (Z, Y, X, C))
    in_specs = (
        P(FS_REP, None),
        P(FS_REP, C),
        P(FS_REP, None),
        P(FS_REP, C),
        P(FS, C),
        P(C, FS),
        P(FS, None),
        P(FS, None),
        *[P(FS, C)] * 4,
    )
    out_specs = (
        P(FS, C),
        P(C, FS),
        P(FS, C),
        P(C, FS),
        *[P(FS, C)] * 4,
        P(None, C),
        P(C, None),
    )
    return jax.shard_map(body, mesh=finer, in_specs=in_specs, out_specs=out_specs, check_vma=False)
```

```python
import math

import jax
import jax.numpy as jnp
from jax import lax
from jax.experimental import pallas as pl
from jax.experimental.pallas import tpu as pltpu
from jax.sharding import Mesh
from jax.sharding import PartitionSpec as P

NZ, NY, NX = 8, 4, 4
NF = NZ * NY
D, RANK, HQ, TOKENS = 2048, 512, 1024, 98304
HALF = HQ // 2
TOK = TOKENS // (NF * NX)
ROWS = D // NF
MINE = RANK // NF
BLOCKS = 4
Z, Y, X, C = "fs_0", "fs_1", "rep", "tp"
FS = (Z, Y)
FS_REP = (Z, Y, X)
BF, F32 = jnp.bfloat16, jnp.float32
MESH = pl.DeviceIdType.MESH


def along(n, mode, flip):
    up, down = (n // 2, n - 1 - n // 2)[:: -1 if flip else 1]
    tree = {}
    for s, far in ((1, up), (-1, down)):
        if mode == "ring":
            hops = [(k, 1) for k in range(far)]
        elif mode == "direct":
            hops = [(0, k) for k in range(far, 0, -1)]
        else:
            hops = [(0, 2), (0, 1), (2, 2), (2, 1)]
        for at, by in hops:
            if at + by <= far:
                tree.setdefault(s * at, []).append((s, by, s * (at + by)))
    return tree, range(-down, up + 1)


def broadcast(axes, flip):
    (axis_1, mode_1), (axis_2, mode_2) = axes
    sizes = {Z: NZ, Y: NY}
    tree_1, span = along(sizes[axis_1], mode_1, flip)
    events = {}
    for i in span:
        tree_2, across = along(sizes[axis_2], mode_2, (i + flip) % 2)
        for j in across:
            on = [(axis_2, s, d, (i, to)) for s, d, to in tree_2.get(j, [])]
            if j == 0:
                on = [(axis_1, s, d, (to, 0)) for s, d, to in tree_1.get(i, [])] + on
            events[i, j] = on
    return events


def expected_order(gathers):
    free, now, order = {}, 0.0, []
    heap = [(0.01 * g.number, g.number, (0, 0)) for g in gathers]
    by_number = {g.number: g for g in gathers}
    while heap:
        heap.sort()
        when, number, key = heap.pop(0)
        now, g = max(now, when), by_number[number]
        if key != (0, 0):
            order.append((when, g, key))
        for axis, sign, distance, landed in g.events[key]:
            now += 0.02
            begin = max(free.get((axis, sign), 0.0), now)
            wire = g.kib / 91.0
            free[axis, sign] = begin + wire * distance
            heap.append((begin + wire + 2.0 + 0.75 * (distance - 1), number, landed))
    return order


class Gather:
    def __init__(self, number, axes, flip, kib, pieces, many, share, shares, where, sems, core):
        self.number, self.axes, self.kib = number, [a for a, _ in axes], kib
        self.events = broadcast(axes, flip)
        self.slots = {key: n for n, key in enumerate(k for k in self.events if k != (0, 0))}
        self.pieces, self.many, self.share, self.shares = pieces, many, share, shares
        self.where, self.core = where, core
        self.send_sem, self.recv_sem, self.pass_sem, self.give_sem = sems

    def index(self, key):
        off = dict(zip(self.axes, key))
        z = lax.rem(self.where[Z] + (NZ - off[Z]), NZ)
        y = lax.rem(self.where[Y] + (NY - off[Y]), NY)
        return z * NY + y

    def copy(self, ref, axis, by, slot):
        n = NZ if axis == Z else NY
        return pltpu.make_async_remote_copy(
            src_ref=ref,
            dst_ref=ref,
            send_sem=self.send_sem,
            recv_sem=self.recv_sem.at[slot],
            device_id={axis: lax.rem(self.where[axis] + (n + by), n)},
            device_id_type=MESH,
        )

    def give(self, ref):
        return pltpu.make_async_remote_copy(
            src_ref=ref,
            dst_ref=ref,
            send_sem=self.pass_sem,
            recv_sem=self.give_sem,
            device_id={C: self.core},
            device_id_type=MESH,
        )

    def pass_on(self, key):
        f = self.index(key)
        for axis, sign, distance, landed in self.events[key]:
            for ref in self.pieces(f):
                self.copy(ref, axis, sign * distance, self.slots[landed]).start()

    def start(self):
        self.pass_on((0, 0))

    def arrive(self, key):
        f = self.index(key)
        self.copy(self.many(1), Z, 1, self.slots[key]).wait_recv()
        self.pass_on(key)
        if self.share is not None:
            self.give(self.share(f)).start()
        return f

    def finish(self):
        self.copy(self.many(PIECES), Z, 1, 0).wait_send()
        if self.shares is not None:
            self.give(self.shares()).wait_send()

    def given(self):
        self.give(self.shares()).wait_recv()


PIECES = NF - 1
EARLY = 6
ZY_RING, YZ_RING = ((Z, "ring"), (Y, "ring")), ((Y, "ring"), (Z, "ring"))
ZY_FAST, YZ_FAST = ((Z, "skip"), (Y, "ring")), ((Y, "direct"), (Z, "skip"))


def reduce_kernel(*refs):
    (
        input_act, query_cot, out_cot, attn_out, query_w, out_w, query_factor, out_factor,
        first_q, second_q, first_o, second_o,
        gf_out, gw_out, gd_out, nm_out, sq_out,
        gf, gw, gd, act, cot, qw, ow, moments, low, px, rx1, rx2, s1, ry, s2,
        rz, sp, sq, sq_parts, nm,
        load, f_send, f_recv, f_pass, f_give, w_send, w_pass, w_give, near_end,
        d_send, d_pass, d_give, own_send, own_recv, mom_send, mom_recv,
        cot_send, cot_recv, px_send, px_recv,
        rx1_send, rx1_recv, rx2_send, rx2_recv, ry_send, ry_recv, rz_send, rz_recv,
        sp_send, sp_recv, nm_sem, sq_sem, out_sem,
    ) = refs
    z, y, x, c = (lax.axis_index(a) for a in (Z, Y, X, C))
    f = z * NY + y
    where = {Z: z, Y: y}
    other = 1 - c
    leads, follows = pl.when(c == 1), pl.when(c == 0)

    def load_own(number, if_q, if_o, dst):
        @follows
        def _():
            pltpu.make_async_copy(if_q, dst, load.at[number]).start()

        @leads
        def _():
            pltpu.make_async_copy(if_o, dst, load.at[number]).start()

        return pltpu.make_async_copy(if_q, dst, load.at[number])

    def load_plain(number, src, dst):
        cp = pltpu.make_async_copy(src, dst, load.at[number])
        cp.start()
        return cp

    for j in range(4):
        cols = pl.ds(128 * j, 128)
        for t, factor in enumerate((query_factor, out_factor)):
            load_plain(0, factor.at[:, cols], gf.at[2 * j + t, f])
    w_loads = [load_plain(1, query_w, qw), load_plain(2, out_w, ow)]
    act_load = load_own(3, input_act, out_cot, act)
    for k in range(2):
        cols = pl.ds(256 * k, 256)
        _ = load_own(4, query_cot.at[:, cols], attn_out.at[:, cols], cot.at[2 * c + k])

    barrier = pltpu.get_barrier_semaphore()
    peers = [{C: other}]
    for axis, at, n in ((Z, z, NZ), (Y, y, NY), (X, x, NX)):
        peers += [{axis: lax.rem(at + 1, n)}, {axis: lax.rem(at + n - 1, n)}]
    peers += [{Z: lax.rem(z + 2, NZ)}, {Z: lax.rem(z + NZ - 2, NZ)}, {Y: lax.rem(y + 2, NY)}]
    for peer in peers:
        pl.semaphore_signal(barrier, inc=1, device_id=peer, device_id_type=MESH)

    for w in w_loads:
        w.wait()
    for k in range(2):
        gw[4 * c + 2 * k, f] = qw[:, 256 * k : 256 * k + 256].astype(BF)
        gw[4 * c + 2 * k + 1, f] = ow[:, 256 * k : 256 * k + 256].astype(BF)
    factors = gf.at[:, f]
    pltpu.make_async_copy(factors, factors, load.at[0]).wait()
    pl.semaphore_wait(barrier, len(peers))

    parts = (pl.ds(0, 5), pl.ds(5, 3))

    def factor_gather(k):
        return Gather(
            k, (ZY_FAST, YZ_RING)[k], 1 - k, (80, 48)[k],
            lambda p: (gf.at[parts[k], p],), lambda n: gf.at[parts[k], pl.ds(0, n)],
            lambda p: gf.at[parts[k], p], lambda: gf.at[parts[k], pl.ds(0, PIECES)],
            where, [a.at[k] for a in (f_send, f_recv, f_pass, f_give)], 0,
        )

    def weight_gather(k):
        give = (pl.ds(4, 1), parts[1])[k]
        return Gather(
            k, (ZY_RING, YZ_RING)[k], k, (160, 96)[k],
            lambda p: (gw.at[parts[k], p],), lambda n: gw.at[parts[k], pl.ds(0, n)],
            lambda p: gw.at[give, p], None,
            where, (w_send.at[k], f_recv.at[k], w_pass, w_give), 1,
        )

    def all_shares():
        return every(gw.at[pl.ds(4, 4), pl.ds(0, PIECES)], w_pass, w_give)

    def dir_gather(k):
        return Gather(
            k, ZY_FAST if k == 0 else YZ_FAST, k, 32,
            lambda p: (gd.at[k, p],), lambda n: gd.at[k, pl.ds(0, n)],
            lambda p: gd.at[k, p, 0], lambda: gd.at[k, :, 0],
            where, (d_send.at[k], f_recv.at[k], d_pass.at[k], d_give.at[k]), 0,
        )

    fg = [factor_gather(k) for k in range(2)]
    wg = [weight_gather(k) for k in range(2)]
    dg = [dir_gather(k) for k in range(2)]
    f_order, w_order, d_order = (expected_order(g) for g in (fg, wg, dg))

    @leads
    def _():
        for g in fg:
            g.start()

    def cot_copy(src, k):
        return pltpu.make_async_remote_copy(
            src_ref=src.at[:, pl.ds(256 * k, 256)],
            dst_ref=cot.at[2 * c + k],
            send_sem=cot_send,
            recv_sem=cot_recv,
            device_id={C: other},
            device_id_type=MESH,
        )

    def every(ref, send_sem, recv_sem):
        return pltpu.make_async_remote_copy(
            src_ref=ref,
            dst_ref=ref,
            send_sem=send_sem,
            recv_sem=recv_sem,
            device_id={C: other},
            device_id_type=MESH,
        )

    def both_cots():
        return every(cot.at[pl.ds(0, 2)], cot_send, cot_recv)

    def own_weights():
        return every(gw.at[pl.ds(4, 4), f], own_send, own_recv)

    def own_moments(k, m):
        return pltpu.make_async_remote_copy(
            src_ref=m,
            dst_ref=moments.at[k, 0],
            send_sem=mom_send,
            recv_sem=mom_recv,
            device_id={C: 1},
            device_id_type=MESH,
        )

    all_moments = (first_q, second_q, first_o, second_o)

    @follows
    def _():
        for k in range(2):
            cot_copy(attn_out, k).start()
        for k, m in enumerate(all_moments):
            own_moments(k, m).start()

    @leads
    def _():
        for k in range(2):
            cot_copy(query_cot, k).start()
        own_weights().start()
        for k, m in enumerate(all_moments):
            pltpu.make_async_copy(m, moments.at[k, 1], load.at[5]).start()

    def project(h):
        def tile(m, _):
            rows = pl.ds(pl.multiple_of(m * 256, 256), 256)
            right = jnp.concatenate(
                [gf[2 * (2 * h + j) + c].reshape(D, 128) for j in range(2)], axis=1
            )
            low[rows, :] = jnp.dot(act[rows, :], right, preferred_element_type=F32).astype(BF)
            return 0

        lax.fori_loop(0, TOK // 256, tile, 0)
        if h:
            @leads
            def _():
                x_start(0)

        for i in range(NX):
            xb = lax.rem(x + 2 + i, NX)
            dims = (((0,), (0,)), ((), ()))
            total = lax.dot_general(low[...], cot[xb], dims, preferred_element_type=F32)
            px[h, xb, c] = total.astype(BF)

            @follows
            def _():
                partial_over(h, i).start()

        if h:

            @leads
            def _():
                x_start(1)

    x_up, x_down, x_far = lax.rem(x + 1, NX), lax.rem(x + 3, NX), lax.rem(x + 2, NX)
    sides = ((x_up, 0), (x_down, 1))

    def partial_over(h, i):
        ref = px.at[h, lax.rem(x + 2 + i, NX), 0]
        return pltpu.make_async_remote_copy(
            src_ref=ref,
            dst_ref=ref,
            send_sem=px_send,
            recv_sem=px_recv.at[h, i],
            device_id={C: 1},
            device_id_type=MESH,
        )

    def x_first(h, k):
        return pltpu.make_async_remote_copy(
            src_ref=px.at[h, x_far, :, pl.ds(128 * k, 128)],
            dst_ref=rx1.at[h, k],
            send_sem=rx1_send,
            recv_sem=rx1_recv.at[h, k],
            device_id={X: sides[k][0]},
            device_id_type=MESH,
        )

    def x_second(h, k):
        return pltpu.make_async_remote_copy(
            src_ref=px.at[h, sides[k][0]],
            dst_ref=rx2.at[h, k],
            send_sem=rx2_send,
            recv_sem=rx2_recv.at[h],
            device_id={X: sides[k][0]},
            device_id_type=MESH,
        )

    def x_start(h):
        partial_over(h, 0).wait_recv()
        for k in range(2):
            x_first(h, k).start()

    def x_merge(h):
        for i in (1, 3):
            partial_over(h, i).wait_recv()
        for to, k in sides:
            x_first(h, k).wait_recv()
            rows = pl.ds(128 * k, 128)
            merged = px[h, to, :, rows].astype(F32) + rx1[h, k].astype(F32)
            px[h, to, :, rows] = merged.astype(BF)
            x_second(h, k).start()

    def x_sum(h):
        partial_over(h, 2).wait_recv()
        every(rx2.at[h], rx2_send, rx2_recv.at[h]).wait_recv()
        for t in range(2):
            total = px[h, x, t].astype(F32)
            for k in range(2):
                total += rx2[h, k, t].astype(F32)
            s1[pl.ds(4 * h, 4), :, t] = total.astype(BF).reshape(4, NY, MINE, 256)
        for d in (2, 1, 3):
            y_copy(h, d).start()

    def y_copy(h, d):
        to = lax.rem(y + d, NY)
        return pltpu.make_async_remote_copy(
            src_ref=s1.at[pl.ds(4 * h, 4), to],
            dst_ref=ry.at[h, d - 1],
            send_sem=ry_send,
            recv_sem=ry_recv.at[h],
            device_id={Y: to},
            device_id_type=MESH,
        )

    def y_sum(h):
        total = s1[pl.ds(4 * h, 4), y].astype(F32)
        every(ry.at[h], ry_send, ry_recv.at[h]).wait_recv()
        for d in range(1, NY):
            total += ry[h, d - 1].astype(F32)
        s2[pl.ds(4 * h, 4)] = total.astype(BF)

    def z_copy(d):
        to = lax.rem(z + d, NZ)
        return pltpu.make_async_remote_copy(
            src_ref=s2.at[to],
            dst_ref=rz.at[d - 1],
            send_sem=rz_send,
            recv_sem=rz_recv,
            device_id={Z: to},
            device_id_type=MESH,
        )

    def sum_copy(d):
        return pltpu.make_async_remote_copy(
            src_ref=sp.at[0],
            dst_ref=sp.at[d],
            send_sem=sp_send,
            recv_sem=sp_recv,
            device_id={X: lax.rem(x + d, NX)},
            device_id_type=MESH,
        )

    def all_sums():
        return every(sp.at[pl.ds(1, NX - 1)], sp_send, sp_recv)

    def moments_over():
        return pltpu.make_async_remote_copy(
            src_ref=nm.at[:, 0],
            dst_ref=nm_out,
            send_sem=nm_sem.at[0],
            recv_sem=nm_sem.at[1],
            device_id={C: 0},
            device_id_type=MESH,
        )

    def squares(t, at):
        part = jnp.square(gd[t, at].astype(F32)).reshape(2 * MINE // 8, 8, HALF)
        part = jnp.sum(part, axis=0)
        return part[:, :128] + part[:, 128:256] + part[:, 256:384] + part[:, 384:]

    def weights_out():
        return pltpu.make_async_copy(gw.at[pl.ds(4 * c, 4)], gw_out, out_sem.at[1])

    def dir_out(t, at):
        return pltpu.make_async_copy(gd.at[t, at, 1], gd_out.at[t, at], out_sem.at[5])

    def own_dirs(t):
        return dg[t].give(gd.at[t, f, 0])

    outs = []

    def put(number, src, dst):
        cp = pltpu.make_async_copy(src, dst, out_sem.at[number])
        cp.start()
        outs.append(cp)

    @leads
    def _():
        cue = sum(when < f_order[-1][0] - 2.5 for when, _, _ in f_order)
        for n, (_, g, key) in enumerate(f_order):
            if n == cue:
                pl.semaphore_signal(near_end, inc=1, device_id={C: 0}, device_id_type=MESH)
            g.arrive(key)

    @follows
    def _():
        own_weights().wait_recv()
        pl.semaphore_wait(near_end, 1)
        for g in wg:
            g.start()
        fg[0].given()

    act_load.wait()
    cot_half = cot.at[pl.ds(0, 2)]
    pltpu.make_async_copy(cot_half, cot_half, load.at[4]).wait()
    both_cots().wait_recv()
    project(0)

    @follows
    def _():
        fg[1].given()
        for _, g, key in w_order[:EARLY]:
            g.arrive(key)

    project(1)
    put(0, gf, gf_out)

    @leads
    def _():
        x_merge(0)
        x_merge(1)
        x_sum(0)
        x_sum(1)
        for h in range(2):
            y_sum(h)
            for d in (4, 3, 5, 2, 6, 1, 7):

                @pl.when(lax.rem(z + d, NZ) // 4 == h)
                def _():
                    z_copy(d).start()

        total = s2[z].astype(F32)
        every(rz, rz_send, rz_recv).wait_recv()
        for d in range(1, NZ):
            total += rz[d - 1].astype(F32)
        sp[0] = total
        for d in (2, 1, 3):
            sum_copy(d).start()
        every(moments.at[:, 0], mom_send, mom_recv).wait_recv()
        pltpu.make_async_copy(moments.at[:, 1], moments.at[:, 1], load.at[5]).wait()
        all_sums().wait_recv()

        for t in range(2):
            for p in range(2):
                proj = jnp.concatenate(
                    [sp[lax.rem(x + (NX - q), NX), t] for q in (2 * p, 2 * p + 1)], axis=1
                )
                proj = proj * (1.0 / math.sqrt(TOKENS))
                first = 0.8 * moments[2 * t, p] + 0.2 * proj
                second = 0.9 * moments[2 * t + 1, p] + 0.1 * proj * proj
                nm[2 * t, p] = first
                nm[2 * t + 1, p] = second
                gd[t, f, p] = (first / jnp.sqrt(second)).astype(BF)
            dg[t].start()
            own_dirs(t).start()
            dir_out(t, f).start()
            sq_parts[t, f] = squares(t, f)
        moments_over().start()
        pltpu.make_async_copy(nm.at[:, 1], nm_out, out_sem.at[4]).start()
        for n, (_, g, key) in enumerate(d_order):
            if n == 3 * len(d_order) // 4:
                all_shares().wait_recv()
                weights_out().start()
            at = g.arrive(key)
            dir_out(g.number, at).start()
            sq_parts[g.number, at] = squares(g.number, at)


    @follows
    def _():
        for _, g, key in w_order[EARLY:]:
            g.arrive(key)

    @follows
    def _():
        weights_out().start()


    @leads
    def _():
        total = jnp.sum(sq_parts[...].reshape(2 * NF, 8, 128), axis=0)
        sq[...] = jnp.broadcast_to(jnp.sum(total, axis=(0, 1), keepdims=True), (8, 128))

    squares_over = pltpu.make_async_remote_copy(
        src_ref=sq,
        dst_ref=sq,
        send_sem=sq_sem.at[0],
        recv_sem=sq_sem.at[1],
        device_id={C: 0},
        device_id_type=MESH,
    )

    @leads
    def _():
        squares_over.start()

    @follows
    def _():
        for t in range(2):
            dg[t].given()
            pltpu.make_async_copy(gd.at[t, :, 0], gd_out.at[t], out_sem.at[5]).start()

    @follows
    def _():
        squares_over.wait_recv()

    put(2, sq, sq_out)

    @leads
    def _():
        for g in fg + dg:
            g.finish()
        own_weights().wait_send()
        every(rx1, rx1_send, rx1_recv.at[0, 0]).wait_send()
        every(rx2, rx2_send, rx2_recv.at[0]).wait_send()
        every(ry, ry_send, ry_recv.at[0]).wait_send()
        every(rz, rz_send, rz_recv).wait_send()
        all_sums().wait_send()
        moments_over().wait_send()
        pltpu.make_async_copy(nm.at[:, 1], nm_out, out_sem.at[4]).wait()
        squares_over.wait_send()

    @follows
    def _():
        for g in wg:
            g.finish()
        all_shares().wait_send()
        every(moments.at[:, 0], mom_send, mom_recv).wait_send()
        moments_over().wait_recv()
        every(px.at[:, :, 0], px_send, px_recv.at[0, 0]).wait_send()

    both_cots().wait_send()
    weights_out().wait()
    for cp in outs:
        cp.wait()
    pltpu.make_async_copy(gd.at[:, :, c], gd_out, out_sem.at[5]).wait()


def update_kernel(
    gf_in, gw_in, gd_in, nm_in, sq_in, query_factor, out_factor, query_w, out_w,
    new_qw, new_ow, q_step, o_step, nf_q, ns_q, nf_o, ns_o, q_copy, o_copy,
    gf, gw, gd, nm, sq, factor, w, steps, new_w, new_q, new_o,
    first_sem, block_sem, small_sem, copy_sem, out_sem,
):
    copy = pltpu.make_async_copy
    per = NF // BLOCKS
    size = D // BLOCKS
    first = [copy(gd_in, gd, first_sem.at[0]), copy(sq_in, sq, first_sem.at[1])]
    small = [copy(nm_in, nm, small_sem.at[0])]
    for t, (fac, old) in enumerate(((query_factor, query_w), (out_factor, out_w))):
        small.append(copy(fac, factor.at[t], small_sem.at[1 + 2 * t]))
        small.append(copy(old, w.at[t], small_sem.at[2 + 2 * t]))

    def block_loads(b):
        some = pl.ds(per * b, per)
        return (
            copy(gf_in.at[:, some], gf.at[:, some], block_sem.at[0, b]),
            copy(gw_in.at[:, some], gw.at[:, some], block_sem.at[1, b]),
        )

    def block_stores(b):
        at = pl.ds(pl.multiple_of(size * b, size), size)
        return (
            copy(new_q.at[b], q_copy.at[at], copy_sem.at[0]),
            copy(new_o.at[b], o_copy.at[:, at], copy_sem.at[1]),
        )

    for cp in first + small:
        cp.start()
    for cp in block_loads(0):
        cp.start()
    for cp in first:
        cp.wait()
    for cp in block_loads(1) + block_loads(2):
        cp.start()
    inverse = 1.0 / jnp.sqrt(sq[0:1] / (2 * RANK * HQ) + 1e-06)
    inverse = jnp.concatenate([inverse] * 4, axis=1)
    def block(b, _):
        some = pl.ds(per * b, per)
        @pl.when(b + 3 < BLOCKS)
        def _():
            for cp in block_loads(b + 3):
                cp.start()

        for cp in block_loads(b):
            cp.wait()
        moved = []
        for t in range(2):
            rows = jnp.concatenate(
                [gf[2 * j + t, some].reshape(size, 128) for j in range(4)], axis=1
            )
            step = jnp.dot(rows, gd[t].reshape(RANK, HALF), preferred_element_type=F32)
            old = jnp.concatenate([gw[i, some].reshape(size, 256) for i in (t, 2 + t)], axis=1)
            moved.append(old.astype(F32) - (0.01 * inverse) * step)
        new_q[b] = moved[0].astype(BF)
        new_o[b] = moved[1].astype(BF).T
        for cp in block_stores(b):
            cp.start()
        return 0

    lax.fori_loop(0, BLOCKS, block, 0)
    for cp in small:
        cp.wait()
    stores = [copy(nm.at[k], o, out_sem.at[k]) for k, o in enumerate((nf_q, ns_q, nf_o, ns_o))]
    for t, (to_step, to_w) in enumerate(((q_step, new_qw), (o_step, new_ow))):
        step = jnp.dot(factor[t], gd[t].reshape(RANK, HALF), preferred_element_type=F32)
        step = step * inverse
        steps[t] = step
        new_w[t] = w[t] - 0.01 * step
        stores.append(copy(steps.at[t], to_step, out_sem.at[4 + 2 * t]))
        stores.append(copy(new_w.at[t], to_w, out_sem.at[5 + 2 * t]))
    for cp in stores:
        cp.start()
    for cp in stores:
        cp.wait()
    copy(new_q, new_q, copy_sem.at[0]).wait()
    copy(new_o, new_o, copy_sem.at[1]).wait()


def body(
    input_act, query_cot, out_cot, attn_out, query_w, out_w, query_factor, out_factor,
    first_q, second_q, first_o, second_o,
):
    struct = jax.ShapeDtypeStruct
    dma = pltpu.SemaphoreType.DMA
    vmem = pltpu.VMEM
    out_w = out_w.T
    scratch = [
        vmem((8, NF, ROWS, 128), BF),
        vmem((8, NF, ROWS, 256), BF),
        vmem((2, NF, 2, MINE, HALF), BF),
        vmem((TOK, D), BF),
        vmem((4, TOK, 256), BF),
        vmem((ROWS, HALF), F32),
        vmem((ROWS, HALF), F32),
        vmem((4, 2, MINE, HALF), F32),
        vmem((TOK, 256), BF),
        vmem((2, NX, 2, 256, 256), BF),
        vmem((2, 2, 2, 128, 256), BF),
        vmem((2, 2, 2, 256, 256), BF),
        vmem((NZ, NY, 2, MINE, 256), BF),
        vmem((2, NY - 1, 4, 2, MINE, 256), BF),
        vmem((NZ, 2, MINE, 256), BF),
        vmem((NZ - 1, 2, MINE, 256), BF),
        vmem((NX, 2, MINE, 256), F32),
        vmem((8, 128), F32),
        vmem((2, NF, 8, 128), F32),
        vmem((4, 2, MINE, HALF), F32),
        dma((6,)),
        dma((2,)), dma((2, PIECES)), dma((2,)), dma((2,)),
        dma((2,)), dma, dma, pltpu.SemaphoreType.REGULAR,
        dma((2,)), dma((2,)), dma((2,)),
        dma, dma, dma, dma, dma, dma,
        dma, dma((2, NX)),
        dma, dma((2, 2)), dma, dma((2,)),
        dma, dma((2,)), dma, dma, dma, dma,
        dma((2,)), dma((2,)), dma((6,)),
    ]
    gf, gw, gd, nm, sq = pl.pallas_call(
        reduce_kernel,
        out_shape=(
            struct((8, NF, ROWS, 128), BF),
            struct((4, NF, ROWS, 256), BF),
            struct((2, NF, MINE, HALF), BF),
            struct((4, MINE, HALF), F32),
            struct((8, 128), F32),
        ),
        in_specs=[pl.BlockSpec(memory_space=pl.ANY)] * 12,
        out_specs=[pl.BlockSpec(memory_space=pl.ANY)] * 5,
        scratch_shapes=scratch,
        compiler_params=pltpu.CompilerParams(
            collective_id=0, has_side_effects=True, vmem_limit_bytes=56 * 1024 * 1024
        ),
        name="reduce",
    )(
        input_act, query_cot, out_cot, attn_out, query_w, out_w, query_factor, out_factor,
        first_q, second_q, first_o, second_o,
    )

    anywhere = pl.BlockSpec(memory_space=pl.ANY)
    shard, small = struct((ROWS, HALF), F32), struct((MINE, HALF), F32)
    outs = pl.pallas_call(
        update_kernel,
        out_shape=(
            *[shard] * 4,
            *[small] * 4,
            struct((D, HALF), BF),
            struct((HALF, D), BF),
        ),
        in_specs=[anywhere] * 9,
        out_specs=[anywhere] * 10,
        scratch_shapes=[
            vmem((8, NF, ROWS, 128), BF),
            vmem((4, NF, ROWS, 256), BF),
            vmem((2, NF, MINE, HALF), BF),
            vmem((4, MINE, HALF), F32),
            vmem((8, 128), F32),
            vmem((2, ROWS, RANK), BF),
            vmem((2, ROWS, HALF), F32),
            vmem((2, ROWS, HALF), F32),
            vmem((2, ROWS, HALF), F32),
            vmem((BLOCKS, D // BLOCKS, HALF), BF),
            vmem((BLOCKS, HALF, D // BLOCKS), BF),
            dma((2,)),
            dma((2, BLOCKS)),
            dma((5,)),
            dma((2,)),
            dma((8,)),
        ],
        compiler_params=pltpu.CompilerParams(vmem_limit_bytes=56 * 1024 * 1024),
        name="update",
    )(gf, gw, gd, nm, sq, query_factor, out_factor, query_w, out_w)
    outs = list(outs)
    outs[1], outs[3] = outs[1].T, outs[3].T
    return tuple(outs)


def solution(mesh):
    finer = Mesh(mesh.devices.reshape(NZ, NY, NX, 2), (Z, Y, X, C))
    in_specs = (
        P(FS_REP, None),
        P(FS_REP, C),
        P(FS_REP, None),
        P(FS_REP, C),
        P(FS, C),
        P(C, FS),
        P(FS, None),
        P(FS, None),
        *[P(FS, C)] * 4,
    )
    out_specs = (
        P(FS, C),
        P(C, FS),
        P(FS, C),
        P(C, FS),
        *[P(FS, C)] * 4,
        P(None, C),
        P(C, None),
    )
    return jax.shard_map(body, mesh=finer, in_specs=in_specs, out_specs=out_specs, check_vma=False)
```

```python
import math

import jax
import jax.numpy as jnp
from jax import lax
from jax.experimental import pallas as pl
from jax.experimental.pallas import tpu as pltpu
from jax.sharding import Mesh
from jax.sharding import PartitionSpec as P

NZ, NY, NX = 8, 4, 4
NF = NZ * NY
D, RANK, HQ, TOKENS = 2048, 512, 1024, 98304
HALF = HQ // 2
TOK = TOKENS // (NF * NX)
ROWS = D // NF
MINE = RANK // NF
BLOCKS = 4
Z, Y, X, C = "fs_0", "fs_1", "rep", "tp"
FS = (Z, Y)
FS_REP = (Z, Y, X)
BF, F32 = jnp.bfloat16, jnp.float32
MESH = pl.DeviceIdType.MESH


def along(n, mode, flip):
    up, down = (n // 2, n - 1 - n // 2)[:: -1 if flip else 1]
    tree = {}
    for s, far in ((1, up), (-1, down)):
        if mode == "ring":
            hops = [(k, 1) for k in range(far)]
        elif mode == "direct":
            hops = [(0, k) for k in range(far, 0, -1)]
        else:
            hops = [(0, 2), (0, 1), (2, 2), (2, 1)]
        for at, by in hops:
            if at + by <= far:
                tree.setdefault(s * at, []).append((s, by, s * (at + by)))
    return tree, range(-down, up + 1)


def broadcast(axes, flip):
    (axis_1, mode_1), (axis_2, mode_2) = axes
    sizes = {Z: NZ, Y: NY}
    tree_1, span = along(sizes[axis_1], mode_1, flip)
    events = {}
    for i in span:
        tree_2, across = along(sizes[axis_2], mode_2, (i + flip) % 2)
        for j in across:
            on = [(axis_2, s, d, (i, to)) for s, d, to in tree_2.get(j, [])]
            if j == 0:
                on = [(axis_1, s, d, (to, 0)) for s, d, to in tree_1.get(i, [])] + on
            events[i, j] = on
    return events


def expected_order(gathers):
    free, now, order = {}, 0.0, []
    heap = [(0.01 * g.number, g.number, (0, 0)) for g in gathers]
    by_number = {g.number: g for g in gathers}
    while heap:
        heap.sort()
        when, number, key = heap.pop(0)
        now, g = max(now, when), by_number[number]
        if key != (0, 0):
            order.append((when, g, key))
        for axis, sign, distance, landed in g.events[key]:
            now += 0.02
            begin = max(free.get((axis, sign), 0.0), now)
            wire = g.kib / 91.0
            free[axis, sign] = begin + wire * distance
            heap.append((begin + wire + 2.0 + 0.75 * (distance - 1), number, landed))
    return order


class Gather:
    def __init__(self, number, axes, flip, kib, pieces, many, share, shares, where, sems, core):
        self.number, self.axes, self.kib = number, [a for a, _ in axes], kib
        self.events = broadcast(axes, flip)
        self.slots = {key: n for n, key in enumerate(k for k in self.events if k != (0, 0))}
        self.pieces, self.many, self.share, self.shares = pieces, many, share, shares
        self.where, self.core = where, core
        self.send_sem, self.recv_sem, self.pass_sem, self.give_sem = sems

    def index(self, key):
        off = dict(zip(self.axes, key))
        z = lax.rem(self.where[Z] + (NZ - off[Z]), NZ)
        y = lax.rem(self.where[Y] + (NY - off[Y]), NY)
        return z * NY + y

    def copy(self, ref, axis, by, slot):
        n = NZ if axis == Z else NY
        return pltpu.make_async_remote_copy(
            src_ref=ref,
            dst_ref=ref,
            send_sem=self.send_sem,
            recv_sem=self.recv_sem.at[slot],
            device_id={axis: lax.rem(self.where[axis] + (n + by), n)},
            device_id_type=MESH,
        )

    def give(self, ref):
        return pltpu.make_async_remote_copy(
            src_ref=ref,
            dst_ref=ref,
            send_sem=self.pass_sem,
            recv_sem=self.give_sem,
            device_id={C: self.core},
            device_id_type=MESH,
        )

    def pass_on(self, key):
        f = self.index(key)
        for axis, sign, distance, landed in self.events[key]:
            for ref in self.pieces(f):
                self.copy(ref, axis, sign * distance, self.slots[landed]).start()

    def start(self):
        self.pass_on((0, 0))

    def arrive(self, key):
        f = self.index(key)
        self.copy(self.many(1), Z, 1, self.slots[key]).wait_recv()
        self.pass_on(key)
        if self.share is not None:
            self.give(self.share(f)).start()
        return f

    def finish(self):
        self.copy(self.many(PIECES), Z, 1, 0).wait_send()
        if self.shares is not None:
            self.give(self.shares()).wait_send()

    def given(self):
        self.give(self.shares()).wait_recv()


PIECES = NF - 1
EARLY = 6
ZY_RING, YZ_RING = ((Z, "ring"), (Y, "ring")), ((Y, "ring"), (Z, "ring"))
ZY_FAST, YZ_FAST = ((Z, "skip"), (Y, "ring")), ((Y, "direct"), (Z, "skip"))


def reduce_kernel(*refs):
    (
        input_act, query_cot, out_cot, attn_out, query_w, out_w, query_factor, out_factor,
        first_q, second_q, first_o, second_o,
        gf_out, gw_out, gd_out, nm_out, sq_out,
        gf, gw, gd, act, cot, qw, ow, moments, low, px, rx1, rx2, s1, ry, s2,
        rz, sp, sq, sq_parts, nm,
        load, f_send, f_recv, f_pass, f_give, w_send, w_pass, w_give, near_end,
        d_send, d_pass, d_give, own_send, own_recv, mom_send, mom_recv,
        cot_send, cot_recv, px_send, px_recv,
        rx1_send, rx1_recv, rx2_send, rx2_recv, ry_send, ry_recv, rz_send, rz_recv,
        sp_send, sp_recv, nm_sem, sq_sem, out_sem,
    ) = refs
    z, y, x, c = (lax.axis_index(a) for a in (Z, Y, X, C))
    f = z * NY + y
    where = {Z: z, Y: y}
    other = 1 - c
    leads, follows = pl.when(c == 1), pl.when(c == 0)

    def load_own(number, if_q, if_o, dst):
        @follows
        def _():
            pltpu.make_async_copy(if_q, dst, load.at[number]).start()

        @leads
        def _():
            pltpu.make_async_copy(if_o, dst, load.at[number]).start()

        return pltpu.make_async_copy(if_q, dst, load.at[number])

    def load_plain(number, src, dst):
        cp = pltpu.make_async_copy(src, dst, load.at[number])
        cp.start()
        return cp

    for j in range(4):
        cols = pl.ds(128 * j, 128)
        for t, factor in enumerate((query_factor, out_factor)):
            load_plain(0, factor.at[:, cols], gf.at[2 * j + t, f])
    w_loads = [load_plain(1, query_w, qw), load_plain(2, out_w, ow)]
    act_load = load_own(3, input_act, out_cot, act)
    for k in range(2):
        cols = pl.ds(256 * k, 256)
        _ = load_own(4, query_cot.at[:, cols], attn_out.at[:, cols], cot.at[2 * c + k])

    barrier = pltpu.get_barrier_semaphore()
    peers = [{C: other}]
    for axis, at, n in ((Z, z, NZ), (Y, y, NY), (X, x, NX)):
        peers += [{axis: lax.rem(at + 1, n)}, {axis: lax.rem(at + n - 1, n)}]
    peers += [{Z: lax.rem(z + 2, NZ)}, {Z: lax.rem(z + NZ - 2, NZ)}, {Y: lax.rem(y + 2, NY)}]
    for peer in peers:
        pl.semaphore_signal(barrier, inc=1, device_id=peer, device_id_type=MESH)

    for w in w_loads:
        w.wait()
    for k in range(2):
        gw[4 * c + 2 * k, f] = qw[:, 256 * k : 256 * k + 256].astype(BF)
        gw[4 * c + 2 * k + 1, f] = ow[:, 256 * k : 256 * k + 256].astype(BF)
    factors = gf.at[:, f]
    pltpu.make_async_copy(factors, factors, load.at[0]).wait()
    pl.semaphore_wait(barrier, len(peers))

    parts = (pl.ds(0, 5), pl.ds(5, 3))

    def factor_gather(k):
        return Gather(
            k, (ZY_FAST, YZ_RING)[k], 1 - k, (80, 48)[k],
            lambda p: (gf.at[parts[k], p],), lambda n: gf.at[parts[k], pl.ds(0, n)],
            lambda p: gf.at[parts[k], p], lambda: gf.at[parts[k], pl.ds(0, PIECES)],
            where, [a.at[k] for a in (f_send, f_recv, f_pass, f_give)], 0,
        )

    def weight_gather(k):
        give = (pl.ds(4, 1), parts[1])[k]
        return Gather(
            k, (ZY_RING, YZ_RING)[k], k, (160, 96)[k],
            lambda p: (gw.at[parts[k], p],), lambda n: gw.at[parts[k], pl.ds(0, n)],
            lambda p: gw.at[give, p], None,
            where, (w_send.at[k], f_recv.at[k], w_pass, w_give), 1,
        )

    def all_shares():
        return every(gw.at[pl.ds(4, 4), pl.ds(0, PIECES)], w_pass, w_give)

    def dir_gather(k):
        return Gather(
            k, ZY_FAST if k == 0 else YZ_FAST, k, 32,
            lambda p: (gd.at[k, p],), lambda n: gd.at[k, pl.ds(0, n)],
            lambda p: gd.at[k, p, 0], lambda: gd.at[k, :, 0],
            where, (d_send.at[k], f_recv.at[k], d_pass.at[k], d_give.at[k]), 0,
        )

    fg = [factor_gather(k) for k in range(2)]
    wg = [weight_gather(k) for k in range(2)]
    dg = [dir_gather(k) for k in range(2)]
    f_order, w_order, d_order = (expected_order(g) for g in (fg, wg, dg))

    @leads
    def _():
        for g in fg:
            g.start()

    def cot_copy(src, k):
        return pltpu.make_async_remote_copy(
            src_ref=src.at[:, pl.ds(256 * k, 256)],
            dst_ref=cot.at[2 * c + k],
            send_sem=cot_send,
            recv_sem=cot_recv,
            device_id={C: other},
            device_id_type=MESH,
        )

    def every(ref, send_sem, recv_sem):
        return pltpu.make_async_remote_copy(
            src_ref=ref,
            dst_ref=ref,
            send_sem=send_sem,
            recv_sem=recv_sem,
            device_id={C: other},
            device_id_type=MESH,
        )

    def both_cots():
        return every(cot.at[pl.ds(0, 2)], cot_send, cot_recv)

    def own_weights():
        return every(gw.at[pl.ds(4, 4), f], own_send, own_recv)

    def own_moments(k, m):
        return pltpu.make_async_remote_copy(
            src_ref=m,
            dst_ref=moments.at[k, 0],
            send_sem=mom_send,
            recv_sem=mom_recv,
            device_id={C: 1},
            device_id_type=MESH,
        )

    all_moments = (first_q, second_q, first_o, second_o)

    @follows
    def _():
        for k in range(2):
            cot_copy(attn_out, k).start()
        for k, m in enumerate(all_moments):
            own_moments(k, m).start()

    @leads
    def _():
        for k in range(2):
            cot_copy(query_cot, k).start()
        own_weights().start()
        for k, m in enumerate(all_moments):
            pltpu.make_async_copy(m, moments.at[k, 1], load.at[5]).start()

    def project(h):
        def tile(m, _):
            rows = pl.ds(pl.multiple_of(m * 256, 256), 256)
            right = jnp.concatenate(
                [gf[2 * (2 * h + j) + c].reshape(D, 128) for j in range(2)], axis=1
            )
            low[rows, :] = jnp.dot(act[rows, :], right, preferred_element_type=F32).astype(BF)
            return 0

        lax.fori_loop(0, TOK // 256, tile, 0)
        if h:
            @leads
            def _():
                x_start(0)

        for i in range(NX):
            xb = lax.rem(x + 2 + i, NX)
            dims = (((0,), (0,)), ((), ()))
            total = lax.dot_general(low[...], cot[xb], dims, preferred_element_type=F32)
            px[h, xb, c] = total.astype(BF)

            @follows
            def _():
                partial_over(h, i).start()

        if h:

            @leads
            def _():
                x_start(1)

    x_up, x_down, x_far = lax.rem(x + 1, NX), lax.rem(x + 3, NX), lax.rem(x + 2, NX)
    sides = ((x_up, 0), (x_down, 1))

    def partial_over(h, i):
        ref = px.at[h, lax.rem(x + 2 + i, NX), 0]
        return pltpu.make_async_remote_copy(
            src_ref=ref,
            dst_ref=ref,
            send_sem=px_send,
            recv_sem=px_recv.at[h, i],
            device_id={C: 1},
            device_id_type=MESH,
        )

    def x_first(h, k):
        return pltpu.make_async_remote_copy(
            src_ref=px.at[h, x_far, :, pl.ds(128 * k, 128)],
            dst_ref=rx1.at[h, k],
            send_sem=rx1_send,
            recv_sem=rx1_recv.at[h, k],
            device_id={X: sides[k][0]},
            device_id_type=MESH,
        )

    def x_second(h, k):
        return pltpu.make_async_remote_copy(
            src_ref=px.at[h, sides[k][0]],
            dst_ref=rx2.at[h, k],
            send_sem=rx2_send,
            recv_sem=rx2_recv.at[h],
            device_id={X: sides[k][0]},
            device_id_type=MESH,
        )

    def x_start(h):
        partial_over(h, 0).wait_recv()
        for k in range(2):
            x_first(h, k).start()

    def x_merge(h):
        for i in (1, 3):
            partial_over(h, i).wait_recv()
        for to, k in sides:
            x_first(h, k).wait_recv()
            rows = pl.ds(128 * k, 128)
            merged = px[h, to, :, rows].astype(F32) + rx1[h, k].astype(F32)
            px[h, to, :, rows] = merged.astype(BF)
            x_second(h, k).start()

    def x_sum(h):
        partial_over(h, 2).wait_recv()
        every(rx2.at[h], rx2_send, rx2_recv.at[h]).wait_recv()
        for t in range(2):
            total = px[h, x, t].astype(F32)
            for k in range(2):
                total += rx2[h, k, t].astype(F32)
            s1[pl.ds(4 * h, 4), :, t] = total.astype(BF).reshape(4, NY, MINE, 256)
        for d in (2, 1, 3):
            y_copy(h, d).start()

    def y_copy(h, d):
        to = lax.rem(y + d, NY)
        return pltpu.make_async_remote_copy(
            src_ref=s1.at[pl.ds(4 * h, 4), to],
            dst_ref=ry.at[h, d - 1],
            send_sem=ry_send,
            recv_sem=ry_recv.at[h],
            device_id={Y: to},
            device_id_type=MESH,
        )

    def y_sum(h):
        total = s1[pl.ds(4 * h, 4), y].astype(F32)
        every(ry.at[h], ry_send, ry_recv.at[h]).wait_recv()
        for d in range(1, NY):
            total += ry[h, d - 1].astype(F32)
        s2[pl.ds(4 * h, 4)] = total.astype(BF)

    def z_copy(d):
        to = lax.rem(z + d, NZ)
        return pltpu.make_async_remote_copy(
            src_ref=s2.at[to],
            dst_ref=rz.at[d - 1],
            send_sem=rz_send,
            recv_sem=rz_recv,
            device_id={Z: to},
            device_id_type=MESH,
        )

    def sum_copy(d):
        return pltpu.make_async_remote_copy(
            src_ref=sp.at[0],
            dst_ref=sp.at[d],
            send_sem=sp_send,
            recv_sem=sp_recv,
            device_id={X: lax.rem(x + d, NX)},
            device_id_type=MESH,
        )

    def all_sums():
        return every(sp.at[pl.ds(1, NX - 1)], sp_send, sp_recv)

    def moments_over():
        return pltpu.make_async_remote_copy(
            src_ref=nm.at[:, 0],
            dst_ref=nm_out,
            send_sem=nm_sem.at[0],
            recv_sem=nm_sem.at[1],
            device_id={C: 0},
            device_id_type=MESH,
        )

    def squares(t, at):
        part = jnp.square(gd[t, at].astype(F32)).reshape(2 * MINE // 8, 8, HALF)
        part = jnp.sum(part, axis=0)
        return part[:, :128] + part[:, 128:256] + part[:, 256:384] + part[:, 384:]

    def weights_out():
        return pltpu.make_async_copy(gw.at[pl.ds(4 * c, 4)], gw_out, out_sem.at[1])

    def dir_out(t, at):
        return pltpu.make_async_copy(gd.at[t, at, 1], gd_out.at[t, at], out_sem.at[5])

    def own_dirs(t):
        return dg[t].give(gd.at[t, f, 0])

    outs = []

    def put(number, src, dst):
        cp = pltpu.make_async_copy(src, dst, out_sem.at[number])
        cp.start()
        outs.append(cp)

    @leads
    def _():
        cue = sum(when < f_order[-1][0] - 2.5 for when, _, _ in f_order)
        for n, (_, g, key) in enumerate(f_order):
            if n == cue:
                pl.semaphore_signal(near_end, inc=1, device_id={C: 0}, device_id_type=MESH)
            g.arrive(key)

    @follows
    def _():
        own_weights().wait_recv()
        pl.semaphore_wait(near_end, 1)
        for g in wg:
            g.start()
        fg[0].given()

    act_load.wait()
    cot_half = cot.at[pl.ds(0, 2)]
    pltpu.make_async_copy(cot_half, cot_half, load.at[4]).wait()
    both_cots().wait_recv()
    project(0)

    @follows
    def _():
        fg[1].given()
        for _, g, key in w_order[:EARLY]:
            g.arrive(key)

    project(1)
    put(0, gf, gf_out)

    @leads
    def _():
        x_merge(0)
        x_merge(1)
        x_sum(0)
        x_sum(1)
        for h in range(2):
            y_sum(h)
            for d in (4, 3, 5, 2, 6, 1, 7):

                @pl.when(lax.rem(z + d, NZ) // 4 == h)
                def _():
                    z_copy(d).start()

        total = s2[z].astype(F32)
        every(rz, rz_send, rz_recv).wait_recv()
        for d in range(1, NZ):
            total += rz[d - 1].astype(F32)
        sp[0] = total
        for d in (2, 1, 3):
            sum_copy(d).start()
        every(moments.at[:, 0], mom_send, mom_recv).wait_recv()
        pltpu.make_async_copy(moments.at[:, 1], moments.at[:, 1], load.at[5]).wait()
        all_sums().wait_recv()

        for t in range(2):
            for p in range(2):
                proj = jnp.concatenate(
                    [sp[lax.rem(x + (NX - q), NX), t] for q in (2 * p, 2 * p + 1)], axis=1
                )
                proj = proj * (1.0 / math.sqrt(TOKENS))
                first = 0.8 * moments[2 * t, p] + 0.2 * proj
                second = 0.9 * moments[2 * t + 1, p] + 0.1 * proj * proj
                nm[2 * t, p] = first
                nm[2 * t + 1, p] = second
                gd[t, f, p] = (first / jnp.sqrt(second)).astype(BF)
            dg[t].start()
            own_dirs(t).start()
            dir_out(t, f).start()
            sq_parts[t, f] = squares(t, f)
        moments_over().start()
        pltpu.make_async_copy(nm.at[:, 1], nm_out, out_sem.at[4]).start()
        for n, (_, g, key) in enumerate(d_order):
            if n == 3 * len(d_order) // 4:
                all_shares().wait_recv()
                weights_out().start()
            at = g.arrive(key)
            dir_out(g.number, at).start()
            sq_parts[g.number, at] = squares(g.number, at)


    @follows
    def _():
        for _, g, key in w_order[EARLY:]:
            g.arrive(key)

    @follows
    def _():
        weights_out().start()


    @leads
    def _():
        total = jnp.sum(sq_parts[...].reshape(2 * NF, 8, 128), axis=0)
        sq[...] = jnp.broadcast_to(jnp.sum(total, axis=(0, 1), keepdims=True), (8, 128))

    squares_over = pltpu.make_async_remote_copy(
        src_ref=sq,
        dst_ref=sq,
        send_sem=sq_sem.at[0],
        recv_sem=sq_sem.at[1],
        device_id={C: 0},
        device_id_type=MESH,
    )

    @leads
    def _():
        squares_over.start()

    @follows
    def _():
        for t in range(2):
            dg[t].given()
            pltpu.make_async_copy(gd.at[t, :, 0], gd_out.at[t], out_sem.at[5]).start()

    @follows
    def _():
        squares_over.wait_recv()

    put(2, sq, sq_out)

    @leads
    def _():
        for g in fg + dg:
            g.finish()
        own_weights().wait_send()
        every(rx1, rx1_send, rx1_recv.at[0, 0]).wait_send()
        every(rx2, rx2_send, rx2_recv.at[0]).wait_send()
        every(ry, ry_send, ry_recv.at[0]).wait_send()
        every(rz, rz_send, rz_recv).wait_send()
        all_sums().wait_send()
        moments_over().wait_send()
        pltpu.make_async_copy(nm.at[:, 1], nm_out, out_sem.at[4]).wait()
        squares_over.wait_send()

    @follows
    def _():
        for g in wg:
            g.finish()
        all_shares().wait_send()
        every(moments.at[:, 0], mom_send, mom_recv).wait_send()
        moments_over().wait_recv()
        every(px.at[:, :, 0], px_send, px_recv.at[0, 0]).wait_send()

    both_cots().wait_send()
    weights_out().wait()
    for cp in outs:
        cp.wait()
    pltpu.make_async_copy(gd.at[:, :, c], gd_out, out_sem.at[5]).wait()


def update_kernel(
    gf_in, gw_in, gd_in, nm_in, sq_in, query_factor, out_factor, query_w, out_w,
    new_qw, new_ow, q_step, o_step, nf_q, ns_q, nf_o, ns_o, q_copy, o_copy,
    gf, gw, gd, nm, sq, factor, w, steps, new_w, new_q, new_o,
    first_sem, block_sem, small_sem, copy_sem, out_sem,
):
    copy = pltpu.make_async_copy
    per = NF // BLOCKS
    size = D // BLOCKS
    first = [copy(gd_in, gd, first_sem.at[0]), copy(sq_in, sq, first_sem.at[1])]
    small = [copy(nm_in, nm, small_sem.at[0])]
    for t, (fac, old) in enumerate(((query_factor, query_w), (out_factor, out_w))):
        small.append(copy(fac, factor.at[t], small_sem.at[1 + 2 * t]))
        small.append(copy(old, w.at[t], small_sem.at[2 + 2 * t]))

    def block_loads(b):
        some = pl.ds(per * b, per)
        return (
            copy(gf_in.at[:, some], gf.at[:, some], block_sem.at[0, b]),
            copy(gw_in.at[:, some], gw.at[:, some], block_sem.at[1, b]),
        )

    def block_stores(b):
        at = pl.ds(pl.multiple_of(size * b, size), size)
        return (
            copy(new_q.at[b], q_copy.at[at], copy_sem.at[0]),
            copy(new_o.at[b], o_copy.at[:, at], copy_sem.at[1]),
        )

    for cp in first:
        cp.start()
    for cp in block_loads(0):
        cp.start()
    for cp in first:
        cp.wait()
    for cp in block_loads(1) + block_loads(2):
        cp.start()
    for cp in small:
        cp.start()
    inverse = 1.0 / jnp.sqrt(sq[0:1] / (2 * RANK * HQ) + 1e-06)
    inverse = jnp.concatenate([inverse] * 4, axis=1)
    def block(b, _):
        some = pl.ds(per * b, per)
        @pl.when(b + 3 < BLOCKS)
        def _():
            for cp in block_loads(b + 3):
                cp.start()

        for cp in block_loads(b):
            cp.wait()
        moved = []
        for t in range(2):
            rows = jnp.concatenate(
                [gf[2 * j + t, some].reshape(size, 128) for j in range(4)], axis=1
            )
            step = jnp.dot(rows, gd[t].reshape(RANK, HALF), preferred_element_type=F32)
            old = jnp.concatenate([gw[i, some].reshape(size, 256) for i in (t, 2 + t)], axis=1)
            moved.append(old.astype(F32) - (0.01 * inverse) * step)
        new_q[b] = moved[0].astype(BF)
        new_o[b] = moved[1].astype(BF).T
        for cp in block_stores(b):
            cp.start()
        return 0

    lax.fori_loop(0, BLOCKS, block, 0)
    for cp in small:
        cp.wait()
    stores = [copy(nm.at[k], o, out_sem.at[k]) for k, o in enumerate((nf_q, ns_q, nf_o, ns_o))]
    for t, (to_step, to_w) in enumerate(((q_step, new_qw), (o_step, new_ow))):
        step = jnp.dot(factor[t], gd[t].reshape(RANK, HALF), preferred_element_type=F32)
        step = step * inverse
        steps[t] = step
        new_w[t] = w[t] - 0.01 * step
        stores.append(copy(steps.at[t], to_step, out_sem.at[4 + 2 * t]))
        stores.append(copy(new_w.at[t], to_w, out_sem.at[5 + 2 * t]))
    for cp in stores:
        cp.start()
    for cp in stores:
        cp.wait()
    copy(new_q, new_q, copy_sem.at[0]).wait()
    copy(new_o, new_o, copy_sem.at[1]).wait()


def body(
    input_act, query_cot, out_cot, attn_out, query_w, out_w, query_factor, out_factor,
    first_q, second_q, first_o, second_o,
):
    struct = jax.ShapeDtypeStruct
    dma = pltpu.SemaphoreType.DMA
    vmem = pltpu.VMEM
    out_w = out_w.T
    scratch = [
        vmem((8, NF, ROWS, 128), BF),
        vmem((8, NF, ROWS, 256), BF),
        vmem((2, NF, 2, MINE, HALF), BF),
        vmem((TOK, D), BF),
        vmem((4, TOK, 256), BF),
        vmem((ROWS, HALF), F32),
        vmem((ROWS, HALF), F32),
        vmem((4, 2, MINE, HALF), F32),
        vmem((TOK, 256), BF),
        vmem((2, NX, 2, 256, 256), BF),
        vmem((2, 2, 2, 128, 256), BF),
        vmem((2, 2, 2, 256, 256), BF),
        vmem((NZ, NY, 2, MINE, 256), BF),
        vmem((2, NY - 1, 4, 2, MINE, 256), BF),
        vmem((NZ, 2, MINE, 256), BF),
        vmem((NZ - 1, 2, MINE, 256), BF),
        vmem((NX, 2, MINE, 256), F32),
        vmem((8, 128), F32),
        vmem((2, NF, 8, 128), F32),
        vmem((4, 2, MINE, HALF), F32),
        dma((6,)),
        dma((2,)), dma((2, PIECES)), dma((2,)), dma((2,)),
        dma((2,)), dma, dma, pltpu.SemaphoreType.REGULAR,
        dma((2,)), dma((2,)), dma((2,)),
        dma, dma, dma, dma, dma, dma,
        dma, dma((2, NX)),
        dma, dma((2, 2)), dma, dma((2,)),
        dma, dma((2,)), dma, dma, dma, dma,
        dma((2,)), dma((2,)), dma((6,)),
    ]
    gf, gw, gd, nm, sq = pl.pallas_call(
        reduce_kernel,
        out_shape=(
            struct((8, NF, ROWS, 128), BF),
            struct((4, NF, ROWS, 256), BF),
            struct((2, NF, MINE, HALF), BF),
            struct((4, MINE, HALF), F32),
            struct((8, 128), F32),
        ),
        in_specs=[pl.BlockSpec(memory_space=pl.ANY)] * 12,
        out_specs=[pl.BlockSpec(memory_space=pl.ANY)] * 5,
        scratch_shapes=scratch,
        compiler_params=pltpu.CompilerParams(
            collective_id=0, has_side_effects=True, vmem_limit_bytes=56 * 1024 * 1024
        ),
        name="reduce",
    )(
        input_act, query_cot, out_cot, attn_out, query_w, out_w, query_factor, out_factor,
        first_q, second_q, first_o, second_o,
    )

    anywhere = pl.BlockSpec(memory_space=pl.ANY)
    shard, small = struct((ROWS, HALF), F32), struct((MINE, HALF), F32)
    outs = pl.pallas_call(
        update_kernel,
        out_shape=(
            *[shard] * 4,
            *[small] * 4,
            struct((D, HALF), BF),
            struct((HALF, D), BF),
        ),
        in_specs=[anywhere] * 9,
        out_specs=[anywhere] * 10,
        scratch_shapes=[
            vmem((8, NF, ROWS, 128), BF),
            vmem((4, NF, ROWS, 256), BF),
            vmem((2, NF, MINE, HALF), BF),
            vmem((4, MINE, HALF), F32),
            vmem((8, 128), F32),
            vmem((2, ROWS, RANK), BF),
            vmem((2, ROWS, HALF), F32),
            vmem((2, ROWS, HALF), F32),
            vmem((2, ROWS, HALF), F32),
            vmem((BLOCKS, D // BLOCKS, HALF), BF),
            vmem((BLOCKS, HALF, D // BLOCKS), BF),
            dma((2,)),
            dma((2, BLOCKS)),
            dma((5,)),
            dma((2,)),
            dma((8,)),
        ],
        compiler_params=pltpu.CompilerParams(vmem_limit_bytes=56 * 1024 * 1024),
        name="update",
    )(gf, gw, gd, nm, sq, query_factor, out_factor, query_w, out_w)
    outs = list(outs)
    outs[1], outs[3] = outs[1].T, outs[3].T
    return tuple(outs)


def solution(mesh):
    finer = Mesh(mesh.devices.reshape(NZ, NY, NX, 2), (Z, Y, X, C))
    in_specs = (
        P(FS_REP, None),
        P(FS_REP, C),
        P(FS_REP, None),
        P(FS_REP, C),
        P(FS, C),
        P(C, FS),
        P(FS, None),
        P(FS, None),
        *[P(FS, C)] * 4,
    )
    out_specs = (
        P(FS, C),
        P(C, FS),
        P(FS, C),
        P(C, FS),
        *[P(FS, C)] * 4,
        P(None, C),
        P(C, None),
    )
    return jax.shard_map(body, mesh=finer, in_specs=in_specs, out_specs=out_specs, check_vma=False)
```
